32 devices in a mesh: sp: 8 (over z, y), tp: 4 (over x, core).
Axes of the slice: x: 2, y: 2, z: 4, core: 2. Of those that a mesh axis runs over, the one named last changes fastest.
Arguments:
- glu_value: bfloat16 [4096, 1024], P('sp', 'tp'), may hold values from -6 to 6
- glu_gate: bfloat16 [4096, 1024], P('sp', 'tp'), may hold values from -8 to 8
- conv_taps: bfloat16 [31, 1024], P(None, 'tp'), may hold values from -1 to 1
- norm_gain: float32 [1024], P('tp'), may hold values from 0.1 to 1.9
- out_weight: bfloat16 [2048, 1024], P(None, 'tp'), may hold values from -0.1875 to 0.1875
- norm_mean: float32 [4096], P('sp'), may hold values from -3 to 3
- norm_scale: float32 [4096], P('sp'), may hold values from 0.5 to 2
- out_grad: bfloat16 [4096, 2048], P('sp'), may hold values from -6 to 6
Outputs:
- value_grad: bfloat16 [4096, 1024], P('sp', 'tp')
- gate_grad: bfloat16 [4096, 1024], P('sp', 'tp')
- taps_grad: float32 [31, 1024], P(None, 'tp')
- gain_grad: float32 [1024], P('tp')
- weight_grad: float32 [2048, 1024], P('sp', 'tp')
The draws below stay inside these ranges and needn't reach their ends.
All inputs are finite; a program needn't handle non-finite values.
Results may differ from the reference program's by a relative error of at most 0.0047.
Values may be sent and summed in bfloat16 or wider, within the bound.
A program may use at most 64 MiB of HBM per device.

```python
import math
import jax
import jax.numpy as jnp
from jax import lax

D = 2048
CH = 1024
KW = 31
TOKENS = 4096


def spiked(drawn, stream_key, source, target, parts, factor):
    owner, partner = [(jnp.arange(drawn.shape[position]) // (drawn.shape[position] // parts)).reshape([-1 if axis == position else 1 for axis in range(drawn.ndim)]) for position in (source, target)]
    chosen = jax.random.permutation(stream_key, parts)[partner]
    strong = (owner == chosen) | (owner == (partner + parts // 2) % parts)
    return jnp.where(strong, factor * drawn, drawn)


def levels(rng, shape, pieces, smallest, largest):
    level = 1.0
    for axis_at, blocks in pieces:
        steps = jax.random.uniform(jax.random.fold_in(jax.random.fold_in(rng, 6), axis_at), (blocks,), jnp.float32, smallest / len(pieces), largest / len(pieces))
        level = level * jnp.repeat(jnp.exp(steps), shape[axis_at] // blocks).reshape((-1,) + (1,) * (len(shape) - 1 - axis_at))
    return level


def centred(own_key, dims, deviation, most, pieces=(), dtype=jnp.bfloat16):
    values = jax.random.normal(own_key, dims, jnp.float32) * deviation
    if len(pieces) > 0:
        values = levels(own_key, dims, pieces, -0.22, 0.18) * values
    return jnp.clip(values, min=-most, max=most).astype(dtype)


def gaussian_with(stream_key, dims, spread, bound, pieces, heavy, dtype=jnp.bfloat16):
    drawn = spread * jax.random.normal(stream_key, dims, jnp.float32)
    if pieces:
        drawn = drawn * levels(stream_key, dims, pieces, -0.22, 0.18)
    return jnp.clip(spiked(drawn, jax.random.fold_in(stream_key, 3), *heavy), -bound, bound).astype(dtype)


def setup_inputs(seed: int = 0) -> dict:
    arg_keys = jax.random.split(jax.random.key(seed), 9)
    return {
        "glu_value": centred(arg_keys[0], (TOKENS, CH), 1.0, 6.0, ((0, 8), (1, 4))),
        "glu_gate": centred(arg_keys[1], (TOKENS, CH), 1.5, 8.0, ((0, 8), (1, 4))),
        "conv_taps": centred(arg_keys[2], (KW, CH), KW ** -0.5, 1.0, ((1, 4),)),
        "norm_gain": jnp.clip(1.0 + 0.18 * jax.random.normal(arg_keys[3], (CH,), jnp.float32), 0.1, 1.9),
        "out_weight": centred(arg_keys[4], (D, CH), CH ** -0.5, 0.1875, ((1, 4),)),
        "norm_mean": centred(arg_keys[5], (TOKENS,), 0.3, 3.0, ((0, 8),), jnp.float32),
        "norm_scale": jnp.clip(jnp.exp(math.log(2.0) - 1.3862944 * jax.random.uniform(arg_keys[6], (TOKENS,), jnp.float32) ** levels(arg_keys[6], (TOKENS,), ((0, 8),), -0.2, 0.2)), 0.5, 2.0),
        "out_grad": gaussian_with(arg_keys[7], (TOKENS, D), 1.0, 6.0, ((0, 8),), (0, 1, 8, 2.0)),
    }


def reference(glu_value, glu_gate, conv_taps, norm_gain, out_weight, norm_mean, norm_scale, out_grad):
    val_float = glu_value.astype(jnp.float32)
    gate_sig = jax.nn.sigmoid(glu_gate.astype(jnp.float32))
    gated = (val_float * gate_sig).astype(jnp.bfloat16)
    padded = jnp.pad(gated.astype(jnp.float32), ((KW - 1, 0), (0, 0)))
    taps_float = conv_taps.astype(jnp.float32)
    conv = jnp.zeros((TOKENS, CH), jnp.float32)
    for offset in range(KW):
        conv = conv + taps_float[offset] * padded[offset:offset + TOKENS]
    centered = (conv - norm_mean[:, None]) * norm_scale[:, None]
    normed = centered * norm_gain
    sig_norm = jax.nn.sigmoid(normed)
    activated = (normed * sig_norm).astype(jnp.bfloat16)
    act_grad = jnp.dot(out_grad, out_weight, preferred_element_type=jnp.float32)
    normed_grad = act_grad * sig_norm * (1.0 + normed * (1.0 - sig_norm))
    gain_grad = jnp.sum(normed_grad * centered, axis=0)
    scaled_grad = normed_grad * norm_gain
    mean_plain = jnp.mean(scaled_grad, axis=1)
    mean_cross = jnp.mean(scaled_grad * centered, axis=1)
    conv_grad = norm_scale[:, None] * (scaled_grad - mean_plain[:, None] - centered * mean_cross[:, None])
    grad_padded = jnp.pad(conv_grad, ((0, KW - 1), (0, 0)))
    gated_grad = jnp.zeros((TOKENS, CH), jnp.float32)
    tap_list = []
    for offset in range(KW):
        begin = KW - 1 - offset
        gated_grad = gated_grad + taps_float[offset] * grad_padded[begin:begin + TOKENS]
        tap_list.append(jnp.sum(conv_grad * padded[offset:offset + TOKENS], axis=0))
    taps_grad = jnp.stack(tap_list, axis=0)
    value_grad = (gated_grad * gate_sig).astype(jnp.bfloat16)
    gate_grad = (gated_grad * val_float * gate_sig * (1.0 - gate_sig)).astype(jnp.bfloat16)
    weight_grad = lax.dot_general(out_grad, activated, (((0,), (0,)), ((), ())), preferred_element_type=jnp.float32)
    return value_grad, gate_grad, taps_grad, gain_grad, weight_grad
```

```python
import functools

import jax
import jax.numpy as jnp
from jax import lax
from jax.experimental import pallas as pl
from jax.experimental.pallas import tpu as pltpu
from jax.sharding import PartitionSpec as P

MESH = pl.DeviceIdType.MESH
F32 = jnp.float32
BF16 = jnp.bfloat16
LANES = 128
VMEM_LIMIT = 30 * 1024 * 1024
BLOCK = 64


def rup(value, unit):
    return -(-value // unit) * unit


def kernel(
    n, m, kw,
    val, gate, taps_in, gain, mean_row, scale_row, og_hbm, ow_hbm,
    value_grad, gate_grad, taps_out, gain_out, w_out,
    taps, og, ow, gp, sh, cg, sh2, centered, slope, act, agrad, psum, csum, meanb, scaleb,
    mpb, mcb, halo_out, halo_in, stats, taploc, tapin, tapsum, wsum, wbf, recv1, send2, recv2,
    load_sem, halo_sem, back_sem, stat_send, stat_recv, tap_send, tap_recv, all_send, all_recv,
    y_send, y_recv, z_send, z_recv,
):
    rows, chans = val.shape
    tiles = chans // LANES
    depth = og.shape[1]
    dr = depth // n
    half = n // 2
    reach = kw - 1
    halo = halo_out.shape[0]
    lead = halo - reach
    blocks = rows // BLOCK
    sp = lax.axis_index("sp")
    tp = lax.axis_index("tp")
    par = lax.rem(sp, 2)
    q = lax.div(sp, 2)
    partner = sp + 1 - 2 * par

    load_og = pltpu.make_async_copy(og_hbm, og, load_sem.at[0])
    load_ow = pltpu.make_async_copy(ow_hbm, ow, load_sem.at[1])
    load_og.start()
    load_ow.start()

    barrier = pltpu.get_barrier_semaphore()

    @pl.loop(1, n)
    def _(k):
        pl.semaphore_signal(
            barrier, inc=1, device_id={"sp": lax.rem(sp + k, n)}, device_id_type=MESH
        )

    @pl.loop(1, m)
    def _(k):
        pl.semaphore_signal(
            barrier, inc=1, device_id={"tp": lax.rem(tp + k, m)}, device_id_type=MESH
        )

    def lanes(ct):
        return slice(ct * LANES, (ct + 1) * LANES)

    taps[...] = taps_in[...].astype(F32)
    tail = slice(rows - halo, rows)
    tail_sig = jax.nn.sigmoid(gate[tail, :].astype(F32))
    halo_out[...] = (val[tail, :].astype(F32) * tail_sig).astype(BF16)

    def gate_block(b, _):
        at = pl.ds(pl.multiple_of(b * BLOCK, BLOCK), BLOCK)
        to = pl.ds(pl.multiple_of(b * BLOCK + halo, 16), BLOCK)
        for ct in range(tiles):
            sig = jax.nn.sigmoid(gate[at, lanes(ct)].astype(F32))
            gp[ct, to, :] = (val[at, lanes(ct)].astype(F32) * sig).astype(BF16).astype(F32)
        return 0

    lax.fori_loop(0, blocks, gate_block, 0)

    load_og.wait()
    load_ow.wait()
    slab = min(rows, 128)

    def grad_block(b, _):
        at = pl.ds(pl.multiple_of(b * slab, slab), slab)
        agrad[at, :] = jnp.dot(og[at, :], ow[...], preferred_element_type=F32)
        return 0

    lax.fori_loop(0, rows // slab, grad_block, 0)

    pl.semaphore_wait(barrier, n - 1 + m - 1)

    halo_copy = pltpu.make_async_remote_copy(
        src_ref=halo_out, dst_ref=halo_in,
        send_sem=halo_sem.at[0], recv_sem=halo_sem.at[1],
        device_id={"sp": lax.rem(sp + 1, n)}, device_id_type=MESH,
    )

    @pl.when(sp < n - 1)
    def _():
        halo_copy.start()

    def shifted(src, dst, begin, count):
        for ct in range(tiles):
            for r in range(1, 8):
                dst[r - 1, ct, begin : begin + count, :] = src[ct, begin + r : begin + r + count, :]

    for at in range(halo, rows + halo - 8, BLOCK):
        shifted(gp, sh, at, min(BLOCK, rows + halo - 8 - at))
    meanb[...] = jnp.broadcast_to(mean_row[...], (LANES, rows)).T
    scaleb[...] = jnp.broadcast_to(scale_row[...], (LANES, rows)).T

    def source(base_ref, copies, shift, ct, start, count):
        r, base = shift % 8, shift - shift % 8
        at = pl.ds(pl.multiple_of(start + base, 8), count)
        if r == 0:
            return base_ref[ct, at, :]
        return copies[r - 1, ct, at, :]

    def conv_block(b, _):
        start = pl.multiple_of(b * BLOCK, BLOCK)
        at = pl.ds(start, BLOCK)
        for ct in range(tiles):
            conv = jnp.zeros((BLOCK, LANES), F32)
            for k in range(kw):
                conv = conv + taps[k : k + 1, lanes(ct)] * source(gp, sh, k + lead, ct, start, BLOCK)
            cen = (conv - meanb[at, :]) * scaleb[at, :]
            nor = cen * gain[:, lanes(ct)]
            sig = jax.nn.sigmoid(nor)
            centered[ct, at, :] = cen
            slope[ct, at, :] = sig * (1.0 + nor * (1.0 - sig))
            act[at, lanes(ct)] = (nor * sig).astype(BF16)
        return 0

    lax.fori_loop(1, blocks, conv_block, 0)

    @pl.when(sp > 0)
    def _():
        halo_copy.wait_recv()
        for ct in range(tiles):
            gp[ct, 0:halo, :] = halo_in[:, lanes(ct)].astype(F32)

    @pl.when(sp == 0)
    def _():
        for ct in range(tiles):
            gp[ct, 0:halo, :] = jnp.zeros((halo, LANES), F32)

    shifted(gp, sh, 0, halo)
    conv_block(0, 0)

    wide = max(dr, min(depth, 256))

    def w_tile(start):
        start = pl.multiple_of(start, wide)
        part = lax.dot_general(
            og[:, pl.ds(start, wide)], act[...], (((0,), (0,)), ((), ())),
            preferred_element_type=F32,
        )
        wsum[pl.ds(start, wide), :] = part
        wbf[pl.ds(start, wide), :] = part.astype(BF16)

    def own_rows(p, side):
        return pl.ds(pl.multiple_of((2 * p + side) * dr, dr), dr)

    def y_copy(p):
        return pltpu.make_async_remote_copy(
            src_ref=wbf.at[own_rows(p, 1 - par), :], dst_ref=recv1.at[p],
            send_sem=y_send.at[p], recv_sem=y_recv.at[p],
            device_id={"sp": partner}, device_id_type=MESH,
        )

    def partner_step(k, _):
        p = lax.rem(q + k, half)
        w_tile((2 * p + 1 - par) * dr)
        y_copy(p).start()
        return 0

    def own_step(k, _):
        w_tile((2 * lax.rem(q + k, half) + par) * dr)
        return 0

    if wide == dr:
        lax.fori_loop(1, half, partner_step, 0)
        w_tile((2 * q + 1 - par) * dr)
    else:
        def tile_step(j, _):
            w_tile(j * wide)
            return 0

        lax.fori_loop(0, depth // wide, tile_step, 0)

        def send_step(k, _):
            y_copy(lax.rem(q + k, half)).start()
            return 0

        lax.fori_loop(1, half, send_step, 0)

    def stat_block(b, sums):
        at = pl.ds(pl.multiple_of(b * BLOCK, BLOCK), BLOCK)
        plain = jnp.zeros((BLOCK, LANES), F32)
        cross = jnp.zeros((BLOCK, LANES), F32)
        new = []
        for ct in range(tiles):
            cen = centered[ct, at, :]
            ngrad = agrad[at, lanes(ct)] * slope[ct, at, :]
            scaled = ngrad * gain[:, lanes(ct)]
            agrad[at, lanes(ct)] = scaled
            plain = plain + scaled
            cross = cross + scaled * cen
            new.append(sums[ct] + jnp.sum((ngrad * cen).reshape(BLOCK // 8, 8, LANES), axis=0))
        psum[at, :] = plain
        csum[at, :] = cross
        return tuple(new)

    gains = lax.fori_loop(
        0, blocks, stat_block, tuple(jnp.zeros((8, LANES), F32) for _ in range(tiles))
    )
    stats[tp, 0:1, :] = jnp.sum(psum[...].T, axis=0, keepdims=True)
    stats[tp, 1:2, :] = jnp.sum(csum[...].T, axis=0, keepdims=True)

    def stat_copy(k, slot):
        return pltpu.make_async_remote_copy(
            src_ref=stats.at[slot], dst_ref=stats.at[slot],
            send_sem=stat_send.at[k], recv_sem=stat_recv.at[slot],
            device_id={"tp": lax.rem(tp + k, m)}, device_id_type=MESH,
        )

    @pl.loop(1, m)
    def _(k):
        stat_copy(k, tp).start()

    if wide == dr:
        lax.fori_loop(1, half + 1, own_step, 0)

    share = taploc.shape[2]

    def keep_tap(k, ct, sums):
        taploc[k // share, ct, k % share : k % share + 1, :] = jnp.sum(sums, axis=0, keepdims=True)

    for ct in range(tiles):
        keep_tap(kw, ct, gains[ct])
        for k in range(kw + 1, n * share):
            keep_tap(k, ct, jnp.zeros((8, LANES), F32))

    @pl.loop(1, m)
    def _(k):
        stat_copy(k, lax.rem(tp + m - k, m)).wait_recv()

    totals = stats[0]
    for k in range(1, m):
        totals = totals + stats[k]
    totals = totals / (chans * m)
    mpb[...] = jnp.broadcast_to(totals[0:1, :], (LANES, rows)).T
    mcb[...] = jnp.broadcast_to(totals[1:2, :], (LANES, rows)).T

    def cg_block(b, _):
        at = pl.ds(pl.multiple_of(b * BLOCK, BLOCK), BLOCK)
        for ct in range(tiles):
            cg[ct, at, :] = scaleb[at, :] * (
                agrad[at, lanes(ct)] - mpb[at, :] - centered[ct, at, :] * mcb[at, :]
            )
        return 0

    lax.fori_loop(0, blocks, cg_block, 0)
    back_copy = pltpu.make_async_remote_copy(
        src_ref=cg.at[:, pl.ds(0, halo), :], dst_ref=cg.at[:, pl.ds(rows, halo), :],
        send_sem=back_sem.at[0], recv_sem=back_sem.at[1],
        device_id={"sp": lax.rem(sp + n - 1, n)}, device_id_type=MESH,
    )

    @pl.when(sp > 0)
    def _():
        back_copy.start()

    def z_copy(k, p, slot):
        return pltpu.make_async_remote_copy(
            src_ref=send2.at[p], dst_ref=recv2.at[slot],
            send_sem=z_send.at[k], recv_sem=z_recv.at[slot],
            device_id={"sp": 2 * p + par}, device_id_type=MESH,
        )

    def relay(k, _):
        p = lax.rem(q + k, half)
        y_copy(p).wait_recv()
        send2[p] = (wsum[own_rows(p, par), :] + recv1[p].astype(F32)).astype(BF16)
        z_copy(k, p, q).start()
        return 0

    cut1 = 1 + (half - 1 + 2) // 3
    cut2 = cut1 + (half - cut1 + 1) // 2
    lax.fori_loop(1, cut1, relay, 0)

    span = 16
    for ct in range(tiles):
        def tap_block(b, sums, ct=ct):
            start = pl.multiple_of(b * span, span)
            grad = cg[ct, pl.ds(start, span), :]
            new = []
            for k in range(kw):
                prod = grad * source(gp, sh, k + lead, ct, start, span)
                new.append(sums[k] + jnp.sum(prod.reshape(span // 8, 8, LANES), axis=0))
            return tuple(new)

        sums = lax.fori_loop(
            0, rows // span, tap_block, tuple(jnp.zeros((8, LANES), F32) for _ in range(kw))
        )
        for k in range(kw):
            keep_tap(k, ct, sums[k])

    def tap_copy(k, slot):
        peer = lax.rem(sp + k, n)
        return pltpu.make_async_remote_copy(
            src_ref=taploc.at[peer], dst_ref=tapin.at[slot],
            send_sem=tap_send.at[k], recv_sem=tap_recv.at[slot],
            device_id={"sp": peer}, device_id_type=MESH,
        )

    def all_copy(k, slot):
        return pltpu.make_async_remote_copy(
            src_ref=tapsum.at[slot], dst_ref=tapsum.at[slot],
            send_sem=all_send.at[k], recv_sem=all_recv.at[slot],
            device_id={"sp": lax.rem(sp + k, n)}, device_id_type=MESH,
        )

    @pl.loop(1, n)
    def _(k):
        tap_copy(k, sp).start()

    y_copy(q).start()

    lax.fori_loop(cut1, cut2, relay, 0)

    for at in range(0, rows - 8, BLOCK):
        shifted(cg, sh2, at, min(BLOCK, rows - 8 - at))

    def back_block(b, _):
        start = pl.multiple_of(b * BLOCK, BLOCK)
        at = pl.ds(start, BLOCK)
        for ct in range(tiles):
            total = jnp.zeros((BLOCK, LANES), F32)
            for k in range(kw):
                total = total + taps[k : k + 1, lanes(ct)] * source(
                    cg, sh2, reach - k, ct, start, BLOCK
                )
            sig = jax.nn.sigmoid(gate[at, lanes(ct)].astype(F32))
            value_grad[at, lanes(ct)] = (total * sig).astype(BF16)
            gate_grad[at, lanes(ct)] = (
                total * val[at, lanes(ct)].astype(F32) * sig * (1.0 - sig)
            ).astype(BF16)
        return 0

    lax.fori_loop(0, blocks - 1, back_block, 0)

    @pl.when(sp < n - 1)
    def _():
        back_copy.wait_recv()

    @pl.when(sp == n - 1)
    def _():
        cg[:, rows : rows + halo, :] = jnp.zeros((tiles, halo, LANES), F32)

    shifted(cg, sh2, rows - 8, halo)
    back_block(blocks - 1, 0)

    lax.fori_loop(cut2, half, relay, 0)

    def tap_wait(k, total):
        slot = lax.rem(sp + n - k, n)
        tap_copy(k, slot).wait_recv()
        return total + tapin[slot]

    tapsum[sp] = lax.fori_loop(1, n, tap_wait, taploc[sp])

    @pl.loop(1, n)
    def _(k):
        all_copy(k, sp).start()

    y_copy(q).wait_recv()
    w_out[...] = wsum[own_rows(q, par), :] + recv1[q].astype(F32)

    def z_wait(k, _):
        p = lax.rem(q + half - k, half)
        z_copy(k, p, p).wait_recv()
        w_out[...] += recv2[p].astype(F32)
        return 0

    lax.fori_loop(1, half, z_wait, 0)

    @pl.loop(1, n)
    def _(k):
        all_copy(k, lax.rem(sp + n - k, n)).wait_recv()

    for ct in range(tiles):
        for k in range(kw):
            taps_out[k : k + 1, lanes(ct)] = tapsum[k // share, ct, k % share : k % share + 1, :]
        gain_out[:, lanes(ct)] = tapsum[kw // share, ct, kw % share : kw % share + 1, :]

    @pl.when(sp < n - 1)
    def _():
        halo_copy.wait_send()

    @pl.when(sp > 0)
    def _():
        back_copy.wait_send()

    @pl.loop(1, m)
    def _(k):
        stat_copy(k, tp).wait_send()

    @pl.loop(1, n)
    def _(k):
        tap_copy(k, sp).wait_send()
        all_copy(k, sp).wait_send()

    @pl.loop(0, half)
    def _(k):
        y_copy(k).wait_send()

    @pl.loop(1, half)
    def _(k):
        z_copy(k, lax.rem(q + k, half), q).wait_send()


def finish(count, *refs):
    sem = refs[-1]
    copies = [
        pltpu.make_async_copy(source, target, sem.at[k])
        for k, (source, target) in enumerate(zip(refs[:count], refs[count : 2 * count]))
    ]
    for copy in copies:
        copy.start()
    for copy in copies:
        copy.wait()


def per_device(
    n, m, glu_value, glu_gate, conv_taps, norm_gain, out_weight, norm_mean, norm_scale, out_grad
):
    rows, chans = glu_value.shape
    kw = conv_taps.shape[0]
    depth = out_grad.shape[1]
    dr = depth // n
    half = n // 2
    tiles = chans // LANES
    halo = rup(kw - 1, 16)
    vm = pltpu.VMEM
    dma = pltpu.SemaphoreType.DMA
    whole = pl.BlockSpec(memory_space=pltpu.VMEM)
    far = pl.BlockSpec(memory_space=pltpu.HBM)
    out = pl.pallas_call(
        functools.partial(kernel, n, m, kw),
        out_shape=(
            pltpu.VMEM((rows, chans), BF16),
            pltpu.VMEM((rows, chans), BF16),
            pltpu.VMEM((kw, chans), F32),
            pltpu.VMEM((1, chans), F32),
            pltpu.VMEM((dr, chans), F32),
        ),
        in_specs=[whole] * 6 + [far] * 2,
        out_specs=(whole,) * 5,
        scratch_shapes=[
            vm((kw, chans), F32),
            vm((rows, depth), BF16),
            vm((depth, chans), BF16),
            vm((tiles, rows + halo, LANES), F32),
            vm((7, tiles, rows + halo, LANES), F32),
            vm((tiles, rows + halo, LANES), F32),
            vm((7, tiles, rows + halo, LANES), F32),
            vm((tiles, rows, LANES), F32),
            vm((tiles, rows, LANES), F32),
            vm((rows, chans), BF16),
            vm((rows, chans), F32),
            vm((rows, LANES), F32),
            vm((rows, LANES), F32),
            vm((rows, LANES), F32),
            vm((rows, LANES), F32),
            vm((rows, LANES), F32),
            vm((rows, LANES), F32),
            vm((halo, chans), BF16),
            vm((halo, chans), BF16),
            vm((m, 2, rows), F32),
            vm((n, tiles, rup(kw + 1, n) // n, LANES), F32),
            vm((n, tiles, rup(kw + 1, n) // n, LANES), F32),
            vm((n, tiles, rup(kw + 1, n) // n, LANES), F32),
            vm((depth, chans), F32),
            vm((depth, chans), BF16),
            vm((half, dr, chans), BF16),
            vm((half, dr, chans), BF16),
            vm((half, dr, chans), BF16),
            dma((2,)), dma((2,)), dma((2,)),
            dma((m,)), dma((m,)), dma((n,)), dma((n,)), dma((n,)), dma((n,)),
            dma((half,)), dma((half,)), dma((half,)), dma((half,)),
        ],
        compiler_params=pltpu.CompilerParams(
            collective_id=0, has_side_effects=True, vmem_limit_bytes=VMEM_LIMIT
        ),
    )(*[
        pltpu.with_memory_space_constraint(x, pltpu.HBM) for x in (
        glu_value, glu_gate, conv_taps, norm_gain[None, :],
        norm_mean[None, :], norm_scale[None, :], out_grad, out_weight,
    )])
    out = pl.pallas_call(
        functools.partial(finish, len(out)),
        out_shape=tuple(jax.ShapeDtypeStruct(x.shape, x.dtype) for x in out),
        in_specs=[whole] * len(out),
        out_specs=(pl.BlockSpec(memory_space=pltpu.HBM),) * len(out),
        scratch_shapes=[pltpu.SemaphoreType.DMA((len(out),))],
        compiler_params=pltpu.CompilerParams(vmem_limit_bytes=2 * 1024 * 1024),
    )(*out)
    value_grad, gate_grad, taps_grad, gain_grad, weight_grad = out
    return value_grad, gate_grad, taps_grad, gain_grad[0], weight_grad


def solution(mesh):
    placed = (
        P("sp", "tp"), P("sp", "tp"), P(None, "tp"), P("tp"),
        P(None, "tp"), P("sp"), P("sp"), P("sp", None),
    )
    return jax.shard_map(
        functools.partial(per_device, mesh.shape["sp"], mesh.shape["tp"]),
        mesh=mesh,
        in_specs=placed,
        out_specs=(P("sp", "tp"), P("sp", "tp"), P(None, "tp"), P("tp"), P("sp", "tp")),
        check_vma=False,
    )
```

```python
import functools

import jax
import jax.numpy as jnp
from jax import lax
from jax.experimental import pallas as pl
from jax.experimental.pallas import tpu as pltpu
from jax.sharding import PartitionSpec as P

MESH = pl.DeviceIdType.MESH
F32 = jnp.float32
BF16 = jnp.bfloat16
LANES = 128
VMEM_LIMIT = 30 * 1024 * 1024
BLOCK = 64


def rup(value, unit):
    return -(-value // unit) * unit


def kernel(
    n, m, kw,
    val, gate, taps_in, gain, mean_row, scale_row, og_hbm, ow_hbm,
    value_grad, gate_grad, taps_out, gain_out, w_out,
    taps, og, ow, gp, sh, cg, sh2, centered, slope, act, agrad, psum, csum, meanb, scaleb,
    mpb, mcb, halo_out, halo_in, stats, taploc, tapin, tapsum, wsum, wbf, recv1, send2, recv2,
    load_sem, halo_sem, back_sem, stat_send, stat_recv, tap_send, tap_recv, all_send, all_recv,
    y_send, y_recv, z_send, z_recv,
):
    rows, chans = val.shape
    tiles = chans // LANES
    depth = og.shape[1]
    dr = depth // n
    half = n // 2
    reach = kw - 1
    halo = halo_out.shape[0]
    lead = halo - reach
    blocks = rows // BLOCK
    sp = lax.axis_index("sp")
    tp = lax.axis_index("tp")
    par = lax.rem(sp, 2)
    q = lax.div(sp, 2)
    partner = sp + 1 - 2 * par

    load_og = pltpu.make_async_copy(og_hbm, og, load_sem.at[0])
    load_ow = pltpu.make_async_copy(ow_hbm, ow, load_sem.at[1])
    load_og.start()
    load_ow.start()

    barrier = pltpu.get_barrier_semaphore()

    @pl.loop(1, n)
    def _(k):
        pl.semaphore_signal(
            barrier, inc=1, device_id={"sp": lax.rem(sp + k, n)}, device_id_type=MESH
        )

    @pl.loop(1, m)
    def _(k):
        pl.semaphore_signal(
            barrier, inc=1, device_id={"tp": lax.rem(tp + k, m)}, device_id_type=MESH
        )

    def lanes(ct):
        return slice(ct * LANES, (ct + 1) * LANES)

    taps[...] = taps_in[...].astype(F32)
    tail = slice(rows - halo, rows)
    tail_sig = jax.nn.sigmoid(gate[tail, :].astype(F32))
    halo_out[...] = (val[tail, :].astype(F32) * tail_sig).astype(BF16)

    def gate_block(b, _):
        at = pl.ds(pl.multiple_of(b * BLOCK, BLOCK), BLOCK)
        to = pl.ds(pl.multiple_of(b * BLOCK + halo, 16), BLOCK)
        for ct in range(tiles):
            sig = jax.nn.sigmoid(gate[at, lanes(ct)].astype(F32))
            gp[ct, to, :] = (val[at, lanes(ct)].astype(F32) * sig).astype(BF16).astype(F32)
        return 0

    lax.fori_loop(0, blocks, gate_block, 0)

    load_og.wait()
    load_ow.wait()
    slab = min(rows, 128)

    def grad_block(b, _):
        at = pl.ds(pl.multiple_of(b * slab, slab), slab)
        agrad[at, :] = jnp.dot(og[at, :], ow[...], preferred_element_type=F32)
        return 0

    lax.fori_loop(0, rows // slab, grad_block, 0)

    pl.semaphore_wait(barrier, n - 1 + m - 1)

    halo_copy = pltpu.make_async_remote_copy(
        src_ref=halo_out, dst_ref=halo_in,
        send_sem=halo_sem.at[0], recv_sem=halo_sem.at[1],
        device_id={"sp": lax.rem(sp + 1, n)}, device_id_type=MESH,
    )

    @pl.when(sp < n - 1)
    def _():
        halo_copy.start()

    def shifted(src, dst, begin, count):
        for ct in range(tiles):
            for r in range(1, 8):
                dst[r - 1, ct, begin : begin + count, :] = src[ct, begin + r : begin + r + count, :]

    for at in range(halo, rows + halo - 8, BLOCK):
        shifted(gp, sh, at, min(BLOCK, rows + halo - 8 - at))
    meanb[...] = jnp.broadcast_to(mean_row[...], (LANES, rows)).T
    scaleb[...] = jnp.broadcast_to(scale_row[...], (LANES, rows)).T

    def source(base_ref, copies, shift, ct, start, count):
        r, base = shift % 8, shift - shift % 8
        at = pl.ds(pl.multiple_of(start + base, 8), count)
        if r == 0:
            return base_ref[ct, at, :]
        return copies[r - 1, ct, at, :]

    def conv_block(b, _):
        start = pl.multiple_of(b * BLOCK, BLOCK)
        at = pl.ds(start, BLOCK)
        for ct in range(tiles):
            conv = jnp.zeros((BLOCK, LANES), F32)
            for k in range(kw):
                conv = conv + taps[k : k + 1, lanes(ct)] * source(gp, sh, k + lead, ct, start, BLOCK)
            cen = (conv - meanb[at, :]) * scaleb[at, :]
            nor = cen * gain[:, lanes(ct)]
            sig = jax.nn.sigmoid(nor)
            centered[ct, at, :] = cen
            slope[ct, at, :] = sig * (1.0 + nor * (1.0 - sig))
            act[at, lanes(ct)] = (nor * sig).astype(BF16)
        return 0

    lax.fori_loop(1, blocks, conv_block, 0)

    @pl.when(sp > 0)
    def _():
        halo_copy.wait_recv()
        for ct in range(tiles):
            gp[ct, 0:halo, :] = halo_in[:, lanes(ct)].astype(F32)

    @pl.when(sp == 0)
    def _():
        for ct in range(tiles):
            gp[ct, 0:halo, :] = jnp.zeros((halo, LANES), F32)

    shifted(gp, sh, 0, halo)
    conv_block(0, 0)

    wide = max(dr, min(depth, 256))

    def w_tile(start):
        start = pl.multiple_of(start, wide)
        part = lax.dot_general(
            og[:, pl.ds(start, wide)], act[...], (((0,), (0,)), ((), ())),
            preferred_element_type=F32,
        )
        wsum[pl.ds(start, wide), :] = part
        wbf[pl.ds(start, wide), :] = part.astype(BF16)

    def own_rows(p, side):
        return pl.ds(pl.multiple_of((2 * p + side) * dr, dr), dr)

    def y_copy(p):
        return pltpu.make_async_remote_copy(
            src_ref=wbf.at[own_rows(p, 1 - par), :], dst_ref=recv1.at[p],
            send_sem=y_send.at[p], recv_sem=y_recv.at[p],
            device_id={"sp": partner}, device_id_type=MESH,
        )

    def partner_step(k, _):
        p = lax.rem(q + k, half)
        w_tile((2 * p + 1 - par) * dr)
        y_copy(p).start()
        return 0

    def own_step(k, _):
        w_tile((2 * lax.rem(q + k, half) + par) * dr)
        return 0

    if wide == dr:
        lax.fori_loop(1, half, partner_step, 0)
        w_tile((2 * q + 1 - par) * dr)
    else:
        def tile_step(j, _):
            w_tile(j * wide)
            return 0

        lax.fori_loop(0, depth // wide, tile_step, 0)

        def send_step(k, _):
            y_copy(lax.rem(q + k, half)).start()
            return 0

        lax.fori_loop(1, half, send_step, 0)

    def stat_block(b, sums):
        at = pl.ds(pl.multiple_of(b * BLOCK, BLOCK), BLOCK)
        plain = jnp.zeros((BLOCK, LANES), F32)
        cross = jnp.zeros((BLOCK, LANES), F32)
        new = []
        for ct in range(tiles):
            cen = centered[ct, at, :]
            ngrad = agrad[at, lanes(ct)] * slope[ct, at, :]
            scaled = ngrad * gain[:, lanes(ct)]
            agrad[at, lanes(ct)] = scaled
            plain = plain + scaled
            cross = cross + scaled * cen
            new.append(sums[ct] + jnp.sum((ngrad * cen).reshape(BLOCK // 8, 8, LANES), axis=0))
        psum[at, :] = plain
        csum[at, :] = cross
        return tuple(new)

    gains = lax.fori_loop(
        0, blocks, stat_block, tuple(jnp.zeros((8, LANES), F32) for _ in range(tiles))
    )
    stats[tp, 0:1, :] = jnp.sum(psum[...].T, axis=0, keepdims=True)
    stats[tp, 1:2, :] = jnp.sum(csum[...].T, axis=0, keepdims=True)

    def stat_copy(k, slot):
        return pltpu.make_async_remote_copy(
            src_ref=stats.at[slot], dst_ref=stats.at[slot],
            send_sem=stat_send.at[k], recv_sem=stat_recv.at[slot],
            device_id={"tp": lax.rem(tp + k, m)}, device_id_type=MESH,
        )

    @pl.loop(1, m)
    def _(k):
        stat_copy(k, tp).start()

    if wide == dr:
        lax.fori_loop(1, half + 1, own_step, 0)

    share = taploc.shape[2]

    def keep_tap(k, ct, sums):
        taploc[k // share, ct, k % share : k % share + 1, :] = jnp.sum(sums, axis=0, keepdims=True)

    for ct in range(tiles):
        keep_tap(kw, ct, gains[ct])
        for k in range(kw + 1, n * share):
            keep_tap(k, ct, jnp.zeros((8, LANES), F32))

    @pl.loop(1, m)
    def _(k):
        stat_copy(k, lax.rem(tp + m - k, m)).wait_recv()

    totals = stats[0]
    for k in range(1, m):
        totals = totals + stats[k]
    totals = totals / (chans * m)
    mpb[...] = jnp.broadcast_to(totals[0:1, :], (LANES, rows)).T
    mcb[...] = jnp.broadcast_to(totals[1:2, :], (LANES, rows)).T

    def cg_block(b, _):
        at = pl.ds(pl.multiple_of(b * BLOCK, BLOCK), BLOCK)
        for ct in range(tiles):
            cg[ct, at, :] = scaleb[at, :] * (
                agrad[at, lanes(ct)] - mpb[at, :] - centered[ct, at, :] * mcb[at, :]
            )
        return 0

    lax.fori_loop(0, blocks, cg_block, 0)
    back_copy = pltpu.make_async_remote_copy(
        src_ref=cg.at[:, pl.ds(0, halo), :], dst_ref=cg.at[:, pl.ds(rows, halo), :],
        send_sem=back_sem.at[0], recv_sem=back_sem.at[1],
        device_id={"sp": lax.rem(sp + n - 1, n)}, device_id_type=MESH,
    )

    @pl.when(sp > 0)
    def _():
        back_copy.start()

    def z_copy(k, p, slot):
        return pltpu.make_async_remote_copy(
            src_ref=send2.at[p], dst_ref=recv2.at[slot],
            send_sem=z_send.at[k], recv_sem=z_recv.at[slot],
            device_id={"sp": 2 * p + par}, device_id_type=MESH,
        )

    def relay(k, _):
        p = lax.rem(q + k, half)
        y_copy(p).wait_recv()
        send2[p] = (wsum[own_rows(p, par), :] + recv1[p].astype(F32)).astype(BF16)
        z_copy(k, p, q).start()
        return 0

    cut1 = 1 + (half - 1 + 2) // 3
    cut2 = cut1 + (half - cut1 + 1) // 2
    lax.fori_loop(1, cut1, relay, 0)

    span = 16
    for ct in range(tiles):
        def tap_block(b, sums, ct=ct):
            start = pl.multiple_of(b * span, span)
            grad = cg[ct, pl.ds(start, span), :]
            new = []
            for k in range(kw):
                prod = grad * source(gp, sh, k + lead, ct, start, span)
                new.append(sums[k] + jnp.sum(prod.reshape(span // 8, 8, LANES), axis=0))
            return tuple(new)

        sums = lax.fori_loop(
            0, rows // span, tap_block, tuple(jnp.zeros((8, LANES), F32) for _ in range(kw))
        )
        for k in range(kw):
            keep_tap(k, ct, sums[k])

    def tap_copy(k, slot):
        peer = lax.rem(sp + k, n)
        return pltpu.make_async_remote_copy(
            src_ref=taploc.at[peer], dst_ref=tapin.at[slot],
            send_sem=tap_send.at[k], recv_sem=tap_recv.at[slot],
            device_id={"sp": peer}, device_id_type=MESH,
        )

    def all_copy(k, slot):
        return pltpu.make_async_remote_copy(
            src_ref=tapsum.at[slot], dst_ref=tapsum.at[slot],
            send_sem=all_send.at[k], recv_sem=all_recv.at[slot],
            device_id={"sp": lax.rem(sp + k, n)}, device_id_type=MESH,
        )

    @pl.loop(1, n)
    def _(k):
        tap_copy(k, sp).start()

    y_copy(q).start()

    lax.fori_loop(cut1, cut2, relay, 0)

    for at in range(0, rows - 8, BLOCK):
        shifted(cg, sh2, at, min(BLOCK, rows - 8 - at))

    def back_block(b, _):
        start = pl.multiple_of(b * BLOCK, BLOCK)
        at = pl.ds(start, BLOCK)
        for ct in range(tiles):
            total = jnp.zeros((BLOCK, LANES), F32)
            for k in range(kw):
                total = total + taps[k : k + 1, lanes(ct)] * source(
                    cg, sh2, reach - k, ct, start, BLOCK
                )
            sig = jax.nn.sigmoid(gate[at, lanes(ct)].astype(F32))
            value_grad[at, lanes(ct)] = (total * sig).astype(BF16)
            gate_grad[at, lanes(ct)] = (
                total * val[at, lanes(ct)].astype(F32) * sig * (1.0 - sig)
            ).astype(BF16)
        return 0

    lax.fori_loop(0, blocks - 1, back_block, 0)

    @pl.when(sp < n - 1)
    def _():
        back_copy.wait_recv()

    @pl.when(sp == n - 1)
    def _():
        cg[:, rows : rows + halo, :] = jnp.zeros((tiles, halo, LANES), F32)

    shifted(cg, sh2, rows - 8, halo)
    back_block(blocks - 1, 0)

    lax.fori_loop(cut2, half, relay, 0)

    def tap_wait(k, total):
        slot = lax.rem(sp + n - k, n)
        tap_copy(k, slot).wait_recv()
        return total + tapin[slot]

    tapsum[sp] = lax.fori_loop(1, n, tap_wait, taploc[sp])

    @pl.loop(1, n)
    def _(k):
        all_copy(k, sp).start()

    y_copy(q).wait_recv()
    w_out[...] = wsum[own_rows(q, par), :] + recv1[q].astype(F32)

    def z_wait(k, _):
        p = lax.rem(q + half - k, half)
        z_copy(k, p, p).wait_recv()
        w_out[...] += recv2[p].astype(F32)
        return 0

    lax.fori_loop(1, half, z_wait, 0)

    @pl.loop(1, n)
    def _(k):
        all_copy(k, lax.rem(sp + n - k, n)).wait_recv()

    for ct in range(tiles):
        for k in range(kw):
            taps_out[k : k + 1, lanes(ct)] = tapsum[k // share, ct, k % share : k % share + 1, :]
        gain_out[:, lanes(ct)] = tapsum[kw // share, ct, kw % share : kw % share + 1, :]

    @pl.when(sp < n - 1)
    def _():
        halo_copy.wait_send()

    @pl.when(sp > 0)
    def _():
        back_copy.wait_send()

    @pl.loop(1, m)
    def _(k):
        stat_copy(k, tp).wait_send()

    @pl.loop(1, n)
    def _(k):
        tap_copy(k, sp).wait_send()
        all_copy(k, sp).wait_send()

    @pl.loop(0, half)
    def _(k):
        y_copy(k).wait_send()

    @pl.loop(1, half)
    def _(k):
        z_copy(k, lax.rem(q + k, half), q).wait_send()


def pair_kernel(
    n, m, kw,
    val_hbm, gate_hbm, taps_hbm, gain_hbm, mean_hbm, scale_hbm, og_hbm, ow_hbm,
    value_grad, gate_grad, taps_out, gain_out, w_out,
    val, gate, taps_in, gain, mean_row, scale_row, og, ow,
    taps, gp, cg, centered, slope, act, actt, agrad, psum, csum, meanb, scaleb, mpb, mcb,
    halo_out, halo_in, stats, taploc, tappair, tapz, wsum, ysend, yrecv, zsend, zrecv, xrecv,
    zfown, zfsend, zfside, zfx, zfysend, zfyrecv, whole,
    load_sem, halo_sem, back_sem, stat_send, stat_recv, pair_sem, tap_send, tap_recv,
    y_send, y_recv, z_send, z_recv, x_recv, zf_send, zf_recv, zfy_sem, hop,
):
    rows, chans = val.shape
    tiles = chans // LANES
    depth = og.shape[1]
    dr = depth // n
    half = n // 2
    reach = kw - 1
    halo = halo_out.shape[0]
    lead = halo - reach
    blocks = rows // BLOCK
    zf = chans // 4
    cut = (chans - zf) // 2
    sp = lax.axis_index("sp")
    tp = lax.axis_index("tp")
    par = lax.rem(sp, 2)
    q = lax.div(sp, 2)
    partner = sp + 1 - 2 * par
    low = q < 2
    outer = jnp.logical_or(q == 0, q == 3)
    sib = q + 1 - 2 * lax.rem(q, 2)

    barrier = pltpu.get_barrier_semaphore()

    up, down = q < half - 1, q > 0
    skew = jnp.where(par == 1, sp + 1, sp - 1)
    has_skew = jnp.logical_and(skew >= 0, skew < n)

    def greet(other):
        pl.semaphore_signal(barrier, inc=1, device_id={"sp": other}, device_id_type=MESH)

    greet(partner)

    @pl.when(up)
    def _():
        greet(sp + 2)

    @pl.when(down)
    def _():
        greet(sp - 2)

    @pl.when(has_skew)
    def _():
        greet(skew)

    @pl.loop(1, m)
    def _(k):
        pl.semaphore_signal(
            barrier, inc=1, device_id={"tp": lax.rem(tp + k, m)}, device_id_type=MESH
        )

    loads = [
        pltpu.make_async_copy(source, target, load_sem.at[k])
        for k, (source, target) in enumerate((
            (gate_hbm, gate), (val_hbm, val), (taps_hbm, taps_in), (mean_hbm, mean_row),
            (scale_hbm, scale_row), (gain_hbm, gain), (og_hbm, og), (ow_hbm, ow),
        ))
    ]
    for load in loads:
        load.start()

    def lanes(ct):
        return slice(ct * LANES, (ct + 1) * LANES)

    for load in loads[:6]:
        load.wait()
    tail = slice(rows - halo, rows)
    tail_sig = jax.nn.sigmoid(gate[tail, :].astype(F32))
    halo_out[...] = (val[tail, :].astype(F32) * tail_sig).astype(BF16)
    taps[...] = taps_in[...].astype(F32)

    def gate_block(b, _):
        at = pl.ds(pl.multiple_of(b * BLOCK, BLOCK), BLOCK)
        to = pl.ds(pl.multiple_of(b * BLOCK + halo, 16), BLOCK)
        for ct in range(tiles):
            sig = jax.nn.sigmoid(gate[at, lanes(ct)].astype(F32))
            gp[ct, to, :] = (val[at, lanes(ct)].astype(F32) * sig).astype(BF16).astype(F32)
        return 0

    lax.fori_loop(0, blocks, gate_block, 0)
    near = up.astype(jnp.int32) + down.astype(jnp.int32) + has_skew.astype(jnp.int32)
    pl.semaphore_wait(barrier, m + near)

    halo_copy = pltpu.make_async_remote_copy(
        src_ref=halo_out, dst_ref=halo_in,
        send_sem=halo_sem.at[0], recv_sem=halo_sem.at[1],
        device_id={"sp": lax.rem(sp + 1, n)}, device_id_type=MESH,
    )

    @pl.when(sp < n - 1)
    def _():
        halo_copy.start()

    def tell(r):
        @pl.when(up)
        def _():
            pl.semaphore_signal(
                hop.at[r, 0], inc=1, device_id={"sp": sp + 2}, device_id_type=MESH
            )

        @pl.when(down)
        def _():
            pl.semaphore_signal(
                hop.at[r, 1], inc=1, device_id={"sp": sp - 2}, device_id_type=MESH
            )

    def hear(r):
        @pl.when(down)
        def _():
            pl.semaphore_wait(hop.at[r, 0], 1)

        @pl.when(up)
        def _():
            pl.semaphore_wait(hop.at[r, 1], 1)

    tell(0)
    meanb[...] = jnp.broadcast_to(mean_row[...], (LANES, rows)).T
    scaleb[...] = jnp.broadcast_to(scale_row[...], (LANES, rows)).T
    def source(ref, shift, ct, start, count):
        return ref[ct, pl.ds(start + shift, count), :]

    def conv_block(b, _):
        start = pl.multiple_of(b * BLOCK, BLOCK)
        at = pl.ds(start, BLOCK)
        for ct in range(tiles):
            conv = jnp.zeros((BLOCK, LANES), F32)
            for k in range(kw):
                conv = conv + taps[k : k + 1, lanes(ct)] * source(gp, k + lead, ct, start, BLOCK)
            cen = (conv - meanb[at, :]) * scaleb[at, :]
            nor = cen * gain[:, lanes(ct)]
            sig = jax.nn.sigmoid(nor)
            centered[ct, at, :] = cen
            slope[ct, at, :] = sig * (1.0 + nor * (1.0 - sig))
            act[at, lanes(ct)] = (nor * sig).astype(BF16)
        return 0

    def turn(chunk):
        at = slice(chunk * LANES, (chunk + 1) * LANES)
        for ct in range(tiles):
            actt[lanes(ct), at] = act[at, lanes(ct)].T

    lax.fori_loop(1, blocks, conv_block, 0)
    for chunk in range(1, rows // LANES):
        turn(chunk)

    for load in loads[6:]:
        load.wait()
    slab = min(rows, 256)

    def grad_block(b, _):
        at = pl.ds(pl.multiple_of(b * slab, slab), slab)
        agrad[at, :] = jnp.dot(og[at, :], ow[...], preferred_element_type=F32)
        return 0

    lax.fori_loop(0, rows // slab, grad_block, 0)

    def stat_block(b, sums):
        at = pl.ds(pl.multiple_of(b * BLOCK, BLOCK), BLOCK)
        plain = jnp.zeros((BLOCK, LANES), F32)
        cross = jnp.zeros((BLOCK, LANES), F32)
        new = []
        for ct in range(tiles):
            cen = centered[ct, at, :]
            ngrad = agrad[at, lanes(ct)] * slope[ct, at, :]
            scaled = ngrad * gain[:, lanes(ct)]
            agrad[at, lanes(ct)] = scaled
            plain = plain + scaled
            cross = cross + scaled * cen
            new.append(sums[ct] + jnp.sum((ngrad * cen).reshape(BLOCK // 8, 8, LANES), axis=0))
        psum[at, :] = plain
        csum[at, :] = cross
        return tuple(new)

    gains = lax.fori_loop(
        1, blocks, stat_block, tuple(jnp.zeros((8, LANES), F32) for _ in range(tiles))
    )

    hear(0)
    tell(1)

    @pl.when(sp > 0)
    def _():
        halo_copy.wait_recv()
        for ct in range(tiles):
            gp[ct, 0:halo, :] = halo_in[:, lanes(ct)].astype(F32)

    @pl.when(sp == 0)
    def _():
        for ct in range(tiles):
            gp[ct, 0:halo, :] = jnp.zeros((halo, LANES), F32)

    conv_block(0, 0)
    turn(0)
    gains = stat_block(0, gains)
    stats[tp, 0:1, :] = jnp.sum(psum[...].T, axis=0, keepdims=True)
    stats[tp, 1:2, :] = jnp.sum(csum[...].T, axis=0, keepdims=True)

    def stat_copy(k, slot):
        return pltpu.make_async_remote_copy(
            src_ref=stats.at[slot], dst_ref=stats.at[slot],
            send_sem=stat_send.at[k], recv_sem=stat_recv.at[slot],
            device_id={"tp": lax.rem(tp + k, m)}, device_id_type=MESH,
        )

    @pl.loop(1, m)
    def _(k):
        stat_copy(k, tp).start()

    def piece(i):
        far = (i, i - 1)
        near_first = jnp.where(low, half - 1 - far[1], far[1]) if i else sib
        far_first = jnp.where(low, half - 1 - far[0], far[0]) if i < 2 else sib
        return jnp.where(outer, far_first, near_first)

    order = [piece(0), piece(1), piece(2), q]
    parts = (slice(0, cut), slice(cut, 2 * cut))
    last = slice(2 * cut, chans)

    def product(block):
        at = pl.ds(pl.multiple_of(block * dr, LANES), dr)
        return jnp.dot(actt[...], og[:, at], preferred_element_type=F32)

    def y_copy(p, s):
        return pltpu.make_async_remote_copy(
            src_ref=ysend.at[p, s], dst_ref=yrecv.at[p, s],
            send_sem=y_send.at[p, s], recv_sem=y_recv.at[p, s],
            device_id={"sp": partner}, device_id_type=MESH,
        )

    def away(p):
        part = product(2 * p + 1 - par)
        for s in range(2):
            ysend[p, s] = part[parts[s], :].astype(BF16)
        zfown[p, 0] = part[last, :]

    def home(p):
        part = product(2 * p + par)
        for s in range(2):
            wsum[p, s] = part[parts[s], :]
        zfown[p, 1] = part[last, :]

    ahead = lax.rem(tp, 2) == 0

    def send(cond, halves):
        @pl.when(cond)
        def _():
            for i, s in halves:
                y_copy(order[i], s).start()

    def zf_copy(i, peer, target, sem):
        return pltpu.make_async_remote_copy(
            src_ref=zfsend.at[i], dst_ref=target,
            send_sem=zf_send.at[i], recv_sem=sem,
            device_id={"sp": 2 * peer + par}, device_id_type=MESH,
        )

    def zf_side(i, p):
        return zf_copy(i, sib, zfside.at[p], zf_recv.at[p])

    def zf_cross(i, p):
        return zf_copy(i, p, zfx, x_recv.at[2])

    def zf_first(i):
        zfsend[i] = zfown[order[i]].astype(BF16)
        zf_side(i, order[i]).start()

    def zf_relay(i):
        zf_side(0, order[i]).wait_recv()
        zfsend[i] = (zfown[order[i]] + zfside[order[i]].astype(F32)).astype(BF16)
        zf_cross(i, order[i]).start()

    inner = jnp.logical_not(outer)
    away(order[0])
    send(ahead, ((0, 0), (0, 1)))
    away(order[1])
    send(ahead, ((1, 0), (1, 1)))
    home(order[0])
    zf_first(0)
    home(order[1])

    @pl.when(outer)
    def _():
        zf_first(1)

    away(order[2])
    home(order[2])

    @pl.when(outer)
    def _():
        zf_first(2)

    send(jnp.logical_not(ahead), ((0, 0), (0, 1)))
    away(order[3])
    home(order[3])

    @pl.loop(1, m)
    def _(k):
        stat_copy(k, lax.rem(tp + m - k, m)).wait_recv()

    totals = stats[0]
    for k in range(1, m):
        totals = totals + stats[k]
    totals = totals / (chans * m)
    mpb[...] = jnp.broadcast_to(totals[0:1, :], (LANES, rows)).T
    mcb[...] = jnp.broadcast_to(totals[1:2, :], (LANES, rows)).T

    def cg_block(b, _):
        at = pl.ds(pl.multiple_of(b * BLOCK, BLOCK), BLOCK)
        for ct in range(tiles):
            cg[ct, at, :] = scaleb[at, :] * (
                agrad[at, lanes(ct)] - mpb[at, :] - centered[ct, at, :] * mcb[at, :]
            )
        return 0

    lax.fori_loop(0, blocks, cg_block, 0)
    back_copy = pltpu.make_async_remote_copy(
        src_ref=cg.at[:, pl.ds(0, halo), :], dst_ref=cg.at[:, pl.ds(rows, halo), :],
        send_sem=back_sem.at[0], recv_sem=back_sem.at[1],
        device_id={"sp": lax.rem(sp + n - 1, n)}, device_id_type=MESH,
    )

    @pl.when(sp > 0)
    def _():
        back_copy.start()

    def side_copy(i, s):
        return pltpu.make_async_remote_copy(
            src_ref=zsend.at[i, s], dst_ref=zrecv.at[order[i], s],
            send_sem=z_send.at[i, s], recv_sem=z_recv.at[order[i], s],
            device_id={"sp": 2 * sib + par}, device_id_type=MESH,
        )

    def side_wait(p, s):
        pltpu.make_async_remote_copy(
            src_ref=zsend.at[0, s], dst_ref=zrecv.at[p, s],
            send_sem=z_send.at[0, s], recv_sem=z_recv.at[p, s],
            device_id={"sp": 2 * sib + par}, device_id_type=MESH,
        ).wait_recv()

    def cross_copy(i, s):
        return pltpu.make_async_remote_copy(
            src_ref=zsend.at[i, s], dst_ref=xrecv.at[s],
            send_sem=z_send.at[i, s], recv_sem=x_recv.at[s],
            device_id={"sp": 2 * order[i] + par}, device_id_type=MESH,
        )

    def relay(i, s):
        p = order[i]
        y_copy(p, s).wait_recv()
        if i == 0:
            zsend[i, s] = (wsum[p, s] + yrecv[p, s].astype(F32)).astype(BF16)
            side_copy(i, s).start()
            return

        @pl.when(outer)
        def _():
            zsend[i, s] = (wsum[p, s] + yrecv[p, s].astype(F32)).astype(BF16)
            side_copy(i, s).start()

        @pl.when(jnp.logical_not(outer))
        def _():
            own = wsum[p, s] + yrecv[p, s].astype(F32)
            side_wait(p, s)
            zsend[i, s] = (own + zrecv[p, s].astype(F32)).astype(BF16)
            cross_copy(i, s).start()

    hear(1)

    def keep_tap(k, ct, sums):
        taploc[ct, k : k + 1, :] = jnp.sum(sums, axis=0, keepdims=True)

    span = 16

    def tap_tile(ct):
        def tap_block(b, sums):
            start = pl.multiple_of(b * span, span)
            grad = cg[ct, pl.ds(start, span), :]
            new = []
            for k in range(kw):
                prod = grad * source(gp, k + lead, ct, start, span)
                new.append(sums[k] + jnp.sum(prod.reshape(span // 8, 8, LANES), axis=0))
            return tuple(new)

        sums = lax.fori_loop(
            0, rows // span, tap_block, tuple(jnp.zeros((8, LANES), F32) for _ in range(kw))
        )
        for k in range(kw):
            keep_tap(k, ct, sums[k])
        keep_tap(kw, ct, gains[ct])

    for ct in range(tiles):
        tap_tile(ct)

    pair_copy = pltpu.make_async_remote_copy(
        src_ref=taploc, dst_ref=tappair, send_sem=pair_sem.at[0], recv_sem=pair_sem.at[1],
        device_id={"sp": partner}, device_id_type=MESH,
    )
    pair_copy.start()
    send(ahead, [(i, s) for i in (2, 3) for s in range(2)])
    send(jnp.logical_not(ahead), [(i, s) for i in (1, 2, 3) for s in range(2)])
    @pl.when(inner)
    def _():
        zf_relay(1)

    relay(0, 0)
    @pl.when(inner)
    def _():
        zf_relay(2)

    relay(0, 1)
    early = jnp.logical_and(outer, ahead)

    @pl.when(early)
    def _():
        relay(1, 0)
        relay(1, 1)


    def back_block(b, _):
        start = pl.multiple_of(b * BLOCK, BLOCK)
        at = pl.ds(start, BLOCK)
        for ct in range(tiles):
            total = jnp.zeros((BLOCK, LANES), F32)
            for k in range(kw):
                total = total + taps[k : k + 1, lanes(ct)] * source(cg, reach - k, ct, start, BLOCK)
            sig = jax.nn.sigmoid(gate[at, lanes(ct)].astype(F32))
            value_grad[at, lanes(ct)] = (total * sig).astype(BF16)
            gate_grad[at, lanes(ct)] = (
                total * val[at, lanes(ct)].astype(F32) * sig * (1.0 - sig)
            ).astype(BF16)
        return 0

    lax.fori_loop(0, blocks - 1, back_block, 0)

    pair_copy.wait_recv()
    tapz[q] = taploc[...] + tappair[...]

    def tap_copy(k, slot):
        return pltpu.make_async_remote_copy(
            src_ref=tapz.at[slot], dst_ref=tapz.at[slot],
            send_sem=tap_send.at[k], recv_sem=tap_recv.at[slot],
            device_id={"sp": 2 * lax.rem(q + k, half) + par}, device_id_type=MESH,
        )

    @pl.loop(1, half)
    def _(k):
        tap_copy(k, q).start()

    @pl.when(jnp.logical_not(early))
    def _():
        relay(1, 0)

    @pl.when(jnp.logical_not(early))
    def _():
        relay(1, 1)

    relay(2, 0)
    @pl.when(sp < n - 1)
    def _():
        back_copy.wait_recv()

    @pl.when(sp == n - 1)
    def _():
        cg[:, rows : rows + halo, :] = jnp.zeros((tiles, halo, LANES), F32)

    back_block(blocks - 1, 0)

    relay(2, 1)

    zf_side(0, q).wait_recv()
    zf_cross(0, q).wait_recv()
    for k in range(2):
        zfown[q, k] += zfside[q, k].astype(F32) + zfx[k].astype(F32)
    zfysend[...] = zfown[q, 0].astype(BF16)
    zf_back = pltpu.make_async_remote_copy(
        src_ref=zfysend, dst_ref=zfyrecv, send_sem=zfy_sem.at[0], recv_sem=zfy_sem.at[1],
        device_id={"sp": partner}, device_id_type=MESH,
    )
    zf_back.start()

    for s in range(2):
        y_copy(q, s).wait_recv()
        wsum[q, s] += yrecv[q, s].astype(F32)
    @pl.loop(1, half)
    def _(k):
        tap_copy(k, lax.rem(q + half - k, half)).wait_recv()

    for ct in range(tiles):
        total = tapz[0, ct]
        for k in range(1, half):
            total = total + tapz[k, ct]
        taps_out[:, lanes(ct)] = total[0:kw]
        gain_out[:, lanes(ct)] = total[kw : kw + 1]

    for s in range(2):
        side_wait(q, s)
        pltpu.make_async_remote_copy(
            src_ref=zsend.at[0, s], dst_ref=xrecv.at[s],
            send_sem=z_send.at[0, s], recv_sem=x_recv.at[s],
            device_id={"sp": partner}, device_id_type=MESH,
        ).wait_recv()
        whole[parts[s], :] = wsum[q, s] + zrecv[q, s].astype(F32) + xrecv[s].astype(F32)
    zf_back.wait_recv()
    whole[last, :] = zfown[q, 1] + zfyrecv[...].astype(F32)
    w_out[...] = whole[...].T

    @pl.when(sp < n - 1)
    def _():
        halo_copy.wait_send()

    @pl.when(sp > 0)
    def _():
        back_copy.wait_send()

    @pl.loop(1, m)
    def _(k):
        stat_copy(k, tp).wait_send()

    pair_copy.wait_send()

    @pl.loop(1, half)
    def _(k):
        tap_copy(k, q).wait_send()

    for i in range(half):
        for s in range(2):
            y_copy(order[i], s).wait_send()
    for i in range(half - 1):
        for s in range(2):
            side_copy(i, s).wait_send()
        zf_side(i, order[i]).wait_send()
    zf_back.wait_send()


def finish(count, *refs):
    sem = refs[-1]
    copies = [
        pltpu.make_async_copy(source, target, sem.at[k])
        for k, (source, target) in enumerate(zip(refs[:count], refs[count : 2 * count]))
    ]
    for copy in copies:
        copy.start()
    for copy in copies:
        copy.wait()


def outputs(rows, chans, kw, dr):
    return (
        pltpu.VMEM((rows, chans), BF16),
        pltpu.VMEM((rows, chans), BF16),
        pltpu.VMEM((kw, chans), F32),
        pltpu.VMEM((1, chans), F32),
        pltpu.VMEM((dr, chans), F32),
    )


def pair_call(n, m, rows, chans, kw, depth):
    dr = depth // n
    half = n // 2
    tiles = chans // LANES
    halo = rup(kw - 1, 16)
    taps_rows = rup(kw + 1, 8)
    zf = chans // 4
    cut = (chans - zf) // 2
    vm = pltpu.VMEM
    dma = pltpu.SemaphoreType.DMA
    wide = vm((rows, LANES), F32)
    block = vm((half, 2, cut, dr), BF16)
    return pl.pallas_call(
        functools.partial(pair_kernel, n, m, kw),
        out_shape=outputs(rows, chans, kw, dr),
        in_specs=[pl.BlockSpec(memory_space=pltpu.HBM)] * 8,
        out_specs=(pl.BlockSpec(memory_space=pltpu.VMEM),) * 5,
        scratch_shapes=[
            vm((rows, chans), BF16), vm((rows, chans), BF16), vm((kw, chans), BF16),
            vm((1, chans), F32), vm((1, rows), F32), vm((1, rows), F32),
            vm((rows, depth), BF16), vm((depth, chans), BF16),
            vm((kw, chans), F32),
            vm((tiles, rows + halo, LANES), F32),
            vm((tiles, rows + halo, LANES), F32),
            vm((tiles, rows, LANES), F32),
            vm((tiles, rows, LANES), F32),
            vm((rows, chans), BF16),
            vm((chans, rows), BF16),
            vm((rows, chans), F32),
            wide, wide, wide, wide, wide, wide,
            vm((halo, chans), BF16), vm((halo, chans), BF16),
            vm((m, 2, rows), F32),
            vm((tiles, taps_rows, LANES), F32), vm((tiles, taps_rows, LANES), F32),
            vm((half, tiles, taps_rows, LANES), F32),
            vm((half, 2, cut, dr), F32),
            block, block, vm((half - 1, 2, cut, dr), BF16), block, vm((2, cut, dr), BF16),
            vm((half, 2, zf, dr), F32), vm((half - 1, 2, zf, dr), BF16), vm((half, 2, zf, dr), BF16),
            vm((2, zf, dr), BF16), vm((zf, dr), BF16), vm((zf, dr), BF16), vm((chans, dr), F32),
            dma((8,)), dma((2,)), dma((2,)), dma((m,)), dma((m,)), dma((2,)),
            dma((half,)), dma((half,)),
            dma((half, 2)), dma((half, 2)), dma((half - 1, 2)), dma((half, 2)), dma((3,)),
            dma((half - 1,)), dma((half,)), dma((2,)),
            pltpu.SemaphoreType.REGULAR((half - 2, 2)),
        ],
        compiler_params=pltpu.CompilerParams(
            collective_id=0, has_side_effects=True, vmem_limit_bytes=VMEM_LIMIT
        ),
    )


def wide_call(n, m, rows, chans, kw, depth):
    dr = depth // n
    half = n // 2
    tiles = chans // LANES
    halo = rup(kw - 1, 16)
    vm = pltpu.VMEM
    dma = pltpu.SemaphoreType.DMA
    whole = pl.BlockSpec(memory_space=pltpu.VMEM)
    far = pl.BlockSpec(memory_space=pltpu.HBM)
    return pl.pallas_call(
        functools.partial(kernel, n, m, kw),
        out_shape=outputs(rows, chans, kw, dr),
        in_specs=[whole] * 6 + [far] * 2,
        out_specs=(whole,) * 5,
        scratch_shapes=[
            vm((kw, chans), F32),
            vm((rows, depth), BF16),
            vm((depth, chans), BF16),
            vm((tiles, rows + halo, LANES), F32),
            vm((7, tiles, rows + halo, LANES), F32),
            vm((tiles, rows + halo, LANES), F32),
            vm((7, tiles, rows + halo, LANES), F32),
            vm((tiles, rows, LANES), F32),
            vm((tiles, rows, LANES), F32),
            vm((rows, chans), BF16),
            vm((rows, chans), F32),
            vm((rows, LANES), F32),
            vm((rows, LANES), F32),
            vm((rows, LANES), F32),
            vm((rows, LANES), F32),
            vm((rows, LANES), F32),
            vm((rows, LANES), F32),
            vm((halo, chans), BF16),
            vm((halo, chans), BF16),
            vm((m, 2, rows), F32),
            vm((n, tiles, rup(kw + 1, n) // n, LANES), F32),
            vm((n, tiles, rup(kw + 1, n) // n, LANES), F32),
            vm((n, tiles, rup(kw + 1, n) // n, LANES), F32),
            vm((depth, chans), F32),
            vm((depth, chans), BF16),
            vm((half, dr, chans), BF16),
            vm((half, dr, chans), BF16),
            vm((half, dr, chans), BF16),
            dma((2,)), dma((2,)), dma((2,)),
            dma((m,)), dma((m,)), dma((n,)), dma((n,)), dma((n,)), dma((n,)),
            dma((half,)), dma((half,)), dma((half,)), dma((half,)),
        ],
        compiler_params=pltpu.CompilerParams(
            collective_id=0, has_side_effects=True, vmem_limit_bytes=VMEM_LIMIT
        ),
    )


def per_device(
    n, m, glu_value, glu_gate, conv_taps, norm_gain, out_weight, norm_mean, norm_scale, out_grad
):
    rows, chans = glu_value.shape
    kw = conv_taps.shape[0]
    depth = out_grad.shape[1]
    paired = n == 8 and (depth // n) % LANES == 0 and chans % (2 * LANES) == 0
    call = (pair_call if paired else wide_call)(n, m, rows, chans, kw, depth)
    out = call(*[
        pltpu.with_memory_space_constraint(x, pltpu.HBM)
        for x in (
            glu_value, glu_gate, conv_taps, norm_gain[None, :],
            norm_mean[None, :], norm_scale[None, :], out_grad, out_weight,
        )
    ])
    whole = pl.BlockSpec(memory_space=pltpu.VMEM)
    out = pl.pallas_call(
        functools.partial(finish, len(out)),
        out_shape=tuple(jax.ShapeDtypeStruct(x.shape, x.dtype) for x in out),
        in_specs=[whole] * len(out),
        out_specs=(pl.BlockSpec(memory_space=pltpu.HBM),) * len(out),
        scratch_shapes=[pltpu.SemaphoreType.DMA((len(out),))],
        compiler_params=pltpu.CompilerParams(vmem_limit_bytes=2 * 1024 * 1024),
    )(*out)
    value_grad, gate_grad, taps_grad, gain_grad, weight_grad = out
    return value_grad, gate_grad, taps_grad, gain_grad[0], weight_grad


def solution(mesh):
    placed = (
        P("sp", "tp"), P("sp", "tp"), P(None, "tp"), P("tp"),
        P(None, "tp"), P("sp"), P("sp"), P("sp", None),
    )
    return jax.shard_map(
        functools.partial(per_device, mesh.shape["sp"], mesh.shape["tp"]),
        mesh=mesh,
        in_specs=placed,
        out_specs=(P("sp", "tp"), P("sp", "tp"), P(None, "tp"), P("tp"), P("sp", "tp")),
        check_vma=False,
    )
```

```python
import functools

import jax
import jax.numpy as jnp
from jax import lax
from jax.experimental import pallas as pl
from jax.experimental.pallas import tpu as pltpu
from jax.sharding import PartitionSpec as P

MESH = pl.DeviceIdType.MESH
F32 = jnp.float32
BF16 = jnp.bfloat16
LANES = 128
VMEM_LIMIT = 30 * 1024 * 1024
BLOCK = 64


def rup(value, unit):
    return -(-value // unit) * unit


def kernel(
    n, m, kw,
    val, gate, taps_in, gain, mean_row, scale_row, og_hbm, ow_hbm,
    value_grad, gate_grad, taps_out, gain_out, w_out,
    taps, og, ow, gp, sh, cg, sh2, centered, slope, act, agrad, psum, csum, meanb, scaleb,
    mpb, mcb, halo_out, halo_in, stats, taploc, tapin, tapsum, wsum, wbf, recv1, send2, recv2,
    load_sem, halo_sem, back_sem, stat_send, stat_recv, tap_send, tap_recv, all_send, all_recv,
    y_send, y_recv, z_send, z_recv,
):
    rows, chans = val.shape
    tiles = chans // LANES
    depth = og.shape[1]
    dr = depth // n
    half = n // 2
    reach = kw - 1
    halo = halo_out.shape[0]
    lead = halo - reach
    blocks = rows // BLOCK
    sp = lax.axis_index("sp")
    tp = lax.axis_index("tp")
    par = lax.rem(sp, 2)
    q = lax.div(sp, 2)
    partner = sp + 1 - 2 * par

    load_og = pltpu.make_async_copy(og_hbm, og, load_sem.at[0])
    load_ow = pltpu.make_async_copy(ow_hbm, ow, load_sem.at[1])
    load_og.start()
    load_ow.start()

    barrier = pltpu.get_barrier_semaphore()

    @pl.loop(1, n)
    def _(k):
        pl.semaphore_signal(
            barrier, inc=1, device_id={"sp": lax.rem(sp + k, n)}, device_id_type=MESH
        )

    @pl.loop(1, m)
    def _(k):
        pl.semaphore_signal(
            barrier, inc=1, device_id={"tp": lax.rem(tp + k, m)}, device_id_type=MESH
        )

    def lanes(ct):
        return slice(ct * LANES, (ct + 1) * LANES)

    taps[...] = taps_in[...].astype(F32)
    tail = slice(rows - halo, rows)
    tail_sig = jax.nn.sigmoid(gate[tail, :].astype(F32))
    halo_out[...] = (val[tail, :].astype(F32) * tail_sig).astype(BF16)

    def gate_block(b, _):
        at = pl.ds(pl.multiple_of(b * BLOCK, BLOCK), BLOCK)
        to = pl.ds(pl.multiple_of(b * BLOCK + halo, 16), BLOCK)
        for ct in range(tiles):
            sig = jax.nn.sigmoid(gate[at, lanes(ct)].astype(F32))
            gp[ct, to, :] = (val[at, lanes(ct)].astype(F32) * sig).astype(BF16).astype(F32)
        return 0

    lax.fori_loop(0, blocks, gate_block, 0)

    load_og.wait()
    load_ow.wait()
    slab = min(rows, 128)

    def grad_block(b, _):
        at = pl.ds(pl.multiple_of(b * slab, slab), slab)
        agrad[at, :] = jnp.dot(og[at, :], ow[...], preferred_element_type=F32)
        return 0

    lax.fori_loop(0, rows // slab, grad_block, 0)

    pl.semaphore_wait(barrier, n - 1 + m - 1)

    halo_copy = pltpu.make_async_remote_copy(
        src_ref=halo_out, dst_ref=halo_in,
        send_sem=halo_sem.at[0], recv_sem=halo_sem.at[1],
        device_id={"sp": lax.rem(sp + 1, n)}, device_id_type=MESH,
    )

    @pl.when(sp < n - 1)
    def _():
        halo_copy.start()

    def shifted(src, dst, begin, count):
        for ct in range(tiles):
            for r in range(1, 8):
                dst[r - 1, ct, begin : begin + count, :] = src[ct, begin + r : begin + r + count, :]

    for at in range(halo, rows + halo - 8, BLOCK):
        shifted(gp, sh, at, min(BLOCK, rows + halo - 8 - at))
    meanb[...] = jnp.broadcast_to(mean_row[...], (LANES, rows)).T
    scaleb[...] = jnp.broadcast_to(scale_row[...], (LANES, rows)).T

    def source(base_ref, copies, shift, ct, start, count):
        r, base = shift % 8, shift - shift % 8
        at = pl.ds(pl.multiple_of(start + base, 8), count)
        if r == 0:
            return base_ref[ct, at, :]
        return copies[r - 1, ct, at, :]

    def conv_block(b, _):
        start = pl.multiple_of(b * BLOCK, BLOCK)
        at = pl.ds(start, BLOCK)
        for ct in range(tiles):
            conv = jnp.zeros((BLOCK, LANES), F32)
            for k in range(kw):
                conv = conv + taps[k : k + 1, lanes(ct)] * source(gp, sh, k + lead, ct, start, BLOCK)
            cen = (conv - meanb[at, :]) * scaleb[at, :]
            nor = cen * gain[:, lanes(ct)]
            sig = jax.nn.sigmoid(nor)
            centered[ct, at, :] = cen
            slope[ct, at, :] = sig * (1.0 + nor * (1.0 - sig))
            act[at, lanes(ct)] = (nor * sig).astype(BF16)
        return 0

    lax.fori_loop(1, blocks, conv_block, 0)

    @pl.when(sp > 0)
    def _():
        halo_copy.wait_recv()
        for ct in range(tiles):
            gp[ct, 0:halo, :] = halo_in[:, lanes(ct)].astype(F32)

    @pl.when(sp == 0)
    def _():
        for ct in range(tiles):
            gp[ct, 0:halo, :] = jnp.zeros((halo, LANES), F32)

    shifted(gp, sh, 0, halo)
    conv_block(0, 0)

    wide = max(dr, min(depth, 256))

    def w_tile(start):
        start = pl.multiple_of(start, wide)
        part = lax.dot_general(
            og[:, pl.ds(start, wide)], act[...], (((0,), (0,)), ((), ())),
            preferred_element_type=F32,
        )
        wsum[pl.ds(start, wide), :] = part
        wbf[pl.ds(start, wide), :] = part.astype(BF16)

    def own_rows(p, side):
        return pl.ds(pl.multiple_of((2 * p + side) * dr, dr), dr)

    def y_copy(p):
        return pltpu.make_async_remote_copy(
            src_ref=wbf.at[own_rows(p, 1 - par), :], dst_ref=recv1.at[p],
            send_sem=y_send.at[p], recv_sem=y_recv.at[p],
            device_id={"sp": partner}, device_id_type=MESH,
        )

    def partner_step(k, _):
        p = lax.rem(q + k, half)
        w_tile((2 * p + 1 - par) * dr)
        y_copy(p).start()
        return 0

    def own_step(k, _):
        w_tile((2 * lax.rem(q + k, half) + par) * dr)
        return 0

    if wide == dr:
        lax.fori_loop(1, half, partner_step, 0)
        w_tile((2 * q + 1 - par) * dr)
    else:
        def tile_step(j, _):
            w_tile(j * wide)
            return 0

        lax.fori_loop(0, depth // wide, tile_step, 0)

        def send_step(k, _):
            y_copy(lax.rem(q + k, half)).start()
            return 0

        lax.fori_loop(1, half, send_step, 0)

    def stat_block(b, sums):
        at = pl.ds(pl.multiple_of(b * BLOCK, BLOCK), BLOCK)
        plain = jnp.zeros((BLOCK, LANES), F32)
        cross = jnp.zeros((BLOCK, LANES), F32)
        new = []
        for ct in range(tiles):
            cen = centered[ct, at, :]
            ngrad = agrad[at, lanes(ct)] * slope[ct, at, :]
            scaled = ngrad * gain[:, lanes(ct)]
            agrad[at, lanes(ct)] = scaled
            plain = plain + scaled
            cross = cross + scaled * cen
            new.append(sums[ct] + jnp.sum((ngrad * cen).reshape(BLOCK // 8, 8, LANES), axis=0))
        psum[at, :] = plain
        csum[at, :] = cross
        return tuple(new)

    gains = lax.fori_loop(
        0, blocks, stat_block, tuple(jnp.zeros((8, LANES), F32) for _ in range(tiles))
    )
    stats[tp, 0:1, :] = jnp.sum(psum[...].T, axis=0, keepdims=True)
    stats[tp, 1:2, :] = jnp.sum(csum[...].T, axis=0, keepdims=True)

    def stat_copy(k, slot):
        return pltpu.make_async_remote_copy(
            src_ref=stats.at[slot], dst_ref=stats.at[slot],
            send_sem=stat_send.at[k], recv_sem=stat_recv.at[slot],
            device_id={"tp": lax.rem(tp + k, m)}, device_id_type=MESH,
        )

    @pl.loop(1, m)
    def _(k):
        stat_copy(k, tp).start()

    if wide == dr:
        lax.fori_loop(1, half + 1, own_step, 0)

    share = taploc.shape[2]

    def keep_tap(k, ct, sums):
        taploc[k // share, ct, k % share : k % share + 1, :] = jnp.sum(sums, axis=0, keepdims=True)

    for ct in range(tiles):
        keep_tap(kw, ct, gains[ct])
        for k in range(kw + 1, n * share):
            keep_tap(k, ct, jnp.zeros((8, LANES), F32))

    @pl.loop(1, m)
    def _(k):
        stat_copy(k, lax.rem(tp + m - k, m)).wait_recv()

    totals = stats[0]
    for k in range(1, m):
        totals = totals + stats[k]
    totals = totals / (chans * m)
    mpb[...] = jnp.broadcast_to(totals[0:1, :], (LANES, rows)).T
    mcb[...] = jnp.broadcast_to(totals[1:2, :], (LANES, rows)).T

    def cg_block(b, _):
        at = pl.ds(pl.multiple_of(b * BLOCK, BLOCK), BLOCK)
        for ct in range(tiles):
            cg[ct, at, :] = scaleb[at, :] * (
                agrad[at, lanes(ct)] - mpb[at, :] - centered[ct, at, :] * mcb[at, :]
            )
        return 0

    lax.fori_loop(0, blocks, cg_block, 0)
    back_copy = pltpu.make_async_remote_copy(
        src_ref=cg.at[:, pl.ds(0, halo), :], dst_ref=cg.at[:, pl.ds(rows, halo), :],
        send_sem=back_sem.at[0], recv_sem=back_sem.at[1],
        device_id={"sp": lax.rem(sp + n - 1, n)}, device_id_type=MESH,
    )

    @pl.when(sp > 0)
    def _():
        back_copy.start()

    def z_copy(k, p, slot):
        return pltpu.make_async_remote_copy(
            src_ref=send2.at[p], dst_ref=recv2.at[slot],
            send_sem=z_send.at[k], recv_sem=z_recv.at[slot],
            device_id={"sp": 2 * p + par}, device_id_type=MESH,
        )

    def relay(k, _):
        p = lax.rem(q + k, half)
        y_copy(p).wait_recv()
        send2[p] = (wsum[own_rows(p, par), :] + recv1[p].astype(F32)).astype(BF16)
        z_copy(k, p, q).start()
        return 0

    cut1 = 1 + (half - 1 + 2) // 3
    cut2 = cut1 + (half - cut1 + 1) // 2
    lax.fori_loop(1, cut1, relay, 0)

    span = 16
    for ct in range(tiles):
        def tap_block(b, sums, ct=ct):
            start = pl.multiple_of(b * span, span)
            grad = cg[ct, pl.ds(start, span), :]
            new = []
            for k in range(kw):
                prod = grad * source(gp, sh, k + lead, ct, start, span)
                new.append(sums[k] + jnp.sum(prod.reshape(span // 8, 8, LANES), axis=0))
            return tuple(new)

        sums = lax.fori_loop(
            0, rows // span, tap_block, tuple(jnp.zeros((8, LANES), F32) for _ in range(kw))
        )
        for k in range(kw):
            keep_tap(k, ct, sums[k])

    def tap_copy(k, slot):
        peer = lax.rem(sp + k, n)
        return pltpu.make_async_remote_copy(
            src_ref=taploc.at[peer], dst_ref=tapin.at[slot],
            send_sem=tap_send.at[k], recv_sem=tap_recv.at[slot],
            device_id={"sp": peer}, device_id_type=MESH,
        )

    def all_copy(k, slot):
        return pltpu.make_async_remote_copy(
            src_ref=tapsum.at[slot], dst_ref=tapsum.at[slot],
            send_sem=all_send.at[k], recv_sem=all_recv.at[slot],
            device_id={"sp": lax.rem(sp + k, n)}, device_id_type=MESH,
        )

    @pl.loop(1, n)
    def _(k):
        tap_copy(k, sp).start()

    y_copy(q).start()

    lax.fori_loop(cut1, cut2, relay, 0)

    for at in range(0, rows - 8, BLOCK):
        shifted(cg, sh2, at, min(BLOCK, rows - 8 - at))

    def back_block(b, _):
        start = pl.multiple_of(b * BLOCK, BLOCK)
        at = pl.ds(start, BLOCK)
        for ct in range(tiles):
            total = jnp.zeros((BLOCK, LANES), F32)
            for k in range(kw):
                total = total + taps[k : k + 1, lanes(ct)] * source(
                    cg, sh2, reach - k, ct, start, BLOCK
                )
            sig = jax.nn.sigmoid(gate[at, lanes(ct)].astype(F32))
            value_grad[at, lanes(ct)] = (total * sig).astype(BF16)
            gate_grad[at, lanes(ct)] = (
                total * val[at, lanes(ct)].astype(F32) * sig * (1.0 - sig)
            ).astype(BF16)
        return 0

    lax.fori_loop(0, blocks - 1, back_block, 0)

    @pl.when(sp < n - 1)
    def _():
        back_copy.wait_recv()

    @pl.when(sp == n - 1)
    def _():
        cg[:, rows : rows + halo, :] = jnp.zeros((tiles, halo, LANES), F32)

    shifted(cg, sh2, rows - 8, halo)
    back_block(blocks - 1, 0)

    lax.fori_loop(cut2, half, relay, 0)

    def tap_wait(k, total):
        slot = lax.rem(sp + n - k, n)
        tap_copy(k, slot).wait_recv()
        return total + tapin[slot]

    tapsum[sp] = lax.fori_loop(1, n, tap_wait, taploc[sp])

    @pl.loop(1, n)
    def _(k):
        all_copy(k, sp).start()

    y_copy(q).wait_recv()
    w_out[...] = wsum[own_rows(q, par), :] + recv1[q].astype(F32)

    def z_wait(k, _):
        p = lax.rem(q + half - k, half)
        z_copy(k, p, p).wait_recv()
        w_out[...] += recv2[p].astype(F32)
        return 0

    lax.fori_loop(1, half, z_wait, 0)

    @pl.loop(1, n)
    def _(k):
        all_copy(k, lax.rem(sp + n - k, n)).wait_recv()

    for ct in range(tiles):
        for k in range(kw):
            taps_out[k : k + 1, lanes(ct)] = tapsum[k // share, ct, k % share : k % share + 1, :]
        gain_out[:, lanes(ct)] = tapsum[kw // share, ct, kw % share : kw % share + 1, :]

    @pl.when(sp < n - 1)
    def _():
        halo_copy.wait_send()

    @pl.when(sp > 0)
    def _():
        back_copy.wait_send()

    @pl.loop(1, m)
    def _(k):
        stat_copy(k, tp).wait_send()

    @pl.loop(1, n)
    def _(k):
        tap_copy(k, sp).wait_send()
        all_copy(k, sp).wait_send()

    @pl.loop(0, half)
    def _(k):
        y_copy(k).wait_send()

    @pl.loop(1, half)
    def _(k):
        z_copy(k, lax.rem(q + k, half), q).wait_send()


def pair_kernel(
    n, m, kw,
    val_hbm, gate_hbm, taps_hbm, gain_hbm, mean_hbm, scale_hbm, og_hbm, ow_hbm,
    value_grad, gate_grad, taps_out, gain_out, w_out,
    val, gate, taps_in, gain, mean_row, scale_row, og, ow,
    taps, gp, cg, centered, slope, act, actt, agrad, psum, csum, meanb, scaleb, mpb, mcb,
    halo_out, halo_in, late_stats, head_stats, tapacc, taploc, tapout, tappair, tapz, wsum, ysend, yrecv, zsend, zrecv, xrecv,
    zfown, zfsend, zfside, zfx, zfysend, zfyrecv, whole,
    load_sem, halo_sem, back_sem, stat_sem, pair_sem, tap_sem,
    y_send, y_recv, z_send, z_recv, x_recv, zf_send, zf_recv, zfy_sem, hop,
):
    rows, chans = val.shape
    tiles = chans // LANES
    depth = og.shape[1]
    dr = depth // n
    half = n // 2
    reach = kw - 1
    halo = halo_out.shape[0]
    lead = halo - reach
    blocks = rows // BLOCK
    zf = chans // 4
    cut = (chans - zf) // 2
    sp = lax.axis_index("sp")
    tp = lax.axis_index("tp")
    par = lax.rem(sp, 2)
    q = lax.div(sp, 2)
    partner = sp + 1 - 2 * par
    low = q < 2
    outer = jnp.logical_or(q == 0, q == 3)
    sib = q + 1 - 2 * lax.rem(q, 2)

    barrier = pltpu.get_barrier_semaphore()

    up, down = q < half - 1, q > 0
    skew = jnp.where(par == 1, sp + 1, sp - 1)
    has_skew = jnp.logical_and(skew >= 0, skew < n)

    def greet(other):
        pl.semaphore_signal(barrier, inc=1, device_id={"sp": other}, device_id_type=MESH)

    greet(partner)

    @pl.when(up)
    def _():
        greet(sp + 2)

    @pl.when(down)
    def _():
        greet(sp - 2)

    @pl.when(has_skew)
    def _():
        greet(skew)

    @pl.loop(1, m)
    def _(k):
        pl.semaphore_signal(
            barrier, inc=1, device_id={"tp": lax.rem(tp + k, m)}, device_id_type=MESH
        )

    loads = [
        pltpu.make_async_copy(source, target, load_sem.at[k])
        for k, (source, target) in enumerate((
            (gate_hbm, gate), (val_hbm, val), (taps_hbm, taps_in), (mean_hbm, mean_row),
            (scale_hbm, scale_row), (gain_hbm, gain), (og_hbm, og), (ow_hbm, ow),
        ))
    ]
    for load in loads:
        load.start()

    def lanes(ct):
        return slice(ct * LANES, (ct + 1) * LANES)

    for load in loads[:6]:
        load.wait()
    tail = slice(rows - halo, rows)
    tail_sig = jax.nn.sigmoid(gate[tail, :].astype(F32))
    halo_out[...] = (val[tail, :].astype(F32) * tail_sig).astype(BF16)
    taps[...] = taps_in[...].astype(F32)

    def gate_block(b, _):
        at = pl.ds(pl.multiple_of(b * BLOCK, BLOCK), BLOCK)
        to = pl.ds(pl.multiple_of(b * BLOCK + halo, 16), BLOCK)
        for ct in range(tiles):
            sig = jax.nn.sigmoid(gate[at, lanes(ct)].astype(F32))
            gp[ct, to, :] = (val[at, lanes(ct)].astype(F32) * sig).astype(BF16).astype(F32)
        return 0

    lax.fori_loop(0, blocks, gate_block, 0)
    meanb[...] = jnp.broadcast_to(mean_row[...], (LANES, rows)).T
    scaleb[...] = jnp.broadcast_to(scale_row[...], (LANES, rows)).T

    near = up.astype(jnp.int32) + down.astype(jnp.int32) + has_skew.astype(jnp.int32)
    pl.semaphore_wait(barrier, m + near)

    halo_copy = pltpu.make_async_remote_copy(
        src_ref=halo_out, dst_ref=halo_in,
        send_sem=halo_sem.at[0], recv_sem=halo_sem.at[1],
        device_id={"sp": lax.rem(sp + 1, n)}, device_id_type=MESH,
    )

    @pl.when(sp < n - 1)
    def _():
        halo_copy.start()

    def tell(r):
        @pl.when(up)
        def _():
            pl.semaphore_signal(
                hop.at[r, 0], inc=1, device_id={"sp": sp + 2}, device_id_type=MESH
            )

        @pl.when(down)
        def _():
            pl.semaphore_signal(
                hop.at[r, 1], inc=1, device_id={"sp": sp - 2}, device_id_type=MESH
            )

    def hear(r):
        @pl.when(down)
        def _():
            pl.semaphore_wait(hop.at[r, 0], 1)

        @pl.when(up)
        def _():
            pl.semaphore_wait(hop.at[r, 1], 1)

    tell(0)
    def source(ref, shift, ct, start, count):
        return ref[ct, pl.ds(start + shift, count), :]

    def conv_block(b, _):
        start = pl.multiple_of(b * BLOCK, BLOCK)
        at = pl.ds(start, BLOCK)
        for ct in range(tiles):
            conv = jnp.zeros((BLOCK, LANES), F32)
            for k in range(kw):
                conv = conv + taps[k : k + 1, lanes(ct)] * source(gp, k + lead, ct, start, BLOCK)
            cen = (conv - meanb[at, :]) * scaleb[at, :]
            nor = cen * gain[:, lanes(ct)]
            sig = jax.nn.sigmoid(nor)
            centered[ct, at, :] = cen
            slope[ct, at, :] = sig * (1.0 + nor * (1.0 - sig))
            act[at, lanes(ct)] = (nor * sig).astype(BF16)
        return 0

    def turn(chunk):
        at = slice(chunk * LANES, (chunk + 1) * LANES)
        for ct in range(tiles):
            actt[lanes(ct), at] = act[at, lanes(ct)].T

    lax.fori_loop(1, blocks, conv_block, 0)
    for chunk in range(1, rows // LANES):
        turn(chunk)

    for load in loads[6:]:
        load.wait()
    slab = min(rows, 256)

    def grad_block(b, _):
        at = pl.ds(pl.multiple_of(b * slab, slab), slab)
        agrad[at, :] = jnp.dot(og[at, :], ow[...], preferred_element_type=F32)
        return 0

    lax.fori_loop(0, rows // slab, grad_block, 0, unroll=True)

    def stat_block(b, sums):
        at = pl.ds(pl.multiple_of(b * BLOCK, BLOCK), BLOCK)
        plain = jnp.zeros((BLOCK, LANES), F32)
        cross = jnp.zeros((BLOCK, LANES), F32)
        new = []
        for ct in range(tiles):
            cen = centered[ct, at, :]
            ngrad = agrad[at, lanes(ct)] * slope[ct, at, :]
            scaled = ngrad * gain[:, lanes(ct)]
            agrad[at, lanes(ct)] = scaled
            plain = plain + scaled
            cross = cross + scaled * cen
            new.append(sums[ct] + jnp.sum((ngrad * cen).reshape(BLOCK // 8, 8, LANES), axis=0))
        psum[at, :] = plain
        csum[at, :] = cross
        return tuple(new)

    first = LANES // BLOCK

    def pack(target, at):
        target[tp, 0:1, :] = jnp.sum(psum[at, :].T, axis=0, keepdims=True)
        target[tp, 1:2, :] = jnp.sum(csum[at, :].T, axis=0, keepdims=True)

    def stat_copy(k, target, c):
        return pltpu.make_async_remote_copy(
            src_ref=target.at[tp], dst_ref=target.at[tp],
            send_sem=stat_sem.at[c, 0], recv_sem=stat_sem.at[c, 1],
            device_id={"tp": lax.rem(tp + k, m)}, device_id_type=MESH,
        )

    def stat_all(target, c):
        others = target.at[pl.ds(0, m - 1)]
        return pltpu.make_async_remote_copy(
            src_ref=others, dst_ref=others,
            send_sem=stat_sem.at[c, 0], recv_sem=stat_sem.at[c, 1],
            device_id={"tp": lax.rem(tp + 1, m)}, device_id_type=MESH,
        )

    def stat_send(target, c):
        @pl.loop(1, m)
        def _(k):
            stat_copy(k, target, c).start()

    gains = lax.fori_loop(
        first, blocks, stat_block, tuple(jnp.zeros((8, LANES), F32) for _ in range(tiles))
    )
    late_rows, head_rows = slice(LANES, rows), slice(0, LANES)
    pack(late_stats, late_rows)
    stat_send(late_stats, 0)

    hear(0)
    tell(1)

    @pl.when(sp > 0)
    def _():
        halo_copy.wait_recv()
        for ct in range(tiles):
            gp[ct, 0:halo, :] = halo_in[:, lanes(ct)].astype(F32)

    @pl.when(sp == 0)
    def _():
        for ct in range(tiles):
            gp[ct, 0:halo, :] = jnp.zeros((halo, LANES), F32)

    conv_block(0, 0)
    turn(0)
    def piece(i):
        far = (i, i - 1)
        near_first = jnp.where(low, half - 1 - far[1], far[1]) if i else sib
        far_first = jnp.where(low, half - 1 - far[0], far[0]) if i < 2 else sib
        return jnp.where(outer, far_first, near_first)

    order = [piece(0), piece(1), piece(2), q]
    parts = (slice(0, cut), slice(cut, 2 * cut))
    last = slice(2 * cut, chans)

    def product(block):
        at = pl.ds(pl.multiple_of(block * dr, LANES), dr)
        return jnp.dot(actt[...], og[:, at], preferred_element_type=F32)

    def y_copy(p, s):
        return pltpu.make_async_remote_copy(
            src_ref=ysend.at[p, s], dst_ref=yrecv.at[p, s],
            send_sem=y_send.at[0], recv_sem=y_recv.at[p, s],
            device_id={"sp": partner}, device_id_type=MESH,
        )

    def away(p):
        part = product(2 * p + 1 - par)
        for s in range(2):
            ysend[p, s] = part[parts[s], :].astype(BF16)
        zfown[p, 0] = part[last, :]

    def home(p):
        part = product(2 * p + par)
        for s in range(2):
            wsum[p, s] = part[parts[s], :]
        zfown[p, 1] = part[last, :]

    ahead = lax.rem(tp, 2) == 0

    def send(cond, halves):
        @pl.when(cond)
        def _():
            for i, s in halves:
                y_copy(order[i], s).start()

    def zf_copy(i, peer, target, sem):
        return pltpu.make_async_remote_copy(
            src_ref=zfsend.at[i], dst_ref=target, send_sem=zf_send.at[0], recv_sem=sem,
            device_id={"sp": 2 * peer + par}, device_id_type=MESH,
        )

    def zf_side(i, slot):
        return zf_copy(i, sib, zfside.at[slot], zf_recv.at[slot])

    def zf_cross(i, p):
        return zf_copy(i, p, zfx, x_recv.at[2])

    def zf_first(i):
        zfsend[i] = zfown[order[i]].astype(BF16)
        zf_side(i, i if i else jnp.where(outer, 0, 2)).start()

    def zf_relay(i):
        zf_side(0, i - 1).wait_recv()
        zfsend[i] = (zfown[order[i]] + zfside[i - 1].astype(F32)).astype(BF16)
        zf_cross(i, order[i]).start()

    inner = jnp.logical_not(outer)
    away(order[0])
    send(ahead, ((0, 0), (0, 1)))
    away(order[1])
    send(ahead, ((1, 0), (1, 1)))
    gains = lax.fori_loop(0, first, stat_block, gains)
    pack(head_stats, head_rows)
    stat_send(head_stats, 1)
    home(order[0])
    zf_first(0)
    home(order[1])

    @pl.when(outer)
    def _():
        zf_first(1)

    away(order[2])
    home(order[2])

    send(jnp.logical_not(ahead), [(i, s) for i in (0, 1) for s in range(2)])
    away(order[3])
    home(order[3])

    def cg_block(b, _):
        at = pl.ds(pl.multiple_of(b * BLOCK, BLOCK), BLOCK)
        for ct in range(tiles):
            cg[ct, at, :] = scaleb[at, :] * (
                agrad[at, lanes(ct)] - mpb[at, :] - centered[ct, at, :] * mcb[at, :]
            )
        return 0

    def cg_rows(target, c, at, begin, end):
        stat_all(target, c).wait_recv()
        totals = target[0]
        for k in range(1, m):
            totals = totals + target[k]
        totals = totals / (chans * m)
        count = target.shape[2]
        mpb[at, :] = jnp.broadcast_to(totals[0:1, :], (LANES, count)).T
        mcb[at, :] = jnp.broadcast_to(totals[1:2, :], (LANES, count)).T
        lax.fori_loop(begin, end, cg_block, 0)

    cg_rows(late_stats, 0, late_rows, first, blocks)

    span = 32

    def tap_rows(ct, begin, end, sums):
        def tap_block(b, sums):
            start = pl.multiple_of(b * span, span)
            grad = cg[ct, pl.ds(start, span), :]
            new = []
            for k in range(kw):
                prod = grad * source(gp, k + lead, ct, start, span)
                new.append(sums[k] + jnp.sum(prod.reshape(span // 8, 8, LANES), axis=0))
            return tuple(new)

        return lax.fori_loop(begin // span, end // span, tap_block, sums)

    for ct in range(tiles):
        sums = tap_rows(ct, LANES, rows, tuple(jnp.zeros((8, LANES), F32) for _ in range(kw)))
        for k in range(kw):
            tapacc[ct, k] = sums[k]

    def side_copy(i, slot, s):
        return pltpu.make_async_remote_copy(
            src_ref=zsend.at[i, s], dst_ref=zrecv.at[slot, s],
            send_sem=z_send.at[0], recv_sem=z_recv.at[slot, s],
            device_id={"sp": 2 * sib + par}, device_id_type=MESH,
        )

    def cross_copy(i, s):
        return pltpu.make_async_remote_copy(
            src_ref=zsend.at[i, s], dst_ref=xrecv.at[s],
            send_sem=z_send.at[0], recv_sem=x_recv.at[s],
            device_id={"sp": 2 * order[i] + par}, device_id_type=MESH,
        )

    def relay(i, s):
        p = order[i]
        y_copy(p, s).wait_recv()
        if i == 0:
            zsend[i, s] = (wsum[p, s] + yrecv[p, s].astype(F32)).astype(BF16)
            side_copy(i, jnp.where(outer, 0, 2), s).start()
            return

        @pl.when(outer)
        def _():
            zsend[i, s] = (wsum[p, s] + yrecv[p, s].astype(F32)).astype(BF16)
            side_copy(i, i, s).start()

        @pl.when(inner)
        def _():
            own = wsum[p, s] + yrecv[p, s].astype(F32)
            side_copy(i, i - 1, s).wait_recv()
            zsend[i, s] = (own + zrecv[i - 1, s].astype(F32)).astype(BF16)
            cross_copy(i, s).start()

    hear(1)

    @pl.when(outer)
    def _():
        relay(0, 0)

    cg_rows(head_stats, 1, head_rows, 0, first)
    back_copy = pltpu.make_async_remote_copy(
        src_ref=cg.at[:, pl.ds(0, halo), :], dst_ref=cg.at[:, pl.ds(rows, halo), :],
        send_sem=back_sem.at[0], recv_sem=back_sem.at[1],
        device_id={"sp": lax.rem(sp + n - 1, n)}, device_id_type=MESH,
    )

    @pl.when(sp > 0)
    def _():
        back_copy.start()

    for ct in range(tiles):
        sums = tap_rows(ct, 0, LANES, tuple(tapacc[ct, k] for k in range(kw)))
        for k, total in enumerate((*sums, gains[ct])):
            taploc[ct, k : k + 1, :] = jnp.sum(total, axis=0, keepdims=True)

    tapout[...] = taploc[...].astype(BF16)
    pair_copy = pltpu.make_async_remote_copy(
        src_ref=tapout, dst_ref=tappair, send_sem=pair_sem.at[0], recv_sem=pair_sem.at[1],
        device_id={"sp": partner}, device_id_type=MESH,
    )
    pair_copy.start()
    for i in (2, 3):
        for s in range(2):
            y_copy(order[i], s).start()
    @pl.when(outer)
    def _():
        relay(0, 1)

    @pl.when(inner)
    def _():
        zf_relay(1)
        relay(0, 0)


    def back_block(b, _):
        start = pl.multiple_of(b * BLOCK, BLOCK)
        at = pl.ds(start, BLOCK)
        for ct in range(tiles):
            total = jnp.zeros((BLOCK, LANES), F32)
            for k in range(kw):
                total = total + taps[k : k + 1, lanes(ct)] * source(cg, reach - k, ct, start, BLOCK)
            sig = jax.nn.sigmoid(gate[at, lanes(ct)].astype(F32))
            value_grad[at, lanes(ct)] = (total * sig).astype(BF16)
            gate_grad[at, lanes(ct)] = (
                total * val[at, lanes(ct)].astype(F32) * sig * (1.0 - sig)
            ).astype(BF16)
        return 0

    lax.fori_loop(0, blocks // 2, back_block, 0)

    @pl.when(outer)
    def _():
        relay(1, 0)
        relay(1, 1)
        zf_first(2)

    @pl.when(inner)
    def _():
        zf_relay(2)
        relay(0, 1)

    lax.fori_loop(blocks // 2, blocks - 1, back_block, 0)

    pair_copy.wait_recv()
    tapz[q] = (tapout[...].astype(F32) + tappair[...].astype(F32)).astype(BF16)

    def tap_copy(k, source_ref):
        return pltpu.make_async_remote_copy(
            src_ref=source_ref, dst_ref=source_ref,
            send_sem=tap_sem.at[0], recv_sem=tap_sem.at[1],
            device_id={"sp": 2 * lax.rem(q + k, half) + par}, device_id_type=MESH,
        )

    @pl.loop(1, half)
    def _(k):
        tap_copy(k, tapz.at[q]).start()

    tap_all = tap_copy(1, tapz.at[pl.ds(0, half - 1)])

    @pl.when(inner)
    def _():
        relay(1, 0)

    @pl.when(inner)
    def _():
        relay(1, 1)

    relay(2, 0)
    @pl.when(sp < n - 1)
    def _():
        back_copy.wait_recv()

    @pl.when(sp == n - 1)
    def _():
        cg[:, rows : rows + halo, :] = jnp.zeros((tiles, halo, LANES), F32)

    back_block(blocks - 1, 0)

    relay(2, 1)

    zf_side(0, 2).wait_recv()
    zf_cross(0, q).wait_recv()
    for k in range(2):
        zfown[q, k] += zfside[2, k].astype(F32) + zfx[k].astype(F32)
    zfysend[...] = zfown[q, 0].astype(BF16)
    zf_back = pltpu.make_async_remote_copy(
        src_ref=zfysend, dst_ref=zfyrecv, send_sem=zfy_sem.at[0], recv_sem=zfy_sem.at[1],
        device_id={"sp": partner}, device_id_type=MESH,
    )
    zf_back.start()

    for s in range(2):
        y_copy(q, s).wait_recv()
        wsum[q, s] += yrecv[q, s].astype(F32)
    tap_all.wait_recv()

    for ct in range(tiles):
        total = tapz[0, ct].astype(F32)
        for k in range(1, half):
            total = total + tapz[k, ct].astype(F32)
        taps_out[:, lanes(ct)] = total[0:kw]
        gain_out[:, lanes(ct)] = total[kw : kw + 1]

    for s in range(2):
        side_copy(0, 2, s).wait_recv()
        cross_copy(0, s).wait_recv()
        whole[parts[s], :] = wsum[q, s] + zrecv[2, s].astype(F32) + xrecv[s].astype(F32)
    zf_back.wait_recv()
    whole[last, :] = zfown[q, 1] + zfyrecv[...].astype(F32)
    w_out[...] = whole[...].T

    @pl.when(sp < n - 1)
    def _():
        halo_copy.wait_send()

    @pl.when(sp > 0)
    def _():
        back_copy.wait_send()

    stat_all(late_stats, 0).wait_send()
    stat_all(head_stats, 1).wait_send()
    pair_copy.wait_send()
    tap_all.wait_send()
    pltpu.make_async_remote_copy(
        src_ref=ysend, dst_ref=yrecv, send_sem=y_send.at[0], recv_sem=y_recv.at[0, 0],
        device_id={"sp": partner}, device_id_type=MESH,
    ).wait_send()
    pltpu.make_async_remote_copy(
        src_ref=zsend, dst_ref=zrecv, send_sem=z_send.at[0], recv_sem=z_recv.at[0, 0],
        device_id={"sp": partner}, device_id_type=MESH,
    ).wait_send()
    pltpu.make_async_remote_copy(
        src_ref=zfsend, dst_ref=zfside, send_sem=zf_send.at[0], recv_sem=zf_recv.at[0],
        device_id={"sp": partner}, device_id_type=MESH,
    ).wait_send()
    zf_back.wait_send()


def finish(count, *refs):
    sem = refs[-1]
    copies = [
        pltpu.make_async_copy(source, target, sem.at[k])
        for k, (source, target) in enumerate(zip(refs[:count], refs[count : 2 * count]))
    ]
    for copy in copies:
        copy.start()
    for copy in copies:
        copy.wait()


def outputs(rows, chans, kw, dr):
    return (
        pltpu.VMEM((rows, chans), BF16),
        pltpu.VMEM((rows, chans), BF16),
        pltpu.VMEM((kw, chans), F32),
        pltpu.VMEM((1, chans), F32),
        pltpu.VMEM((dr, chans), F32),
    )


def pair_call(n, m, rows, chans, kw, depth):
    dr = depth // n
    half = n // 2
    tiles = chans // LANES
    halo = rup(kw - 1, 16)
    taps_rows = rup(kw + 1, 16)
    zf = chans // 4
    cut = (chans - zf) // 2
    vm = pltpu.VMEM
    dma = pltpu.SemaphoreType.DMA
    wide = vm((rows, LANES), F32)
    block = vm((half, 2, cut, dr), BF16)
    part = vm((half - 1, 2, cut, dr), BF16)
    return pl.pallas_call(
        functools.partial(pair_kernel, n, m, kw),
        out_shape=outputs(rows, chans, kw, dr),
        in_specs=[pl.BlockSpec(memory_space=pltpu.HBM)] * 8,
        out_specs=(pl.BlockSpec(memory_space=pltpu.VMEM),) * 5,
        scratch_shapes=[
            vm((rows, chans), BF16), vm((rows, chans), BF16), vm((kw, chans), BF16),
            vm((1, chans), F32), vm((1, rows), F32), vm((1, rows), F32),
            vm((rows, depth), BF16), vm((depth, chans), BF16),
            vm((kw, chans), F32),
            vm((tiles, rows + halo, LANES), F32),
            vm((tiles, rows + halo, LANES), F32),
            vm((tiles, rows, LANES), F32),
            vm((tiles, rows, LANES), F32),
            vm((rows, chans), BF16),
            vm((chans, rows), BF16),
            vm((rows, chans), F32),
            wide, wide, wide, wide, wide, wide,
            vm((halo, chans), BF16), vm((halo, chans), BF16),
            vm((m, 2, rows - LANES), F32), vm((m, 2, LANES), F32), vm((tiles, kw, 8, LANES), F32),
            vm((tiles, taps_rows, LANES), F32), vm((tiles, taps_rows, LANES), BF16),
            vm((tiles, taps_rows, LANES), BF16),
            vm((half, tiles, taps_rows, LANES), BF16),
            vm((half, 2, cut, dr), F32),
            block, block, part, part, vm((2, cut, dr), BF16),
            vm((half, 2, zf, dr), F32), vm((half - 1, 2, zf, dr), BF16), vm((half - 1, 2, zf, dr), BF16),
            vm((2, zf, dr), BF16), vm((zf, dr), BF16), vm((zf, dr), BF16), vm((chans, dr), F32),
            dma((8,)), dma((2,)), dma((2,)), dma((2, 2)), dma((2,)), dma((2,)),
            dma((1,)), dma((half, 2)), dma((1,)), dma((half - 1, 2)), dma((3,)),
            dma((1,)), dma((half - 1,)), dma((2,)),
            pltpu.SemaphoreType.REGULAR((half - 2, 2)),
        ],
        compiler_params=pltpu.CompilerParams(
            collective_id=0, has_side_effects=True, vmem_limit_bytes=VMEM_LIMIT
        ),
    )


def wide_call(n, m, rows, chans, kw, depth):
    dr = depth // n
    half = n // 2
    tiles = chans // LANES
    halo = rup(kw - 1, 16)
    vm = pltpu.VMEM
    dma = pltpu.SemaphoreType.DMA
    whole = pl.BlockSpec(memory_space=pltpu.VMEM)
    far = pl.BlockSpec(memory_space=pltpu.HBM)
    return pl.pallas_call(
        functools.partial(kernel, n, m, kw),
        out_shape=outputs(rows, chans, kw, dr),
        in_specs=[whole] * 6 + [far] * 2,
        out_specs=(whole,) * 5,
        scratch_shapes=[
            vm((kw, chans), F32),
            vm((rows, depth), BF16),
            vm((depth, chans), BF16),
            vm((tiles, rows + halo, LANES), F32),
            vm((7, tiles, rows + halo, LANES), F32),
            vm((tiles, rows + halo, LANES), F32),
            vm((7, tiles, rows + halo, LANES), F32),
            vm((tiles, rows, LANES), F32),
            vm((tiles, rows, LANES), F32),
            vm((rows, chans), BF16),
            vm((rows, chans), F32),
            vm((rows, LANES), F32),
            vm((rows, LANES), F32),
            vm((rows, LANES), F32),
            vm((rows, LANES), F32),
            vm((rows, LANES), F32),
            vm((rows, LANES), F32),
            vm((halo, chans), BF16),
            vm((halo, chans), BF16),
            vm((m, 2, rows), F32),
            vm((n, tiles, rup(kw + 1, n) // n, LANES), F32),
            vm((n, tiles, rup(kw + 1, n) // n, LANES), F32),
            vm((n, tiles, rup(kw + 1, n) // n, LANES), F32),
            vm((depth, chans), F32),
            vm((depth, chans), BF16),
            vm((half, dr, chans), BF16),
            vm((half, dr, chans), BF16),
            vm((half, dr, chans), BF16),
            dma((2,)), dma((2,)), dma((2,)),
            dma((m,)), dma((m,)), dma((n,)), dma((n,)), dma((n,)), dma((n,)),
            dma((half,)), dma((half,)), dma((half,)), dma((half,)),
        ],
        compiler_params=pltpu.CompilerParams(
            collective_id=0, has_side_effects=True, vmem_limit_bytes=VMEM_LIMIT
        ),
    )


def per_device(
    n, m, glu_value, glu_gate, conv_taps, norm_gain, out_weight, norm_mean, norm_scale, out_grad
):
    rows, chans = glu_value.shape
    kw = conv_taps.shape[0]
    depth = out_grad.shape[1]
    paired = n == 8 and (depth // n) % LANES == 0 and chans % (2 * LANES) == 0
    call = (pair_call if paired else wide_call)(n, m, rows, chans, kw, depth)
    out = call(*[
        pltpu.with_memory_space_constraint(x, pltpu.HBM)
        for x in (
            glu_value, glu_gate, conv_taps, norm_gain[None, :],
            norm_mean[None, :], norm_scale[None, :], out_grad, out_weight,
        )
    ])
    whole = pl.BlockSpec(memory_space=pltpu.VMEM)
    out = pl.pallas_call(
        functools.partial(finish, len(out)),
        out_shape=tuple(jax.ShapeDtypeStruct(x.shape, x.dtype) for x in out),
        in_specs=[whole] * len(out),
        out_specs=(pl.BlockSpec(memory_space=pltpu.HBM),) * len(out),
        scratch_shapes=[pltpu.SemaphoreType.DMA((len(out),))],
        compiler_params=pltpu.CompilerParams(vmem_limit_bytes=2 * 1024 * 1024),
    )(*out)
    value_grad, gate_grad, taps_grad, gain_grad, weight_grad = out
    return value_grad, gate_grad, taps_grad, gain_grad[0], weight_grad


def solution(mesh):
    placed = (
        P("sp", "tp"), P("sp", "tp"), P(None, "tp"), P("tp"),
        P(None, "tp"), P("sp"), P("sp"), P("sp", None),
    )
    return jax.shard_map(
        functools.partial(per_device, mesh.shape["sp"], mesh.shape["tp"]),
        mesh=mesh,
        in_specs=placed,
        out_specs=(P("sp", "tp"), P("sp", "tp"), P(None, "tp"), P("tp"), P("sp", "tp")),
        check_vma=False,
    )
```

```python
import functools

import jax
import jax.numpy as jnp
from jax import lax
from jax.experimental import pallas as pl
from jax.experimental.pallas import tpu as pltpu
from jax.sharding import PartitionSpec as P

MESH = pl.DeviceIdType.MESH
F32 = jnp.float32
BF16 = jnp.bfloat16
LANES = 128
VMEM_LIMIT = 30 * 1024 * 1024
BLOCK = 64


def rup(value, unit):
    return -(-value // unit) * unit


def kernel(
    n, m, kw,
    val, gate, taps_in, gain, mean_row, scale_row, og_hbm, ow_hbm,
    value_grad, gate_grad, taps_out, gain_out, w_out,
    taps, og, ow, gp, sh, cg, sh2, centered, slope, act, agrad, psum, csum, meanb, scaleb,
    mpb, mcb, halo_out, halo_in, stats, taploc, tapin, tapsum, wsum, wbf, recv1, send2, recv2,
    load_sem, halo_sem, back_sem, stat_send, stat_recv, tap_send, tap_recv, all_send, all_recv,
    y_send, y_recv, z_send, z_recv,
):
    rows, chans = val.shape
    tiles = chans // LANES
    depth = og.shape[1]
    dr = depth // n
    half = n // 2
    reach = kw - 1
    halo = halo_out.shape[0]
    lead = halo - reach
    blocks = rows // BLOCK
    sp = lax.axis_index("sp")
    tp = lax.axis_index("tp")
    par = lax.rem(sp, 2)
    q = lax.div(sp, 2)
    partner = sp + 1 - 2 * par

    load_og = pltpu.make_async_copy(og_hbm, og, load_sem.at[0])
    load_ow = pltpu.make_async_copy(ow_hbm, ow, load_sem.at[1])
    load_og.start()
    load_ow.start()

    barrier = pltpu.get_barrier_semaphore()

    @pl.loop(1, n)
    def _(k):
        pl.semaphore_signal(
            barrier, inc=1, device_id={"sp": lax.rem(sp + k, n)}, device_id_type=MESH
        )

    @pl.loop(1, m)
    def _(k):
        pl.semaphore_signal(
            barrier, inc=1, device_id={"tp": lax.rem(tp + k, m)}, device_id_type=MESH
        )

    def lanes(ct):
        return slice(ct * LANES, (ct + 1) * LANES)

    taps[...] = taps_in[...].astype(F32)
    tail = slice(rows - halo, rows)
    tail_sig = jax.nn.sigmoid(gate[tail, :].astype(F32))
    halo_out[...] = (val[tail, :].astype(F32) * tail_sig).astype(BF16)

    def gate_block(b, _):
        at = pl.ds(pl.multiple_of(b * BLOCK, BLOCK), BLOCK)
        to = pl.ds(pl.multiple_of(b * BLOCK + halo, 16), BLOCK)
        for ct in range(tiles):
            sig = jax.nn.sigmoid(gate[at, lanes(ct)].astype(F32))
            gp[ct, to, :] = (val[at, lanes(ct)].astype(F32) * sig).astype(BF16).astype(F32)
        return 0

    lax.fori_loop(0, blocks, gate_block, 0)

    load_og.wait()
    load_ow.wait()
    slab = min(rows, 128)

    def grad_block(b, _):
        at = pl.ds(pl.multiple_of(b * slab, slab), slab)
        agrad[at, :] = jnp.dot(og[at, :], ow[...], preferred_element_type=F32)
        return 0

    lax.fori_loop(0, rows // slab, grad_block, 0)

    pl.semaphore_wait(barrier, n - 1 + m - 1)

    halo_copy = pltpu.make_async_remote_copy(
        src_ref=halo_out, dst_ref=halo_in,
        send_sem=halo_sem.at[0], recv_sem=halo_sem.at[1],
        device_id={"sp": lax.rem(sp + 1, n)}, device_id_type=MESH,
    )

    @pl.when(sp < n - 1)
    def _():
        halo_copy.start()

    def shifted(src, dst, begin, count):
        for ct in range(tiles):
            for r in range(1, 8):
                dst[r - 1, ct, begin : begin + count, :] = src[ct, begin + r : begin + r + count, :]

    for at in range(halo, rows + halo - 8, BLOCK):
        shifted(gp, sh, at, min(BLOCK, rows + halo - 8 - at))
    meanb[...] = jnp.broadcast_to(mean_row[...], (LANES, rows)).T
    scaleb[...] = jnp.broadcast_to(scale_row[...], (LANES, rows)).T

    def source(base_ref, copies, shift, ct, start, count):
        r, base = shift % 8, shift - shift % 8
        at = pl.ds(pl.multiple_of(start + base, 8), count)
        if r == 0:
            return base_ref[ct, at, :]
        return copies[r - 1, ct, at, :]

    def conv_block(b, _):
        start = pl.multiple_of(b * BLOCK, BLOCK)
        at = pl.ds(start, BLOCK)
        for ct in range(tiles):
            conv = jnp.zeros((BLOCK, LANES), F32)
            for k in range(kw):
                conv = conv + taps[k : k + 1, lanes(ct)] * source(gp, sh, k + lead, ct, start, BLOCK)
            cen = (conv - meanb[at, :]) * scaleb[at, :]
            nor = cen * gain[:, lanes(ct)]
            sig = jax.nn.sigmoid(nor)
            centered[ct, at, :] = cen
            slope[ct, at, :] = sig * (1.0 + nor * (1.0 - sig))
            act[at, lanes(ct)] = (nor * sig).astype(BF16)
        return 0

    lax.fori_loop(1, blocks, conv_block, 0)

    @pl.when(sp > 0)
    def _():
        halo_copy.wait_recv()
        for ct in range(tiles):
            gp[ct, 0:halo, :] = halo_in[:, lanes(ct)].astype(F32)

    @pl.when(sp == 0)
    def _():
        for ct in range(tiles):
            gp[ct, 0:halo, :] = jnp.zeros((halo, LANES), F32)

    shifted(gp, sh, 0, halo)
    conv_block(0, 0)

    wide = max(dr, min(depth, 256))

    def w_tile(start):
        start = pl.multiple_of(start, wide)
        part = lax.dot_general(
            og[:, pl.ds(start, wide)], act[...], (((0,), (0,)), ((), ())),
            preferred_element_type=F32,
        )
        wsum[pl.ds(start, wide), :] = part
        wbf[pl.ds(start, wide), :] = part.astype(BF16)

    def own_rows(p, side):
        return pl.ds(pl.multiple_of((2 * p + side) * dr, dr), dr)

    def y_copy(p):
        return pltpu.make_async_remote_copy(
            src_ref=wbf.at[own_rows(p, 1 - par), :], dst_ref=recv1.at[p],
            send_sem=y_send.at[p], recv_sem=y_recv.at[p],
            device_id={"sp": partner}, device_id_type=MESH,
        )

    def partner_step(k, _):
        p = lax.rem(q + k, half)
        w_tile((2 * p + 1 - par) * dr)
        y_copy(p).start()
        return 0

    def own_step(k, _):
        w_tile((2 * lax.rem(q + k, half) + par) * dr)
        return 0

    if wide == dr:
        lax.fori_loop(1, half, partner_step, 0)
        w_tile((2 * q + 1 - par) * dr)
    else:
        def tile_step(j, _):
            w_tile(j * wide)
            return 0

        lax.fori_loop(0, depth // wide, tile_step, 0)

        def send_step(k, _):
            y_copy(lax.rem(q + k, half)).start()
            return 0

        lax.fori_loop(1, half, send_step, 0)

    def stat_block(b, sums):
        at = pl.ds(pl.multiple_of(b * BLOCK, BLOCK), BLOCK)
        plain = jnp.zeros((BLOCK, LANES), F32)
        cross = jnp.zeros((BLOCK, LANES), F32)
        new = []
        for ct in range(tiles):
            cen = centered[ct, at, :]
            ngrad = agrad[at, lanes(ct)] * slope[ct, at, :]
            scaled = ngrad * gain[:, lanes(ct)]
            agrad[at, lanes(ct)] = scaled
            plain = plain + scaled
            cross = cross + scaled * cen
            new.append(sums[ct] + jnp.sum((ngrad * cen).reshape(BLOCK // 8, 8, LANES), axis=0))
        psum[at, :] = plain
        csum[at, :] = cross
        return tuple(new)

    gains = lax.fori_loop(
        0, blocks, stat_block, tuple(jnp.zeros((8, LANES), F32) for _ in range(tiles))
    )
    stats[tp, 0:1, :] = jnp.sum(psum[...].T, axis=0, keepdims=True)
    stats[tp, 1:2, :] = jnp.sum(csum[...].T, axis=0, keepdims=True)

    def stat_copy(k, slot):
        return pltpu.make_async_remote_copy(
            src_ref=stats.at[slot], dst_ref=stats.at[slot],
            send_sem=stat_send.at[k], recv_sem=stat_recv.at[slot],
            device_id={"tp": lax.rem(tp + k, m)}, device_id_type=MESH,
        )

    @pl.loop(1, m)
    def _(k):
        stat_copy(k, tp).start()

    if wide == dr:
        lax.fori_loop(1, half + 1, own_step, 0)

    share = taploc.shape[2]

    def keep_tap(k, ct, sums):
        taploc[k // share, ct, k % share : k % share + 1, :] = jnp.sum(sums, axis=0, keepdims=True)

    for ct in range(tiles):
        keep_tap(kw, ct, gains[ct])
        for k in range(kw + 1, n * share):
            keep_tap(k, ct, jnp.zeros((8, LANES), F32))

    @pl.loop(1, m)
    def _(k):
        stat_copy(k, lax.rem(tp + m - k, m)).wait_recv()

    totals = stats[0]
    for k in range(1, m):
        totals = totals + stats[k]
    totals = totals / (chans * m)
    mpb[...] = jnp.broadcast_to(totals[0:1, :], (LANES, rows)).T
    mcb[...] = jnp.broadcast_to(totals[1:2, :], (LANES, rows)).T

    def cg_block(b, _):
        at = pl.ds(pl.multiple_of(b * BLOCK, BLOCK), BLOCK)
        for ct in range(tiles):
            cg[ct, at, :] = scaleb[at, :] * (
                agrad[at, lanes(ct)] - mpb[at, :] - centered[ct, at, :] * mcb[at, :]
            )
        return 0

    lax.fori_loop(0, blocks, cg_block, 0)
    back_copy = pltpu.make_async_remote_copy(
        src_ref=cg.at[:, pl.ds(0, halo), :], dst_ref=cg.at[:, pl.ds(rows, halo), :],
        send_sem=back_sem.at[0], recv_sem=back_sem.at[1],
        device_id={"sp": lax.rem(sp + n - 1, n)}, device_id_type=MESH,
    )

    @pl.when(sp > 0)
    def _():
        back_copy.start()

    def z_copy(k, p, slot):
        return pltpu.make_async_remote_copy(
            src_ref=send2.at[p], dst_ref=recv2.at[slot],
            send_sem=z_send.at[k], recv_sem=z_recv.at[slot],
            device_id={"sp": 2 * p + par}, device_id_type=MESH,
        )

    def relay(k, _):
        p = lax.rem(q + k, half)
        y_copy(p).wait_recv()
        send2[p] = (wsum[own_rows(p, par), :] + recv1[p].astype(F32)).astype(BF16)
        z_copy(k, p, q).start()
        return 0

    cut1 = 1 + (half - 1 + 2) // 3
    cut2 = cut1 + (half - cut1 + 1) // 2
    lax.fori_loop(1, cut1, relay, 0)

    span = 16
    for ct in range(tiles):
        def tap_block(b, sums, ct=ct):
            start = pl.multiple_of(b * span, span)
            grad = cg[ct, pl.ds(start, span), :]
            new = []
            for k in range(kw):
                prod = grad * source(gp, sh, k + lead, ct, start, span)
                new.append(sums[k] + jnp.sum(prod.reshape(span // 8, 8, LANES), axis=0))
            return tuple(new)

        sums = lax.fori_loop(
            0, rows // span, tap_block, tuple(jnp.zeros((8, LANES), F32) for _ in range(kw))
        )
        for k in range(kw):
            keep_tap(k, ct, sums[k])

    def tap_copy(k, slot):
        peer = lax.rem(sp + k, n)
        return pltpu.make_async_remote_copy(
            src_ref=taploc.at[peer], dst_ref=tapin.at[slot],
            send_sem=tap_send.at[k], recv_sem=tap_recv.at[slot],
            device_id={"sp": peer}, device_id_type=MESH,
        )

    def all_copy(k, slot):
        return pltpu.make_async_remote_copy(
            src_ref=tapsum.at[slot], dst_ref=tapsum.at[slot],
            send_sem=all_send.at[k], recv_sem=all_recv.at[slot],
            device_id={"sp": lax.rem(sp + k, n)}, device_id_type=MESH,
        )

    @pl.loop(1, n)
    def _(k):
        tap_copy(k, sp).start()

    y_copy(q).start()

    lax.fori_loop(cut1, cut2, relay, 0)

    for at in range(0, rows - 8, BLOCK):
        shifted(cg, sh2, at, min(BLOCK, rows - 8 - at))

    def back_block(b, _):
        start = pl.multiple_of(b * BLOCK, BLOCK)
        at = pl.ds(start, BLOCK)
        for ct in range(tiles):
            total = jnp.zeros((BLOCK, LANES), F32)
            for k in range(kw):
                total = total + taps[k : k + 1, lanes(ct)] * source(
                    cg, sh2, reach - k, ct, start, BLOCK
                )
            sig = jax.nn.sigmoid(gate[at, lanes(ct)].astype(F32))
            value_grad[at, lanes(ct)] = (total * sig).astype(BF16)
            gate_grad[at, lanes(ct)] = (
                total * val[at, lanes(ct)].astype(F32) * sig * (1.0 - sig)
            ).astype(BF16)
        return 0

    lax.fori_loop(0, blocks - 1, back_block, 0)

    @pl.when(sp < n - 1)
    def _():
        back_copy.wait_recv()

    @pl.when(sp == n - 1)
    def _():
        cg[:, rows : rows + halo, :] = jnp.zeros((tiles, halo, LANES), F32)

    shifted(cg, sh2, rows - 8, halo)
    back_block(blocks - 1, 0)

    lax.fori_loop(cut2, half, relay, 0)

    def tap_wait(k, total):
        slot = lax.rem(sp + n - k, n)
        tap_copy(k, slot).wait_recv()
        return total + tapin[slot]

    tapsum[sp] = lax.fori_loop(1, n, tap_wait, taploc[sp])

    @pl.loop(1, n)
    def _(k):
        all_copy(k, sp).start()

    y_copy(q).wait_recv()
    w_out[...] = wsum[own_rows(q, par), :] + recv1[q].astype(F32)

    def z_wait(k, _):
        p = lax.rem(q + half - k, half)
        z_copy(k, p, p).wait_recv()
        w_out[...] += recv2[p].astype(F32)
        return 0

    lax.fori_loop(1, half, z_wait, 0)

    @pl.loop(1, n)
    def _(k):
        all_copy(k, lax.rem(sp + n - k, n)).wait_recv()

    for ct in range(tiles):
        for k in range(kw):
            taps_out[k : k + 1, lanes(ct)] = tapsum[k // share, ct, k % share : k % share + 1, :]
        gain_out[:, lanes(ct)] = tapsum[kw // share, ct, kw % share : kw % share + 1, :]

    @pl.when(sp < n - 1)
    def _():
        halo_copy.wait_send()

    @pl.when(sp > 0)
    def _():
        back_copy.wait_send()

    @pl.loop(1, m)
    def _(k):
        stat_copy(k, tp).wait_send()

    @pl.loop(1, n)
    def _(k):
        tap_copy(k, sp).wait_send()
        all_copy(k, sp).wait_send()

    @pl.loop(0, half)
    def _(k):
        y_copy(k).wait_send()

    @pl.loop(1, half)
    def _(k):
        z_copy(k, lax.rem(q + k, half), q).wait_send()


def pair_body(
    n, m, kw,
    val_hbm, gate_hbm, taps_hbm, gain_hbm, mean_hbm, scale_hbm, og_hbm, ow_hbm,
    value_grad, gate_grad, taps_out, gain_out, w_out,
    val, gate, taps_in, gain, mean_row, scale_row, og, ow,
    taps, gp, cg, centered, slope, act, actt, agrad, psum, csum, meanb, scaleb, mpb, mcb,
    halo_out, halo_in, late_stats, head_stats, tapacc, taploc, tapout, tappair, tapz, wsum, ysend, yrecv, zsend, zrecv, xrecv,
    zfown, zfsend, zfin, zfysend, zfyrecv, whole,
    halo_sem, back_sem, stat_sem, pair_sem, tap_sem, y_recv, z_recv, x_recv, zf_recv, zfy_sem, hop,
    load_sem, sent,
):
    rows, chans = val.shape
    tiles = chans // LANES
    depth = og.shape[1]
    dr = depth // n
    half = n // 2
    reach = kw - 1
    halo = halo_out.shape[0]
    lead = halo - reach
    blocks = rows // BLOCK
    zf = chans // 4
    cut = (chans - zf) // 2
    sp = lax.axis_index("sp")
    tp = lax.axis_index("tp")
    par = lax.rem(sp, 2)
    q = lax.div(sp, 2)
    partner = sp + 1 - 2 * par
    low = q < 2
    outer = jnp.logical_or(q == 0, q == 3)
    sib = q + 1 - 2 * lax.rem(q, 2)

    barrier = pltpu.get_barrier_semaphore()

    up, down = q < half - 1, q > 0
    skew = jnp.where(par == 1, sp + 1, sp - 1)
    has_skew = jnp.logical_and(skew >= 0, skew < n)

    def greet(other):
        pl.semaphore_signal(barrier, inc=1, device_id={"sp": other}, device_id_type=MESH)

    greet(partner)

    @pl.when(up)
    def _():
        greet(sp + 2)

    @pl.when(down)
    def _():
        greet(sp - 2)

    @pl.when(has_skew)
    def _():
        greet(skew)

    @pl.loop(1, m)
    def _(k):
        pl.semaphore_signal(
            barrier, inc=1, device_id={"tp": lax.rem(tp + k, m)}, device_id_type=MESH
        )

    loads = [
        pltpu.make_async_copy(source, target, load_sem.at[k])
        for k, (source, target) in enumerate((
            (gate_hbm, gate), (val_hbm, val), (taps_hbm, taps_in), (mean_hbm, mean_row),
            (scale_hbm, scale_row), (gain_hbm, gain), (og_hbm, og), (ow_hbm, ow),
        ))
    ]
    for load in loads:
        load.start()

    def lanes(ct):
        return slice(ct * LANES, (ct + 1) * LANES)

    for load in loads[:6]:
        load.wait()
    tail = slice(rows - halo, rows)
    tail_sig = jax.nn.sigmoid(gate[tail, :].astype(F32))
    halo_out[...] = (val[tail, :].astype(F32) * tail_sig).astype(BF16)
    taps[...] = taps_in[...].astype(F32)

    def gate_block(b, _):
        at = pl.ds(pl.multiple_of(b * BLOCK, BLOCK), BLOCK)
        to = pl.ds(pl.multiple_of(b * BLOCK + halo, 16), BLOCK)
        for ct in range(tiles):
            sig = jax.nn.sigmoid(gate[at, lanes(ct)].astype(F32))
            gp[ct, to, :] = (val[at, lanes(ct)].astype(F32) * sig).astype(BF16).astype(F32)
        return 0

    lax.fori_loop(0, blocks, gate_block, 0)
    meanb[...] = jnp.broadcast_to(mean_row[...], (LANES, rows)).T
    scaleb[...] = jnp.broadcast_to(scale_row[...], (LANES, rows)).T

    def source(ref, shift, ct, start, count):
        return ref[ct, pl.ds(start + shift, count), :]

    def conv_rows(start, count):
        at = pl.ds(start, count)
        for ct in range(tiles):
            conv = jnp.zeros((count, LANES), F32)
            for k in range(kw):
                conv = conv + taps[k : k + 1, lanes(ct)] * source(gp, k + lead, ct, start, count)
            cen = (conv - meanb[at, :]) * scaleb[at, :]
            nor = cen * gain[:, lanes(ct)]
            sig = jax.nn.sigmoid(nor)
            centered[ct, at, :] = cen
            slope[ct, at, :] = sig * (1.0 + nor * (1.0 - sig))
            act[at, lanes(ct)] = (nor * sig).astype(BF16)

    def conv_block(b, _):
        conv_rows(pl.multiple_of(b * BLOCK, BLOCK), BLOCK)
        return 0

    lax.fori_loop(1, 2, conv_block, 0)

    near = up.astype(jnp.int32) + down.astype(jnp.int32) + has_skew.astype(jnp.int32)
    pl.semaphore_wait(barrier, m + near)

    halo_copy = pltpu.make_async_remote_copy(
        src_ref=halo_out, dst_ref=halo_in,
        send_sem=sent.at[0], recv_sem=halo_sem,
        device_id={"sp": lax.rem(sp + 1, n)}, device_id_type=MESH,
    )

    @pl.when(sp < n - 1)
    def _():
        halo_copy.start()

    def tell(r):
        @pl.when(up)
        def _():
            pl.semaphore_signal(
                hop.at[r, 0], inc=1, device_id={"sp": sp + 2}, device_id_type=MESH
            )

        @pl.when(down)
        def _():
            pl.semaphore_signal(
                hop.at[r, 1], inc=1, device_id={"sp": sp - 2}, device_id_type=MESH
            )

    def hear(r):
        @pl.when(down)
        def _():
            pl.semaphore_wait(hop.at[r, 0], 1)

        @pl.when(up)
        def _():
            pl.semaphore_wait(hop.at[r, 1], 1)

    tell(0)
    def turn(chunk):
        at = slice(chunk * LANES, (chunk + 1) * LANES)
        for ct in range(tiles):
            actt[lanes(ct), at] = act[at, lanes(ct)].T

    lax.fori_loop(2, blocks, conv_block, 0)
    conv_rows(halo, BLOCK - halo)
    for chunk in range(1, rows // LANES):
        turn(chunk)

    for load in loads[6:]:
        load.wait()
    slab = min(rows, 256)

    def grad_block(b, _):
        at = pl.ds(pl.multiple_of(b * slab, slab), slab)
        agrad[at, :] = jnp.dot(og[at, :], ow[...], preferred_element_type=F32)
        return 0

    lax.fori_loop(0, rows // slab, grad_block, 0, unroll=True)

    def stat_block(b, sums):
        at = pl.ds(pl.multiple_of(b * BLOCK, BLOCK), BLOCK)
        plain = jnp.zeros((BLOCK, LANES), F32)
        cross = jnp.zeros((BLOCK, LANES), F32)
        new = []
        for ct in range(tiles):
            cen = centered[ct, at, :]
            ngrad = agrad[at, lanes(ct)] * slope[ct, at, :]
            scaled = ngrad * gain[:, lanes(ct)]
            agrad[at, lanes(ct)] = scaled
            plain = plain + scaled
            cross = cross + scaled * cen
            new.append(sums[ct] + jnp.sum((ngrad * cen).reshape(BLOCK // 8, 8, LANES), axis=0))
        psum[at, :] = plain
        csum[at, :] = cross
        return tuple(new)

    first = LANES // BLOCK

    def pack(target, at):
        target[tp, 0:1, :] = jnp.sum(psum[at, :].T, axis=0, keepdims=True)
        target[tp, 1:2, :] = jnp.sum(csum[at, :].T, axis=0, keepdims=True)

    def stat_copy(k, target, c):
        return pltpu.make_async_remote_copy(
            src_ref=target.at[tp], dst_ref=target.at[tp],
            send_sem=sent.at[2 + c], recv_sem=stat_sem.at[c],
            device_id={"tp": lax.rem(tp + k, m)}, device_id_type=MESH,
        )

    def stat_all(target, c):
        others = target.at[pl.ds(0, m - 1)]
        return pltpu.make_async_remote_copy(
            src_ref=others, dst_ref=others,
            send_sem=sent.at[2 + c], recv_sem=stat_sem.at[c],
            device_id={"tp": lax.rem(tp + 1, m)}, device_id_type=MESH,
        )

    def stat_send(target, c):
        @pl.loop(1, m)
        def _(k):
            stat_copy(k, target, c).start()

    gains = lax.fori_loop(
        first, blocks, stat_block, tuple(jnp.zeros((8, LANES), F32) for _ in range(tiles))
    )
    late_rows, head_rows = slice(LANES, rows), slice(0, LANES)
    pack(late_stats, late_rows)
    stat_send(late_stats, 0)

    hear(0)
    tell(1)

    @pl.when(sp > 0)
    def _():
        halo_copy.wait_recv()
        for ct in range(tiles):
            gp[ct, 0:halo, :] = halo_in[:, lanes(ct)].astype(F32)

    @pl.when(sp == 0)
    def _():
        for ct in range(tiles):
            gp[ct, 0:halo, :] = jnp.zeros((halo, LANES), F32)

    conv_rows(0, halo)
    turn(0)
    below = q == 1
    above = q == 2

    def far(i):
        return jnp.where(low, half - 1 - i, i)

    order = [
        jnp.where(below, sib, far(0)),
        jnp.where(below, far(0), far(1)),
        jnp.where(below, far(1), sib),
        q,
    ]
    parts = (slice(0, cut), slice(cut, 2 * cut))
    last = slice(2 * cut, chans)

    def product(block):
        at = pl.ds(pl.multiple_of(block * dr, LANES), dr)
        return jnp.dot(actt[...], og[:, at], preferred_element_type=F32)

    def y_copy(p, s):
        return pltpu.make_async_remote_copy(
            src_ref=ysend.at[p, s], dst_ref=yrecv.at[p, s],
            send_sem=sent.at[6], recv_sem=y_recv.at[p, s],
            device_id={"sp": partner}, device_id_type=MESH,
        )

    def away(p):
        part = product(2 * p + 1 - par)
        for s in range(2):
            ysend[p, s] = part[parts[s], :].astype(BF16)
        zfown[p, 0] = part[last, :]

    def home(p):
        part = product(2 * p + par)
        for s in range(2):
            wsum[p, s] = part[parts[s], :]
        zfown[p, 1] = part[last, :]

    ahead = lax.rem(tp, 2) == 0

    def send(cond, halves):
        @pl.when(cond)
        def _():
            for i, s in halves:
                y_copy(order[i], s).start()

    def zf_copy(i, peer, slot):
        return pltpu.make_async_remote_copy(
            src_ref=zfsend.at[i], dst_ref=zfin.at[slot],
            send_sem=sent.at[8], recv_sem=zf_recv.at[slot],
            device_id={"sp": 2 * peer + par}, device_id_type=MESH,
        )

    def zf_far(i):
        zfsend[i] = zfown[far(i)].astype(BF16)
        zf_copy(i, far(i), jnp.where(outer, 1, 2)).start()

    def zf_sib():
        zfsend[2] = zfown[sib].astype(BF16)
        zf_copy(2, sib, 0).start()

    inner = jnp.logical_not(outer)
    away(order[0])
    send(ahead, ((0, 0), (0, 1)))
    gains = lax.fori_loop(0, first, stat_block, gains)
    pack(head_stats, head_rows)
    stat_send(head_stats, 1)
    away(order[1])
    send(ahead, ((1, 0), (1, 1)))
    hear(1)
    home(order[0])

    @pl.when(jnp.logical_not(below))
    def _():
        zf_far(0)

    home(order[1])

    @pl.when(below)
    def _():
        zf_far(0)

    @pl.when(jnp.logical_not(below))
    def _():
        zf_far(1)

    away(order[2])
    home(order[2])

    @pl.when(below)
    def _():
        zf_far(1)

    @pl.when(inner)
    def _():
        zf_sib()

    send(jnp.logical_not(ahead), [(i, s) for i in (0, 1) for s in range(2)])
    away(order[3])
    home(order[3])

    def cg_block(b, _):
        at = pl.ds(pl.multiple_of(b * BLOCK, BLOCK), BLOCK)
        for ct in range(tiles):
            cg[ct, at, :] = scaleb[at, :] * (
                agrad[at, lanes(ct)] - mpb[at, :] - centered[ct, at, :] * mcb[at, :]
            )
        return 0

    def cg_rows(target, c, at, begin, end):
        stat_all(target, c).wait_recv()
        totals = target[0]
        for k in range(1, m):
            totals = totals + target[k]
        totals = totals / (chans * m)
        count = target.shape[2]
        mpb[at, :] = jnp.broadcast_to(totals[0:1, :], (LANES, count)).T
        mcb[at, :] = jnp.broadcast_to(totals[1:2, :], (LANES, count)).T
        lax.fori_loop(begin, end, cg_block, 0)

    cg_rows(late_stats, 0, late_rows, first, blocks)

    span = 32

    def tap_rows(ct, begin, end, sums):
        def tap_block(b, sums):
            start = pl.multiple_of(b * span, span)
            grad = cg[ct, pl.ds(start, span), :]
            new = []
            for k in range(kw):
                prod = grad * source(gp, k + lead, ct, start, span)
                new.append(sums[k] + jnp.sum(prod.reshape(span // 8, 8, LANES), axis=0))
            return tuple(new)

        return lax.fori_loop(begin // span, end // span, tap_block, sums)

    for ct in range(tiles):
        sums = tap_rows(ct, LANES, rows, tuple(jnp.zeros((8, LANES), F32) for _ in range(kw)))
        for k in range(kw):
            tapacc[ct, k] = sums[k]

    def side_copy(i, slot, s):
        return pltpu.make_async_remote_copy(
            src_ref=zsend.at[i, s], dst_ref=zrecv.at[slot, s],
            send_sem=sent.at[7], recv_sem=z_recv.at[slot, s],
            device_id={"sp": 2 * sib + par}, device_id_type=MESH,
        )

    def cross_copy(i, s):
        return pltpu.make_async_remote_copy(
            src_ref=zsend.at[i, s], dst_ref=xrecv.at[s],
            send_sem=sent.at[7], recv_sem=x_recv.at[s],
            device_id={"sp": 2 * order[i] + par}, device_id_type=MESH,
        )

    def relay(i, s):
        p = order[i]
        crossing = (above, inner, below)[i]
        slot = (jnp.where(below, 2, 0), jnp.where(below, 0, 1), jnp.where(below, 1, 2))[i]
        y_copy(p, s).wait_recv()

        @pl.when(jnp.logical_not(crossing))
        def _():
            zsend[i, s] = (wsum[p, s] + yrecv[p, s].astype(F32)).astype(BF16)
            side_copy(i, slot, s).start()

        @pl.when(crossing)
        def _():
            own = wsum[p, s] + yrecv[p, s].astype(F32)
            side_copy(i, slot, s).wait_recv()
            zsend[i, s] = (own + zrecv[slot, s].astype(F32)).astype(BF16)
            cross_copy(i, s).start()

    @pl.when(outer)
    def _():
        relay(0, 0)

    cg_rows(head_stats, 1, head_rows, 0, first)
    back_copy = pltpu.make_async_remote_copy(
        src_ref=cg.at[:, pl.ds(0, halo), :], dst_ref=cg.at[:, pl.ds(rows, halo), :],
        send_sem=sent.at[1], recv_sem=back_sem,
        device_id={"sp": lax.rem(sp + n - 1, n)}, device_id_type=MESH,
    )

    @pl.when(sp > 0)
    def _():
        back_copy.start()

    for ct in range(tiles):
        sums = tap_rows(ct, 0, LANES, tuple(tapacc[ct, k] for k in range(kw)))
        for k, total in enumerate((*sums, gains[ct])):
            taploc[ct, k : k + 1, :] = jnp.sum(total, axis=0, keepdims=True)

    tapout[...] = taploc[...].astype(BF16)
    pair_copy = pltpu.make_async_remote_copy(
        src_ref=tapout, dst_ref=tappair, send_sem=sent.at[4], recv_sem=pair_sem,
        device_id={"sp": partner}, device_id_type=MESH,
    )
    pair_copy.start()
    for i in (2, 3):
        for s in range(2):
            y_copy(order[i], s).start()
    @pl.when(outer)
    def _():
        relay(0, 1)

    @pl.when(below)
    def _():
        relay(0, 0)


    def back_block(b, _):
        start = pl.multiple_of(b * BLOCK, BLOCK)
        at = pl.ds(start, BLOCK)
        for ct in range(tiles):
            total = jnp.zeros((BLOCK, LANES), F32)
            for k in range(kw):
                total = total + taps[k : k + 1, lanes(ct)] * source(cg, reach - k, ct, start, BLOCK)
            sig = jax.nn.sigmoid(gate[at, lanes(ct)].astype(F32))
            value_grad[at, lanes(ct)] = (total * sig).astype(BF16)
            gate_grad[at, lanes(ct)] = (
                total * val[at, lanes(ct)].astype(F32) * sig * (1.0 - sig)
            ).astype(BF16)
        return 0

    lax.fori_loop(0, blocks // 2, back_block, 0)

    @pl.when(outer)
    def _():
        relay(1, 0)
        relay(1, 1)
        zf_sib()

    @pl.when(below)
    def _():
        relay(0, 1)

    lax.fori_loop(blocks // 2, blocks - 1, back_block, 0)

    pair_copy.wait_recv()
    tapz[q] = (tapout[...].astype(F32) + tappair[...].astype(F32)).astype(BF16)

    def tap_copy(k, source_ref):
        return pltpu.make_async_remote_copy(
            src_ref=source_ref, dst_ref=source_ref,
            send_sem=sent.at[5], recv_sem=tap_sem,
            device_id={"sp": 2 * lax.rem(q + k, half) + par}, device_id_type=MESH,
        )

    @pl.loop(1, half)
    def _(k):
        tap_copy(k, tapz.at[q]).start()

    tap_all = tap_copy(1, tapz.at[pl.ds(0, half - 1)])

    @pl.when(above)
    def _():
        relay(0, 0)
        relay(0, 1)

    @pl.when(inner)
    def _():
        relay(1, 0)

    @pl.when(inner)
    def _():
        relay(1, 1)

    relay(2, 0)
    @pl.when(sp < n - 1)
    def _():
        back_copy.wait_recv()

    @pl.when(sp == n - 1)
    def _():
        cg[:, rows : rows + halo, :] = jnp.zeros((tiles, halo, LANES), F32)

    back_block(blocks - 1, 0)

    relay(2, 1)

    for slot in range(half - 1):
        zf_copy(0, sib, slot).wait_recv()
    for k in range(2):
        zfown[q, k] += (
            zfin[0, k].astype(F32) + zfin[1, k].astype(F32) + zfin[2, k].astype(F32)
        )
    zfysend[...] = zfown[q, 0].astype(BF16)
    zf_back = pltpu.make_async_remote_copy(
        src_ref=zfysend, dst_ref=zfyrecv, send_sem=sent.at[9], recv_sem=zfy_sem,
        device_id={"sp": partner}, device_id_type=MESH,
    )
    zf_back.start()

    for s in range(2):
        y_copy(q, s).wait_recv()
        wsum[q, s] += yrecv[q, s].astype(F32)
    tap_all.wait_recv()

    for ct in range(tiles):
        total = tapz[0, ct].astype(F32)
        for k in range(1, half):
            total = total + tapz[k, ct].astype(F32)
        taps_out[:, lanes(ct)] = total[0:kw]
        gain_out[:, lanes(ct)] = total[kw : kw + 1]

    for s in range(2):
        side_copy(0, 2, s).wait_recv()
        cross_copy(0, s).wait_recv()
        whole[parts[s], :] = wsum[q, s] + zrecv[2, s].astype(F32) + xrecv[s].astype(F32)
    zf_back.wait_recv()
    whole[last, :] = zfown[q, 1] + zfyrecv[...].astype(F32)
    w_out[...] = whole[...].T

    @pl.when(sp < n - 1)
    def _():
        halo_copy.wait_send()

    @pl.when(sp > 0)
    def _():
        back_copy.wait_send()

    stat_all(late_stats, 0).wait_send()
    stat_all(head_stats, 1).wait_send()
    pair_copy.wait_send()
    tap_all.wait_send()
    pltpu.make_async_remote_copy(
        src_ref=ysend, dst_ref=yrecv, send_sem=sent.at[6], recv_sem=y_recv.at[0, 0],
        device_id={"sp": partner}, device_id_type=MESH,
    ).wait_send()
    pltpu.make_async_remote_copy(
        src_ref=zsend, dst_ref=zrecv, send_sem=sent.at[7], recv_sem=z_recv.at[0, 0],
        device_id={"sp": partner}, device_id_type=MESH,
    ).wait_send()
    pltpu.make_async_remote_copy(
        src_ref=zfsend, dst_ref=zfin, send_sem=sent.at[8], recv_sem=zf_recv.at[0],
        device_id={"sp": partner}, device_id_type=MESH,
    ).wait_send()
    zf_back.wait_send()


def finish(count, *refs):
    sem = refs[-1]
    copies = [
        pltpu.make_async_copy(source, target, sem.at[k])
        for k, (source, target) in enumerate(zip(refs[:count], refs[count : 2 * count]))
    ]
    for copy in copies:
        copy.start()
    for copy in copies:
        copy.wait()


def pair_kernel(n, m, kw, *refs):
    pl.run_scoped(
        functools.partial(pair_body, n, m, kw, *refs),
        pltpu.SemaphoreType.DMA((8,)), pltpu.SemaphoreType.DMA((10,)),
    )


def outputs(rows, chans, kw, dr):
    return (
        pltpu.VMEM((rows, chans), BF16),
        pltpu.VMEM((rows, chans), BF16),
        pltpu.VMEM((kw, chans), F32),
        pltpu.VMEM((1, chans), F32),
        pltpu.VMEM((dr, chans), F32),
    )


def pair_call(n, m, rows, chans, kw, depth):
    dr = depth // n
    half = n // 2
    tiles = chans // LANES
    halo = rup(kw - 1, 16)
    taps_rows = rup(kw + 1, 16)
    zf = chans // 4
    cut = (chans - zf) // 2
    vm = pltpu.VMEM
    dma = pltpu.SemaphoreType.DMA
    wide = vm((rows, LANES), F32)
    block = vm((half, 2, cut, dr), BF16)
    part = vm((half - 1, 2, cut, dr), BF16)
    return pl.pallas_call(
        functools.partial(pair_kernel, n, m, kw),
        out_shape=outputs(rows, chans, kw, dr),
        in_specs=[pl.BlockSpec(memory_space=pltpu.HBM)] * 8,
        out_specs=(pl.BlockSpec(memory_space=pltpu.VMEM),) * 5,
        scratch_shapes=[
            vm((rows, chans), BF16), vm((rows, chans), BF16), vm((kw, chans), BF16),
            vm((1, chans), F32), vm((1, rows), F32), vm((1, rows), F32),
            vm((rows, depth), BF16), vm((depth, chans), BF16),
            vm((kw, chans), F32),
            vm((tiles, rows + halo, LANES), F32),
            vm((tiles, rows + halo, LANES), F32),
            vm((tiles, rows, LANES), F32),
            vm((tiles, rows, LANES), F32),
            vm((rows, chans), BF16),
            vm((chans, rows), BF16),
            vm((rows, chans), F32),
            wide, wide, wide, wide, wide, wide,
            vm((halo, chans), BF16), vm((halo, chans), BF16),
            vm((m, 2, rows - LANES), F32), vm((m, 2, LANES), F32), vm((tiles, kw, 8, LANES), F32),
            vm((tiles, taps_rows, LANES), F32), vm((tiles, taps_rows, LANES), BF16),
            vm((tiles, taps_rows, LANES), BF16),
            vm((half, tiles, taps_rows, LANES), BF16),
            vm((half, 2, cut, dr), F32),
            block, block, part, part, vm((2, cut, dr), BF16),
            vm((half, 2, zf, dr), F32), vm((half - 1, 2, zf, dr), BF16), vm((half - 1, 2, zf, dr), BF16),
            vm((zf, dr), BF16), vm((zf, dr), BF16), vm((chans, dr), F32),
            dma, dma, dma((2,)), dma, dma, dma((half, 2)), dma((half - 1, 2)), dma((2,)),
            dma((half - 1,)), dma,
            pltpu.SemaphoreType.REGULAR((half - 2, 2)),
        ],
        compiler_params=pltpu.CompilerParams(
            collective_id=0, has_side_effects=True, vmem_limit_bytes=VMEM_LIMIT
        ),
    )


def wide_call(n, m, rows, chans, kw, depth):
    dr = depth // n
    half = n // 2
    tiles = chans // LANES
    halo = rup(kw - 1, 16)
    vm = pltpu.VMEM
    dma = pltpu.SemaphoreType.DMA
    whole = pl.BlockSpec(memory_space=pltpu.VMEM)
    far = pl.BlockSpec(memory_space=pltpu.HBM)
    return pl.pallas_call(
        functools.partial(kernel, n, m, kw),
        out_shape=outputs(rows, chans, kw, dr),
        in_specs=[whole] * 6 + [far] * 2,
        out_specs=(whole,) * 5,
        scratch_shapes=[
            vm((kw, chans), F32),
            vm((rows, depth), BF16),
            vm((depth, chans), BF16),
            vm((tiles, rows + halo, LANES), F32),
            vm((7, tiles, rows + halo, LANES), F32),
            vm((tiles, rows + halo, LANES), F32),
            vm((7, tiles, rows + halo, LANES), F32),
            vm((tiles, rows, LANES), F32),
            vm((tiles, rows, LANES), F32),
            vm((rows, chans), BF16),
            vm((rows, chans), F32),
            vm((rows, LANES), F32),
            vm((rows, LANES), F32),
            vm((rows, LANES), F32),
            vm((rows, LANES), F32),
            vm((rows, LANES), F32),
            vm((rows, LANES), F32),
            vm((halo, chans), BF16),
            vm((halo, chans), BF16),
            vm((m, 2, rows), F32),
            vm((n, tiles, rup(kw + 1, n) // n, LANES), F32),
            vm((n, tiles, rup(kw + 1, n) // n, LANES), F32),
            vm((n, tiles, rup(kw + 1, n) // n, LANES), F32),
            vm((depth, chans), F32),
            vm((depth, chans), BF16),
            vm((half, dr, chans), BF16),
            vm((half, dr, chans), BF16),
            vm((half, dr, chans), BF16),
            dma((2,)), dma((2,)), dma((2,)),
            dma((m,)), dma((m,)), dma((n,)), dma((n,)), dma((n,)), dma((n,)),
            dma((half,)), dma((half,)), dma((half,)), dma((half,)),
        ],
        compiler_params=pltpu.CompilerParams(
            collective_id=0, has_side_effects=True, vmem_limit_bytes=VMEM_LIMIT
        ),
    )


def per_device(
    n, m, glu_value, glu_gate, conv_taps, norm_gain, out_weight, norm_mean, norm_scale, out_grad
):
    rows, chans = glu_value.shape
    kw = conv_taps.shape[0]
    depth = out_grad.shape[1]
    paired = n == 8 and (depth // n) % LANES == 0 and chans % (2 * LANES) == 0
    call = (pair_call if paired else wide_call)(n, m, rows, chans, kw, depth)
    out = call(*[
        pltpu.with_memory_space_constraint(x, pltpu.HBM)
        for x in (
            glu_value, glu_gate, conv_taps, norm_gain[None, :],
            norm_mean[None, :], norm_scale[None, :], out_grad, out_weight,
        )
    ])
    whole = pl.BlockSpec(memory_space=pltpu.VMEM)
    out = pl.pallas_call(
        functools.partial(finish, len(out)),
        out_shape=tuple(jax.ShapeDtypeStruct(x.shape, x.dtype) for x in out),
        in_specs=[whole] * len(out),
        out_specs=(pl.BlockSpec(memory_space=pltpu.HBM),) * len(out),
        scratch_shapes=[pltpu.SemaphoreType.DMA((len(out),))],
        compiler_params=pltpu.CompilerParams(vmem_limit_bytes=2 * 1024 * 1024),
    )(*out)
    value_grad, gate_grad, taps_grad, gain_grad, weight_grad = out
    return value_grad, gate_grad, taps_grad, gain_grad[0], weight_grad


def solution(mesh):
    placed = (
        P("sp", "tp"), P("sp", "tp"), P(None, "tp"), P("tp"),
        P(None, "tp"), P("sp"), P("sp"), P("sp", None),
    )
    return jax.shard_map(
        functools.partial(per_device, mesh.shape["sp"], mesh.shape["tp"]),
        mesh=mesh,
        in_specs=placed,
        out_specs=(P("sp", "tp"), P("sp", "tp"), P(None, "tp"), P("tp"), P("sp", "tp")),
        check_vma=False,
    )
```

```python
import functools

import jax
import jax.numpy as jnp
from jax import lax
from jax.experimental import pallas as pl
from jax.experimental.pallas import tpu as pltpu
from jax.sharding import PartitionSpec as P

MESH = pl.DeviceIdType.MESH
F32 = jnp.float32
BF16 = jnp.bfloat16
LANES = 128
VMEM_LIMIT = 30 * 1024 * 1024
BLOCK = 64


def rup(value, unit):
    return -(-value // unit) * unit


def kernel(
    n, m, kw,
    val, gate, taps_in, gain, mean_row, scale_row, og_hbm, ow_hbm,
    value_grad, gate_grad, taps_out, gain_out, w_out,
    taps, og, ow, gp, sh, cg, sh2, centered, slope, act, agrad, psum, csum, meanb, scaleb,
    mpb, mcb, halo_out, halo_in, stats, taploc, tapin, tapsum, wsum, wbf, recv1, send2, recv2,
    load_sem, halo_sem, back_sem, stat_send, stat_recv, tap_send, tap_recv, all_send, all_recv,
    y_send, y_recv, z_send, z_recv,
):
    rows, chans = val.shape
    tiles = chans // LANES
    depth = og.shape[1]
    dr = depth // n
    half = n // 2
    reach = kw - 1
    halo = halo_out.shape[0]
    lead = halo - reach
    blocks = rows // BLOCK
    sp = lax.axis_index("sp")
    tp = lax.axis_index("tp")
    par = lax.rem(sp, 2)
    q = lax.div(sp, 2)
    partner = sp + 1 - 2 * par

    load_og = pltpu.make_async_copy(og_hbm, og, load_sem.at[0])
    load_ow = pltpu.make_async_copy(ow_hbm, ow, load_sem.at[1])
    load_og.start()
    load_ow.start()

    barrier = pltpu.get_barrier_semaphore()

    @pl.loop(1, n)
    def _(k):
        pl.semaphore_signal(
            barrier, inc=1, device_id={"sp": lax.rem(sp + k, n)}, device_id_type=MESH
        )

    @pl.loop(1, m)
    def _(k):
        pl.semaphore_signal(
            barrier, inc=1, device_id={"tp": lax.rem(tp + k, m)}, device_id_type=MESH
        )

    def lanes(ct):
        return slice(ct * LANES, (ct + 1) * LANES)

    taps[...] = taps_in[...].astype(F32)
    tail = slice(rows - halo, rows)
    tail_sig = jax.nn.sigmoid(gate[tail, :].astype(F32))
    halo_out[...] = (val[tail, :].astype(F32) * tail_sig).astype(BF16)

    def gate_block(b, _):
        at = pl.ds(pl.multiple_of(b * BLOCK, BLOCK), BLOCK)
        to = pl.ds(pl.multiple_of(b * BLOCK + halo, 16), BLOCK)
        for ct in range(tiles):
            sig = jax.nn.sigmoid(gate[at, lanes(ct)].astype(F32))
            gp[ct, to, :] = (val[at, lanes(ct)].astype(F32) * sig).astype(BF16).astype(F32)
        return 0

    lax.fori_loop(0, blocks, gate_block, 0)

    load_og.wait()
    load_ow.wait()
    slab = min(rows, 128)

    def grad_block(b, _):
        at = pl.ds(pl.multiple_of(b * slab, slab), slab)
        agrad[at, :] = jnp.dot(og[at, :], ow[...], preferred_element_type=F32)
        return 0

    lax.fori_loop(0, rows // slab, grad_block, 0)

    pl.semaphore_wait(barrier, n - 1 + m - 1)

    halo_copy = pltpu.make_async_remote_copy(
        src_ref=halo_out, dst_ref=halo_in,
        send_sem=halo_sem.at[0], recv_sem=halo_sem.at[1],
        device_id={"sp": lax.rem(sp + 1, n)}, device_id_type=MESH,
    )

    @pl.when(sp < n - 1)
    def _():
        halo_copy.start()

    def shifted(src, dst, begin, count):
        for ct in range(tiles):
            for r in range(1, 8):
                dst[r - 1, ct, begin : begin + count, :] = src[ct, begin + r : begin + r + count, :]

    for at in range(halo, rows + halo - 8, BLOCK):
        shifted(gp, sh, at, min(BLOCK, rows + halo - 8 - at))
    meanb[...] = jnp.broadcast_to(mean_row[...], (LANES, rows)).T
    scaleb[...] = jnp.broadcast_to(scale_row[...], (LANES, rows)).T

    def source(base_ref, copies, shift, ct, start, count):
        r, base = shift % 8, shift - shift % 8
        at = pl.ds(pl.multiple_of(start + base, 8), count)
        if r == 0:
            return base_ref[ct, at, :]
        return copies[r - 1, ct, at, :]

    def conv_block(b, _):
        start = pl.multiple_of(b * BLOCK, BLOCK)
        at = pl.ds(start, BLOCK)
        for ct in range(tiles):
            conv = jnp.zeros((BLOCK, LANES), F32)
            for k in range(kw):
                conv = conv + taps[k : k + 1, lanes(ct)] * source(gp, sh, k + lead, ct, start, BLOCK)
            cen = (conv - meanb[at, :]) * scaleb[at, :]
            nor = cen * gain[:, lanes(ct)]
            sig = jax.nn.sigmoid(nor)
            centered[ct, at, :] = cen
            slope[ct, at, :] = sig * (1.0 + nor * (1.0 - sig))
            act[at, lanes(ct)] = (nor * sig).astype(BF16)
        return 0

    lax.fori_loop(1, blocks, conv_block, 0)

    @pl.when(sp > 0)
    def _():
        halo_copy.wait_recv()
        for ct in range(tiles):
            gp[ct, 0:halo, :] = halo_in[:, lanes(ct)].astype(F32)

    @pl.when(sp == 0)
    def _():
        for ct in range(tiles):
            gp[ct, 0:halo, :] = jnp.zeros((halo, LANES), F32)

    shifted(gp, sh, 0, halo)
    conv_block(0, 0)

    wide = max(dr, min(depth, 256))

    def w_tile(start):
        start = pl.multiple_of(start, wide)
        part = lax.dot_general(
            og[:, pl.ds(start, wide)], act[...], (((0,), (0,)), ((), ())),
            preferred_element_type=F32,
        )
        wsum[pl.ds(start, wide), :] = part
        wbf[pl.ds(start, wide), :] = part.astype(BF16)

    def own_rows(p, side):
        return pl.ds(pl.multiple_of((2 * p + side) * dr, dr), dr)

    def y_copy(p):
        return pltpu.make_async_remote_copy(
            src_ref=wbf.at[own_rows(p, 1 - par), :], dst_ref=recv1.at[p],
            send_sem=y_send.at[p], recv_sem=y_recv.at[p],
            device_id={"sp": partner}, device_id_type=MESH,
        )

    def partner_step(k, _):
        p = lax.rem(q + k, half)
        w_tile((2 * p + 1 - par) * dr)
        y_copy(p).start()
        return 0

    def own_step(k, _):
        w_tile((2 * lax.rem(q + k, half) + par) * dr)
        return 0

    if wide == dr:
        lax.fori_loop(1, half, partner_step, 0)
        w_tile((2 * q + 1 - par) * dr)
    else:
        def tile_step(j, _):
            w_tile(j * wide)
            return 0

        lax.fori_loop(0, depth // wide, tile_step, 0)

        def send_step(k, _):
            y_copy(lax.rem(q + k, half)).start()
            return 0

        lax.fori_loop(1, half, send_step, 0)

    def stat_block(b, sums):
        at = pl.ds(pl.multiple_of(b * BLOCK, BLOCK), BLOCK)
        plain = jnp.zeros((BLOCK, LANES), F32)
        cross = jnp.zeros((BLOCK, LANES), F32)
        new = []
        for ct in range(tiles):
            cen = centered[ct, at, :]
            ngrad = agrad[at, lanes(ct)] * slope[ct, at, :]
            scaled = ngrad * gain[:, lanes(ct)]
            agrad[at, lanes(ct)] = scaled
            plain = plain + scaled
            cross = cross + scaled * cen
            new.append(sums[ct] + jnp.sum((ngrad * cen).reshape(BLOCK // 8, 8, LANES), axis=0))
        psum[at, :] = plain
        csum[at, :] = cross
        return tuple(new)

    gains = lax.fori_loop(
        0, blocks, stat_block, tuple(jnp.zeros((8, LANES), F32) for _ in range(tiles))
    )
    stats[tp, 0:1, :] = jnp.sum(psum[...].T, axis=0, keepdims=True)
    stats[tp, 1:2, :] = jnp.sum(csum[...].T, axis=0, keepdims=True)

    def stat_copy(k, slot):
        return pltpu.make_async_remote_copy(
            src_ref=stats.at[slot], dst_ref=stats.at[slot],
            send_sem=stat_send.at[k], recv_sem=stat_recv.at[slot],
            device_id={"tp": lax.rem(tp + k, m)}, device_id_type=MESH,
        )

    @pl.loop(1, m)
    def _(k):
        stat_copy(k, tp).start()

    if wide == dr:
        lax.fori_loop(1, half + 1, own_step, 0)

    share = taploc.shape[2]

    def keep_tap(k, ct, sums):
        taploc[k // share, ct, k % share : k % share + 1, :] = jnp.sum(sums, axis=0, keepdims=True)

    for ct in range(tiles):
        keep_tap(kw, ct, gains[ct])
        for k in range(kw + 1, n * share):
            keep_tap(k, ct, jnp.zeros((8, LANES), F32))

    @pl.loop(1, m)
    def _(k):
        stat_copy(k, lax.rem(tp + m - k, m)).wait_recv()

    totals = stats[0]
    for k in range(1, m):
        totals = totals + stats[k]
    totals = totals / (chans * m)
    mpb[...] = jnp.broadcast_to(totals[0:1, :], (LANES, rows)).T
    mcb[...] = jnp.broadcast_to(totals[1:2, :], (LANES, rows)).T

    def cg_block(b, _):
        at = pl.ds(pl.multiple_of(b * BLOCK, BLOCK), BLOCK)
        for ct in range(tiles):
            cg[ct, at, :] = scaleb[at, :] * (
                agrad[at, lanes(ct)] - mpb[at, :] - centered[ct, at, :] * mcb[at, :]
            )
        return 0

    lax.fori_loop(0, blocks, cg_block, 0)
    back_copy = pltpu.make_async_remote_copy(
        src_ref=cg.at[:, pl.ds(0, halo), :], dst_ref=cg.at[:, pl.ds(rows, halo), :],
        send_sem=back_sem.at[0], recv_sem=back_sem.at[1],
        device_id={"sp": lax.rem(sp + n - 1, n)}, device_id_type=MESH,
    )

    @pl.when(sp > 0)
    def _():
        back_copy.start()

    def z_copy(k, p, slot):
        return pltpu.make_async_remote_copy(
            src_ref=send2.at[p], dst_ref=recv2.at[slot],
            send_sem=z_send.at[k], recv_sem=z_recv.at[slot],
            device_id={"sp": 2 * p + par}, device_id_type=MESH,
        )

    def relay(k, _):
        p = lax.rem(q + k, half)
        y_copy(p).wait_recv()
        send2[p] = (wsum[own_rows(p, par), :] + recv1[p].astype(F32)).astype(BF16)
        z_copy(k, p, q).start()
        return 0

    cut1 = 1 + (half - 1 + 2) // 3
    cut2 = cut1 + (half - cut1 + 1) // 2
    lax.fori_loop(1, cut1, relay, 0)

    span = 16
    for ct in range(tiles):
        def tap_block(b, sums, ct=ct):
            start = pl.multiple_of(b * span, span)
            grad = cg[ct, pl.ds(start, span), :]
            new = []
            for k in range(kw):
                prod = grad * source(gp, sh, k + lead, ct, start, span)
                new.append(sums[k] + jnp.sum(prod.reshape(span // 8, 8, LANES), axis=0))
            return tuple(new)

        sums = lax.fori_loop(
            0, rows // span, tap_block, tuple(jnp.zeros((8, LANES), F32) for _ in range(kw))
        )
        for k in range(kw):
            keep_tap(k, ct, sums[k])

    def tap_copy(k, slot):
        peer = lax.rem(sp + k, n)
        return pltpu.make_async_remote_copy(
            src_ref=taploc.at[peer], dst_ref=tapin.at[slot],
            send_sem=tap_send.at[k], recv_sem=tap_recv.at[slot],
            device_id={"sp": peer}, device_id_type=MESH,
        )

    def all_copy(k, slot):
        return pltpu.make_async_remote_copy(
            src_ref=tapsum.at[slot], dst_ref=tapsum.at[slot],
            send_sem=all_send.at[k], recv_sem=all_recv.at[slot],
            device_id={"sp": lax.rem(sp + k, n)}, device_id_type=MESH,
        )

    @pl.loop(1, n)
    def _(k):
        tap_copy(k, sp).start()

    y_copy(q).start()

    lax.fori_loop(cut1, cut2, relay, 0)

    for at in range(0, rows - 8, BLOCK):
        shifted(cg, sh2, at, min(BLOCK, rows - 8 - at))

    def back_block(b, _):
        start = pl.multiple_of(b * BLOCK, BLOCK)
        at = pl.ds(start, BLOCK)
        for ct in range(tiles):
            total = jnp.zeros((BLOCK, LANES), F32)
            for k in range(kw):
                total = total + taps[k : k + 1, lanes(ct)] * source(
                    cg, sh2, reach - k, ct, start, BLOCK
                )
            sig = jax.nn.sigmoid(gate[at, lanes(ct)].astype(F32))
            value_grad[at, lanes(ct)] = (total * sig).astype(BF16)
            gate_grad[at, lanes(ct)] = (
                total * val[at, lanes(ct)].astype(F32) * sig * (1.0 - sig)
            ).astype(BF16)
        return 0

    lax.fori_loop(0, blocks - 1, back_block, 0)

    @pl.when(sp < n - 1)
    def _():
        back_copy.wait_recv()

    @pl.when(sp == n - 1)
    def _():
        cg[:, rows : rows + halo, :] = jnp.zeros((tiles, halo, LANES), F32)

    shifted(cg, sh2, rows - 8, halo)
    back_block(blocks - 1, 0)

    lax.fori_loop(cut2, half, relay, 0)

    def tap_wait(k, total):
        slot = lax.rem(sp + n - k, n)
        tap_copy(k, slot).wait_recv()
        return total + tapin[slot]

    tapsum[sp] = lax.fori_loop(1, n, tap_wait, taploc[sp])

    @pl.loop(1, n)
    def _(k):
        all_copy(k, sp).start()

    y_copy(q).wait_recv()
    w_out[...] = wsum[own_rows(q, par), :] + recv1[q].astype(F32)

    def z_wait(k, _):
        p = lax.rem(q + half - k, half)
        z_copy(k, p, p).wait_recv()
        w_out[...] += recv2[p].astype(F32)
        return 0

    lax.fori_loop(1, half, z_wait, 0)

    @pl.loop(1, n)
    def _(k):
        all_copy(k, lax.rem(sp + n - k, n)).wait_recv()

    for ct in range(tiles):
        for k in range(kw):
            taps_out[k : k + 1, lanes(ct)] = tapsum[k // share, ct, k % share : k % share + 1, :]
        gain_out[:, lanes(ct)] = tapsum[kw // share, ct, kw % share : kw % share + 1, :]

    @pl.when(sp < n - 1)
    def _():
        halo_copy.wait_send()

    @pl.when(sp > 0)
    def _():
        back_copy.wait_send()

    @pl.loop(1, m)
    def _(k):
        stat_copy(k, tp).wait_send()

    @pl.loop(1, n)
    def _(k):
        tap_copy(k, sp).wait_send()
        all_copy(k, sp).wait_send()

    @pl.loop(0, half)
    def _(k):
        y_copy(k).wait_send()

    @pl.loop(1, half)
    def _(k):
        z_copy(k, lax.rem(q + k, half), q).wait_send()


def pair_body(
    n, m, kw,
    val_hbm, gate_hbm, taps_hbm, gain_hbm, mean_hbm, scale_hbm, og_hbm, ow_hbm,
    value_grad, gate_grad, taps_out, gain_out, w_out,
    val, gate, taps_in, gain, mean_row, scale_row, og, ow,
    taps, gp, cg, centered, slope, act, actt, agrad, psum, csum, meanb, scaleb, mpb, mcb,
    halo_out, halo_in, late_stats, head_stats, tapacc, taploc, tapout, tappair, tapz, wsum, ysend, yrecv, zsend, zrecv, xrecv,
    zfown, zfsend, zfin, zfysend, zfyrecv, whole,
    halo_sem, back_sem, stat_sem, pair_sem, tap_sem, y_recv, z_recv, x_recv, zf_recv, zfy_sem, hop,
    load_sem, sent,
):
    rows, chans = val.shape
    tiles = chans // LANES
    depth = og.shape[1]
    dr = depth // n
    half = n // 2
    reach = kw - 1
    halo = halo_out.shape[0]
    lead = halo - reach
    blocks = rows // BLOCK
    zf = chans // 4
    cut = (chans - zf) // 2
    sp = lax.axis_index("sp")
    tp = lax.axis_index("tp")
    par = lax.rem(sp, 2)
    q = lax.div(sp, 2)
    partner = sp + 1 - 2 * par
    low = q < 2
    outer = jnp.logical_or(q == 0, q == 3)
    sib = q + 1 - 2 * lax.rem(q, 2)

    barrier = pltpu.get_barrier_semaphore()

    up, down = q < half - 1, q > 0
    skew = jnp.where(par == 1, sp + 1, sp - 1)
    has_skew = jnp.logical_and(skew >= 0, skew < n)

    def greet(other):
        pl.semaphore_signal(barrier, inc=1, device_id={"sp": other}, device_id_type=MESH)

    greet(partner)

    @pl.when(up)
    def _():
        greet(sp + 2)

    @pl.when(down)
    def _():
        greet(sp - 2)

    @pl.when(has_skew)
    def _():
        greet(skew)

    @pl.loop(1, m)
    def _(k):
        pl.semaphore_signal(
            barrier, inc=1, device_id={"tp": lax.rem(tp + k, m)}, device_id_type=MESH
        )

    loads = [
        pltpu.make_async_copy(source, target, load_sem.at[k])
        for k, (source, target) in enumerate((
            (gate_hbm, gate), (val_hbm, val), (taps_hbm, taps_in), (mean_hbm, mean_row),
            (scale_hbm, scale_row), (gain_hbm, gain), (og_hbm, og), (ow_hbm, ow),
        ))
    ]
    for load in loads:
        load.start()

    def lanes(ct):
        return slice(ct * LANES, (ct + 1) * LANES)

    for load in loads[:6]:
        load.wait()
    tail = slice(rows - halo, rows)
    tail_sig = jax.nn.sigmoid(gate[tail, :].astype(F32))
    halo_out[...] = (val[tail, :].astype(F32) * tail_sig).astype(BF16)
    taps[...] = taps_in[...].astype(F32)

    def gate_block(b, _):
        at = pl.ds(pl.multiple_of(b * BLOCK, BLOCK), BLOCK)
        to = pl.ds(pl.multiple_of(b * BLOCK + halo, 16), BLOCK)
        for ct in range(tiles):
            sig = jax.nn.sigmoid(gate[at, lanes(ct)].astype(F32))
            gp[ct, to, :] = (val[at, lanes(ct)].astype(F32) * sig).astype(BF16).astype(F32)
        return 0

    lax.fori_loop(0, blocks, gate_block, 0)
    meanb[...] = jnp.broadcast_to(mean_row[...], (LANES, rows)).T
    scaleb[...] = jnp.broadcast_to(scale_row[...], (LANES, rows)).T

    def source(ref, shift, ct, start, count):
        return ref[ct, pl.ds(start + shift, count), :]

    def conv_rows(start, count):
        at = pl.ds(start, count)
        for ct in range(tiles):
            conv = jnp.zeros((count, LANES), F32)
            for k in range(kw):
                conv = conv + taps[k : k + 1, lanes(ct)] * source(gp, k + lead, ct, start, count)
            cen = (conv - meanb[at, :]) * scaleb[at, :]
            nor = cen * gain[:, lanes(ct)]
            sig = jax.nn.sigmoid(nor)
            centered[ct, at, :] = cen
            slope[ct, at, :] = sig * (1.0 + nor * (1.0 - sig))
            act[at, lanes(ct)] = (nor * sig).astype(BF16)

    def conv_block(b, _):
        conv_rows(pl.multiple_of(b * BLOCK, BLOCK), BLOCK)
        return 0

    lax.fori_loop(1, 2, conv_block, 0)

    near = up.astype(jnp.int32) + down.astype(jnp.int32) + has_skew.astype(jnp.int32)
    pl.semaphore_wait(barrier, m + near)

    halo_copy = pltpu.make_async_remote_copy(
        src_ref=halo_out, dst_ref=halo_in,
        send_sem=sent.at[0], recv_sem=halo_sem,
        device_id={"sp": lax.rem(sp + 1, n)}, device_id_type=MESH,
    )

    @pl.when(sp < n - 1)
    def _():
        halo_copy.start()

    def tell(r):
        @pl.when(up)
        def _():
            pl.semaphore_signal(
                hop.at[r, 0], inc=1, device_id={"sp": sp + 2}, device_id_type=MESH
            )

        @pl.when(down)
        def _():
            pl.semaphore_signal(
                hop.at[r, 1], inc=1, device_id={"sp": sp - 2}, device_id_type=MESH
            )

    def hear(r):
        @pl.when(down)
        def _():
            pl.semaphore_wait(hop.at[r, 0], 1)

        @pl.when(up)
        def _():
            pl.semaphore_wait(hop.at[r, 1], 1)

    tell(0)
    def turn(chunk):
        at = slice(chunk * LANES, (chunk + 1) * LANES)
        for ct in range(tiles):
            actt[lanes(ct), at] = act[at, lanes(ct)].T

    lax.fori_loop(2, blocks, conv_block, 0)
    conv_rows(halo, BLOCK - halo)
    for chunk in range(1, rows // LANES):
        turn(chunk)

    for load in loads[6:]:
        load.wait()
    slab = min(rows, 256)

    def grad_block(b, _):
        at = pl.ds(pl.multiple_of(b * slab, slab), slab)
        agrad[at, :] = jnp.dot(og[at, :], ow[...], preferred_element_type=F32)
        return 0

    lax.fori_loop(0, rows // slab, grad_block, 0, unroll=True)

    def stat_block(b, sums):
        at = pl.ds(pl.multiple_of(b * BLOCK, BLOCK), BLOCK)
        plain = jnp.zeros((BLOCK, LANES), F32)
        cross = jnp.zeros((BLOCK, LANES), F32)
        new = []
        for ct in range(tiles):
            cen = centered[ct, at, :]
            ngrad = agrad[at, lanes(ct)] * slope[ct, at, :]
            scaled = ngrad * gain[:, lanes(ct)]
            agrad[at, lanes(ct)] = scaled
            plain = plain + scaled
            cross = cross + scaled * cen
            new.append(sums[ct] + jnp.sum((ngrad * cen).reshape(BLOCK // 8, 8, LANES), axis=0))
        psum[at, :] = plain
        csum[at, :] = cross
        return tuple(new)

    first = LANES // BLOCK

    def pack(target, at):
        target[tp, 0:1, :] = jnp.sum(psum[at, :].T, axis=0, keepdims=True)
        target[tp, 1:2, :] = jnp.sum(csum[at, :].T, axis=0, keepdims=True)

    def stat_copy(k, target, c):
        return pltpu.make_async_remote_copy(
            src_ref=target.at[tp], dst_ref=target.at[tp],
            send_sem=sent.at[2 + c], recv_sem=stat_sem.at[c],
            device_id={"tp": lax.rem(tp + k, m)}, device_id_type=MESH,
        )

    def stat_all(target, c):
        others = target.at[pl.ds(0, m - 1)]
        return pltpu.make_async_remote_copy(
            src_ref=others, dst_ref=others,
            send_sem=sent.at[2 + c], recv_sem=stat_sem.at[c],
            device_id={"tp": lax.rem(tp + 1, m)}, device_id_type=MESH,
        )

    def stat_send(target, c):
        @pl.loop(1, m)
        def _(k):
            stat_copy(k, target, c).start()

    gains = lax.fori_loop(
        first, blocks, stat_block, tuple(jnp.zeros((8, LANES), F32) for _ in range(tiles))
    )
    late_rows, head_rows = slice(LANES, rows), slice(0, LANES)
    pack(late_stats, late_rows)
    stat_send(late_stats, 0)

    hear(0)
    tell(1)

    @pl.when(sp > 0)
    def _():
        halo_copy.wait_recv()
        for ct in range(tiles):
            gp[ct, 0:halo, :] = halo_in[:, lanes(ct)].astype(F32)

    @pl.when(sp == 0)
    def _():
        for ct in range(tiles):
            gp[ct, 0:halo, :] = jnp.zeros((halo, LANES), F32)

    conv_rows(0, halo)
    turn(0)
    below = q == 1
    above = q == 2

    def far(i):
        return jnp.where(low, half - 1 - i, i)

    order = [
        jnp.where(below, sib, far(0)),
        jnp.where(below, far(0), far(1)),
        jnp.where(below, far(1), sib),
        q,
    ]
    parts = (slice(0, cut), slice(cut, 2 * cut))
    last = slice(2 * cut, chans)

    def product(block):
        at = pl.ds(pl.multiple_of(block * dr, LANES), dr)
        return jnp.dot(actt[...], og[:, at], preferred_element_type=F32)

    def y_copy(p, s):
        return pltpu.make_async_remote_copy(
            src_ref=ysend.at[p, s], dst_ref=yrecv.at[p, s],
            send_sem=sent.at[6], recv_sem=y_recv.at[p, s],
            device_id={"sp": partner}, device_id_type=MESH,
        )

    def away(p):
        part = product(2 * p + 1 - par)
        for s in range(2):
            ysend[p, s] = part[parts[s], :].astype(BF16)
        zfown[p, 0] = part[last, :]

    def home(p):
        part = product(2 * p + par)
        for s in range(2):
            wsum[p, s] = part[parts[s], :]
        zfown[p, 1] = part[last, :]

    ahead = lax.rem(tp, 2) == 0

    def send(cond, halves):
        @pl.when(cond)
        def _():
            for i, s in halves:
                y_copy(order[i], s).start()

    def zf_copy(i, peer, slot):
        return pltpu.make_async_remote_copy(
            src_ref=zfsend.at[i], dst_ref=zfin.at[slot],
            send_sem=sent.at[8], recv_sem=zf_recv.at[slot],
            device_id={"sp": 2 * peer + par}, device_id_type=MESH,
        )

    def zf_far(i):
        zfsend[i] = zfown[far(i)].astype(BF16)
        zf_copy(i, far(i), jnp.where(outer, 1, 2)).start()

    def zf_sib():
        zfsend[2] = zfown[sib].astype(BF16)
        zf_copy(2, sib, 0).start()

    inner = jnp.logical_not(outer)
    away(order[0])
    send(ahead, ((0, 0), (0, 1)))
    gains = lax.fori_loop(0, first, stat_block, gains)
    pack(head_stats, head_rows)
    stat_send(head_stats, 1)
    away(order[1])
    send(ahead, ((1, 0), (1, 1)))
    hear(1)
    home(order[0])

    @pl.when(jnp.logical_not(below))
    def _():
        zf_far(0)

    home(order[1])

    @pl.when(below)
    def _():
        zf_far(0)

    @pl.when(jnp.logical_not(below))
    def _():
        zf_far(1)

    away(order[2])
    home(order[2])

    @pl.when(below)
    def _():
        zf_far(1)

    @pl.when(inner)
    def _():
        zf_sib()

    send(jnp.logical_not(ahead), [(i, s) for i in (0, 1) for s in range(2)])

    def cg_block(b, _):
        at = pl.ds(pl.multiple_of(b * BLOCK, BLOCK), BLOCK)
        for ct in range(tiles):
            cg[ct, at, :] = scaleb[at, :] * (
                agrad[at, lanes(ct)] - mpb[at, :] - centered[ct, at, :] * mcb[at, :]
            )
        return 0

    def cg_rows(target, c, at, begin, end):
        stat_all(target, c).wait_recv()
        totals = target[0]
        for k in range(1, m):
            totals = totals + target[k]
        totals = totals / (chans * m)
        count = target.shape[2]
        mpb[at, :] = jnp.broadcast_to(totals[0:1, :], (LANES, count)).T
        mcb[at, :] = jnp.broadcast_to(totals[1:2, :], (LANES, count)).T
        lax.fori_loop(begin, end, cg_block, 0)

    cg_rows(late_stats, 0, late_rows, first, blocks)

    span = 32

    def tap_rows(ct, begin, end, sums):
        def tap_block(b, sums):
            start = pl.multiple_of(b * span, span)
            grad = cg[ct, pl.ds(start, span), :]
            new = []
            for k in range(kw):
                prod = grad * source(gp, k + lead, ct, start, span)
                new.append(sums[k] + jnp.sum(prod.reshape(span // 8, 8, LANES), axis=0))
            return tuple(new)

        return lax.fori_loop(begin // span, end // span, tap_block, sums)

    for ct in range(tiles):
        sums = tap_rows(ct, LANES, rows, tuple(jnp.zeros((8, LANES), F32) for _ in range(kw)))
        for k in range(kw):
            tapacc[ct, k] = sums[k]

    def side_copy(i, slot, s):
        return pltpu.make_async_remote_copy(
            src_ref=zsend.at[i, s], dst_ref=zrecv.at[slot, s],
            send_sem=sent.at[7], recv_sem=z_recv.at[slot, s],
            device_id={"sp": 2 * sib + par}, device_id_type=MESH,
        )

    def cross_copy(i, s):
        return pltpu.make_async_remote_copy(
            src_ref=zsend.at[i, s], dst_ref=xrecv.at[s],
            send_sem=sent.at[7], recv_sem=x_recv.at[s],
            device_id={"sp": 2 * order[i] + par}, device_id_type=MESH,
        )

    def relay(i, s):
        p = order[i]
        crossing = (above, inner, below)[i]
        slot = (jnp.where(below, 2, 0), jnp.where(below, 0, 1), jnp.where(below, 1, 2))[i]
        y_copy(p, s).wait_recv()

        @pl.when(jnp.logical_not(crossing))
        def _():
            zsend[i, s] = (wsum[p, s] + yrecv[p, s].astype(F32)).astype(BF16)
            side_copy(i, slot, s).start()

        @pl.when(crossing)
        def _():
            own = wsum[p, s] + yrecv[p, s].astype(F32)
            side_copy(i, slot, s).wait_recv()
            zsend[i, s] = (own + zrecv[slot, s].astype(F32)).astype(BF16)
            cross_copy(i, s).start()

    @pl.when(jnp.logical_and(outer, ahead))
    def _():
        relay(0, 0)

    cg_rows(head_stats, 1, head_rows, 0, first)
    back_copy = pltpu.make_async_remote_copy(
        src_ref=cg.at[:, pl.ds(0, halo), :], dst_ref=cg.at[:, pl.ds(rows, halo), :],
        send_sem=sent.at[1], recv_sem=back_sem,
        device_id={"sp": lax.rem(sp + n - 1, n)}, device_id_type=MESH,
    )

    @pl.when(sp > 0)
    def _():
        back_copy.start()

    for ct in range(tiles):
        sums = tap_rows(ct, 0, LANES, tuple(tapacc[ct, k] for k in range(kw)))
        for k, total in enumerate((*sums, gains[ct])):
            taploc[ct, k : k + 1, :] = jnp.sum(total, axis=0, keepdims=True)

    tapout[...] = taploc[...].astype(BF16)
    pair_copy = pltpu.make_async_remote_copy(
        src_ref=tapout, dst_ref=tappair, send_sem=sent.at[4], recv_sem=pair_sem,
        device_id={"sp": partner}, device_id_type=MESH,
    )
    pair_copy.start()
    for s in range(2):
        y_copy(order[2], s).start()
    away(order[3])
    for s in range(2):
        y_copy(order[3], s).start()
    home(order[3])
    @pl.when(jnp.logical_and(outer, jnp.logical_not(ahead)))
    def _():
        relay(0, 0)

    @pl.when(outer)
    def _():
        relay(0, 1)

    @pl.when(below)
    def _():
        relay(0, 0)


    def back_block(b, _):
        start = pl.multiple_of(b * BLOCK, BLOCK)
        at = pl.ds(start, BLOCK)
        for ct in range(tiles):
            total = jnp.zeros((BLOCK, LANES), F32)
            for k in range(kw):
                total = total + taps[k : k + 1, lanes(ct)] * source(cg, reach - k, ct, start, BLOCK)
            sig = jax.nn.sigmoid(gate[at, lanes(ct)].astype(F32))
            value_grad[at, lanes(ct)] = (total * sig).astype(BF16)
            gate_grad[at, lanes(ct)] = (
                total * val[at, lanes(ct)].astype(F32) * sig * (1.0 - sig)
            ).astype(BF16)
        return 0

    lax.fori_loop(0, blocks // 2, back_block, 0)

    @pl.when(outer)
    def _():
        relay(1, 0)
        relay(1, 1)
        zf_sib()

    @pl.when(below)
    def _():
        relay(0, 1)

    pair_copy.wait_recv()
    tapz[q] = (tapout[...].astype(F32) + tappair[...].astype(F32)).astype(BF16)

    def tap_copy(k, source_ref):
        return pltpu.make_async_remote_copy(
            src_ref=source_ref, dst_ref=source_ref,
            send_sem=sent.at[5], recv_sem=tap_sem,
            device_id={"sp": 2 * lax.rem(q + k, half) + par}, device_id_type=MESH,
        )

    @pl.loop(1, half)
    def _(k):
        tap_copy(k, tapz.at[q]).start()

    tap_all = tap_copy(1, tapz.at[pl.ds(0, half - 1)])

    lax.fori_loop(blocks // 2, blocks - 1, back_block, 0)

    @pl.when(above)
    def _():
        relay(0, 0)
        relay(0, 1)

    @pl.when(inner)
    def _():
        relay(1, 0)

    @pl.when(inner)
    def _():
        relay(1, 1)

    relay(2, 0)
    @pl.when(sp < n - 1)
    def _():
        back_copy.wait_recv()

    @pl.when(sp == n - 1)
    def _():
        cg[:, rows : rows + halo, :] = jnp.zeros((tiles, halo, LANES), F32)

    back_block(blocks - 1, 0)

    relay(2, 1)

    for slot in range(half - 1):
        zf_copy(0, sib, slot).wait_recv()
    for k in range(2):
        zfown[q, k] += (
            zfin[0, k].astype(F32) + zfin[1, k].astype(F32) + zfin[2, k].astype(F32)
        )
    zfysend[...] = zfown[q, 0].astype(BF16)
    zf_back = pltpu.make_async_remote_copy(
        src_ref=zfysend, dst_ref=zfyrecv, send_sem=sent.at[9], recv_sem=zfy_sem,
        device_id={"sp": partner}, device_id_type=MESH,
    )
    zf_back.start()

    for s in range(2):
        y_copy(q, s).wait_recv()
        wsum[q, s] += yrecv[q, s].astype(F32)
    tap_all.wait_recv()

    for ct in range(tiles):
        total = tapz[0, ct].astype(F32)
        for k in range(1, half):
            total = total + tapz[k, ct].astype(F32)
        taps_out[:, lanes(ct)] = total[0:kw]
        gain_out[:, lanes(ct)] = total[kw : kw + 1]

    for s in range(2):
        side_copy(0, 2, s).wait_recv()
        cross_copy(0, s).wait_recv()
        whole[parts[s], :] = wsum[q, s] + zrecv[2, s].astype(F32) + xrecv[s].astype(F32)
    zf_back.wait_recv()
    whole[last, :] = zfown[q, 1] + zfyrecv[...].astype(F32)
    w_out[...] = whole[...].T

    @pl.when(sp < n - 1)
    def _():
        halo_copy.wait_send()

    @pl.when(sp > 0)
    def _():
        back_copy.wait_send()

    stat_all(late_stats, 0).wait_send()
    stat_all(head_stats, 1).wait_send()
    pair_copy.wait_send()
    tap_all.wait_send()
    pltpu.make_async_remote_copy(
        src_ref=ysend, dst_ref=yrecv, send_sem=sent.at[6], recv_sem=y_recv.at[0, 0],
        device_id={"sp": partner}, device_id_type=MESH,
    ).wait_send()
    pltpu.make_async_remote_copy(
        src_ref=zsend, dst_ref=zrecv, send_sem=sent.at[7], recv_sem=z_recv.at[0, 0],
        device_id={"sp": partner}, device_id_type=MESH,
    ).wait_send()
    pltpu.make_async_remote_copy(
        src_ref=zfsend, dst_ref=zfin, send_sem=sent.at[8], recv_sem=zf_recv.at[0],
        device_id={"sp": partner}, device_id_type=MESH,
    ).wait_send()
    zf_back.wait_send()


def finish(count, *refs):
    sem = refs[-1]
    copies = [
        pltpu.make_async_copy(source, target, sem.at[k])
        for k, (source, target) in enumerate(zip(refs[:count], refs[count : 2 * count]))
    ]
    for copy in copies:
        copy.start()
    for copy in copies:
        copy.wait()


def pair_kernel(n, m, kw, *refs):
    pl.run_scoped(
        functools.partial(pair_body, n, m, kw, *refs),
        pltpu.SemaphoreType.DMA((8,)), pltpu.SemaphoreType.DMA((10,)),
    )


def outputs(rows, chans, kw, dr):
    return (
        pltpu.VMEM((rows, chans), BF16),
        pltpu.VMEM((rows, chans), BF16),
        pltpu.VMEM((kw, chans), F32),
        pltpu.VMEM((1, chans), F32),
        pltpu.VMEM((dr, chans), F32),
    )


def pair_call(n, m, rows, chans, kw, depth):
    dr = depth // n
    half = n // 2
    tiles = chans // LANES
    halo = rup(kw - 1, 16)
    taps_rows = rup(kw + 1, 16)
    zf = chans // 4
    cut = (chans - zf) // 2
    vm = pltpu.VMEM
    dma = pltpu.SemaphoreType.DMA
    wide = vm((rows, LANES), F32)
    block = vm((half, 2, cut, dr), BF16)
    part = vm((half - 1, 2, cut, dr), BF16)
    return pl.pallas_call(
        functools.partial(pair_kernel, n, m, kw),
        out_shape=outputs(rows, chans, kw, dr),
        in_specs=[pl.BlockSpec(memory_space=pltpu.HBM)] * 8,
        out_specs=(pl.BlockSpec(memory_space=pltpu.VMEM),) * 5,
        scratch_shapes=[
            vm((rows, chans), BF16), vm((rows, chans), BF16), vm((kw, chans), BF16),
            vm((1, chans), F32), vm((1, rows), F32), vm((1, rows), F32),
            vm((rows, depth), BF16), vm((depth, chans), BF16),
            vm((kw, chans), F32),
            vm((tiles, rows + halo, LANES), F32),
            vm((tiles, rows + halo, LANES), F32),
            vm((tiles, rows, LANES), F32),
            vm((tiles, rows, LANES), F32),
            vm((rows, chans), BF16),
            vm((chans, rows), BF16),
            vm((rows, chans), F32),
            wide, wide, wide, wide, wide, wide,
            vm((halo, chans), BF16), vm((halo, chans), BF16),
            vm((m, 2, rows - LANES), F32), vm((m, 2, LANES), F32), vm((tiles, kw, 8, LANES), F32),
            vm((tiles, taps_rows, LANES), F32), vm((tiles, taps_rows, LANES), BF16),
            vm((tiles, taps_rows, LANES), BF16),
            vm((half, tiles, taps_rows, LANES), BF16),
            vm((half, 2, cut, dr), F32),
            block, block, part, part, vm((2, cut, dr), BF16),
            vm((half, 2, zf, dr), F32), vm((half - 1, 2, zf, dr), BF16), vm((half - 1, 2, zf, dr), BF16),
            vm((zf, dr), BF16), vm((zf, dr), BF16), vm((chans, dr), F32),
            dma, dma, dma((2,)), dma, dma, dma((half, 2)), dma((half - 1, 2)), dma((2,)),
            dma((half - 1,)), dma,
            pltpu.SemaphoreType.REGULAR((half - 2, 2)),
        ],
        compiler_params=pltpu.CompilerParams(
            collective_id=0, has_side_effects=True, vmem_limit_bytes=VMEM_LIMIT,
        ),
    )


def wide_call(n, m, rows, chans, kw, depth):
    dr = depth // n
    half = n // 2
    tiles = chans // LANES
    halo = rup(kw - 1, 16)
    vm = pltpu.VMEM
    dma = pltpu.SemaphoreType.DMA
    whole = pl.BlockSpec(memory_space=pltpu.VMEM)
    far = pl.BlockSpec(memory_space=pltpu.HBM)
    return pl.pallas_call(
        functools.partial(kernel, n, m, kw),
        out_shape=outputs(rows, chans, kw, dr),
        in_specs=[whole] * 6 + [far] * 2,
        out_specs=(whole,) * 5,
        scratch_shapes=[
            vm((kw, chans), F32),
            vm((rows, depth), BF16),
            vm((depth, chans), BF16),
            vm((tiles, rows + halo, LANES), F32),
            vm((7, tiles, rows + halo, LANES), F32),
            vm((tiles, rows + halo, LANES), F32),
            vm((7, tiles, rows + halo, LANES), F32),
            vm((tiles, rows, LANES), F32),
            vm((tiles, rows, LANES), F32),
            vm((rows, chans), BF16),
            vm((rows, chans), F32),
            vm((rows, LANES), F32),
            vm((rows, LANES), F32),
            vm((rows, LANES), F32),
            vm((rows, LANES), F32),
            vm((rows, LANES), F32),
            vm((rows, LANES), F32),
            vm((halo, chans), BF16),
            vm((halo, chans), BF16),
            vm((m, 2, rows), F32),
            vm((n, tiles, rup(kw + 1, n) // n, LANES), F32),
            vm((n, tiles, rup(kw + 1, n) // n, LANES), F32),
            vm((n, tiles, rup(kw + 1, n) // n, LANES), F32),
            vm((depth, chans), F32),
            vm((depth, chans), BF16),
            vm((half, dr, chans), BF16),
            vm((half, dr, chans), BF16),
            vm((half, dr, chans), BF16),
            dma((2,)), dma((2,)), dma((2,)),
            dma((m,)), dma((m,)), dma((n,)), dma((n,)), dma((n,)), dma((n,)),
            dma((half,)), dma((half,)), dma((half,)), dma((half,)),
        ],
        compiler_params=pltpu.CompilerParams(
            collective_id=0, has_side_effects=True, vmem_limit_bytes=VMEM_LIMIT
        ),
    )


def per_device(
    n, m, glu_value, glu_gate, conv_taps, norm_gain, out_weight, norm_mean, norm_scale, out_grad
):
    rows, chans = glu_value.shape
    kw = conv_taps.shape[0]
    depth = out_grad.shape[1]
    paired = n == 8 and (depth // n) % LANES == 0 and chans % (2 * LANES) == 0
    call = (pair_call if paired else wide_call)(n, m, rows, chans, kw, depth)
    out = call(*[
        pltpu.with_memory_space_constraint(x, pltpu.HBM)
        for x in (
            glu_value, glu_gate, conv_taps, norm_gain[None, :],
            norm_mean[None, :], norm_scale[None, :], out_grad, out_weight,
        )
    ])
    whole = pl.BlockSpec(memory_space=pltpu.VMEM)
    out = pl.pallas_call(
        functools.partial(finish, len(out)),
        out_shape=tuple(jax.ShapeDtypeStruct(x.shape, x.dtype) for x in out),
        in_specs=[whole] * len(out),
        out_specs=(pl.BlockSpec(memory_space=pltpu.HBM),) * len(out),
        scratch_shapes=[pltpu.SemaphoreType.DMA((len(out),))],
        compiler_params=pltpu.CompilerParams(vmem_limit_bytes=2 * 1024 * 1024),
    )(*out)
    value_grad, gate_grad, taps_grad, gain_grad, weight_grad = out
    return value_grad, gate_grad, taps_grad, gain_grad[0], weight_grad


def solution(mesh):
    placed = (
        P("sp", "tp"), P("sp", "tp"), P(None, "tp"), P("tp"),
        P(None, "tp"), P("sp"), P("sp"), P("sp", None),
    )
    return jax.shard_map(
        functools.partial(per_device, mesh.shape["sp"], mesh.shape["tp"]),
        mesh=mesh,
        in_specs=placed,
        out_specs=(P("sp", "tp"), P("sp", "tp"), P(None, "tp"), P("tp"), P("sp", "tp")),
        check_vma=False,
    )
```

```python
import functools

import jax
import jax.numpy as jnp
from jax import lax
from jax.experimental import pallas as pl
from jax.experimental.pallas import tpu as pltpu
from jax.sharding import PartitionSpec as P

MESH = pl.DeviceIdType.MESH
F32 = jnp.float32
BF16 = jnp.bfloat16
LANES = 128
VMEM_LIMIT = 30 * 1024 * 1024
BLOCK = 64


def rup(value, unit):
    return -(-value // unit) * unit


def kernel(
    n, m, kw,
    val, gate, taps_in, gain, mean_row, scale_row, og_hbm, ow_hbm,
    value_grad, gate_grad, taps_out, gain_out, w_out,
    taps, og, ow, gp, sh, cg, sh2, centered, slope, act, agrad, psum, csum, meanb, scaleb,
    mpb, mcb, halo_out, halo_in, stats, taploc, tapin, tapsum, wsum, wbf, recv1, send2, recv2,
    load_sem, halo_sem, back_sem, stat_send, stat_recv, tap_send, tap_recv, all_send, all_recv,
    y_send, y_recv, z_send, z_recv,
):
    rows, chans = val.shape
    tiles = chans // LANES
    depth = og.shape[1]
    dr = depth // n
    half = n // 2
    reach = kw - 1
    halo = halo_out.shape[0]
    lead = halo - reach
    blocks = rows // BLOCK
    sp = lax.axis_index("sp")
    tp = lax.axis_index("tp")
    par = lax.rem(sp, 2)
    q = lax.div(sp, 2)
    partner = sp + 1 - 2 * par

    load_og = pltpu.make_async_copy(og_hbm, og, load_sem.at[0])
    load_ow = pltpu.make_async_copy(ow_hbm, ow, load_sem.at[1])
    load_og.start()
    load_ow.start()

    barrier = pltpu.get_barrier_semaphore()

    @pl.loop(1, n)
    def _(k):
        pl.semaphore_signal(
            barrier, inc=1, device_id={"sp": lax.rem(sp + k, n)}, device_id_type=MESH
        )

    @pl.loop(1, m)
    def _(k):
        pl.semaphore_signal(
            barrier, inc=1, device_id={"tp": lax.rem(tp + k, m)}, device_id_type=MESH
        )

    def lanes(ct):
        return slice(ct * LANES, (ct + 1) * LANES)

    taps[...] = taps_in[...].astype(F32)
    tail = slice(rows - halo, rows)
    tail_sig = jax.nn.sigmoid(gate[tail, :].astype(F32))
    halo_out[...] = (val[tail, :].astype(F32) * tail_sig).astype(BF16)

    def gate_block(b, _):
        at = pl.ds(pl.multiple_of(b * BLOCK, BLOCK), BLOCK)
        to = pl.ds(pl.multiple_of(b * BLOCK + halo, 16), BLOCK)
        for ct in range(tiles):
            sig = jax.nn.sigmoid(gate[at, lanes(ct)].astype(F32))
            gp[ct, to, :] = (val[at, lanes(ct)].astype(F32) * sig).astype(BF16).astype(F32)
        return 0

    lax.fori_loop(0, blocks, gate_block, 0)

    load_og.wait()
    load_ow.wait()
    slab = min(rows, 128)

    def grad_block(b, _):
        at = pl.ds(pl.multiple_of(b * slab, slab), slab)
        agrad[at, :] = jnp.dot(og[at, :], ow[...], preferred_element_type=F32)
        return 0

    lax.fori_loop(0, rows // slab, grad_block, 0)

    pl.semaphore_wait(barrier, n - 1 + m - 1)

    halo_copy = pltpu.make_async_remote_copy(
        src_ref=halo_out, dst_ref=halo_in,
        send_sem=halo_sem.at[0], recv_sem=halo_sem.at[1],
        device_id={"sp": lax.rem(sp + 1, n)}, device_id_type=MESH,
    )

    @pl.when(sp < n - 1)
    def _():
        halo_copy.start()

    def shifted(src, dst, begin, count):
        for ct in range(tiles):
            for r in range(1, 8):
                dst[r - 1, ct, begin : begin + count, :] = src[ct, begin + r : begin + r + count, :]

    for at in range(halo, rows + halo - 8, BLOCK):
        shifted(gp, sh, at, min(BLOCK, rows + halo - 8 - at))
    meanb[...] = jnp.broadcast_to(mean_row[...], (LANES, rows)).T
    scaleb[...] = jnp.broadcast_to(scale_row[...], (LANES, rows)).T

    def source(base_ref, copies, shift, ct, start, count):
        r, base = shift % 8, shift - shift % 8
        at = pl.ds(pl.multiple_of(start + base, 8), count)
        if r == 0:
            return base_ref[ct, at, :]
        return copies[r - 1, ct, at, :]

    def conv_block(b, _):
        start = pl.multiple_of(b * BLOCK, BLOCK)
        at = pl.ds(start, BLOCK)
        for ct in range(tiles):
            conv = jnp.zeros((BLOCK, LANES), F32)
            for k in range(kw):
                conv = conv + taps[k : k + 1, lanes(ct)] * source(gp, sh, k + lead, ct, start, BLOCK)
            cen = (conv - meanb[at, :]) * scaleb[at, :]
            nor = cen * gain[:, lanes(ct)]
            sig = jax.nn.sigmoid(nor)
            centered[ct, at, :] = cen
            slope[ct, at, :] = sig * (1.0 + nor * (1.0 - sig))
            act[at, lanes(ct)] = (nor * sig).astype(BF16)
        return 0

    lax.fori_loop(1, blocks, conv_block, 0)

    @pl.when(sp > 0)
    def _():
        halo_copy.wait_recv()
        for ct in range(tiles):
            gp[ct, 0:halo, :] = halo_in[:, lanes(ct)].astype(F32)

    @pl.when(sp == 0)
    def _():
        for ct in range(tiles):
            gp[ct, 0:halo, :] = jnp.zeros((halo, LANES), F32)

    shifted(gp, sh, 0, halo)
    conv_block(0, 0)

    wide = max(dr, min(depth, 256))

    def w_tile(start):
        start = pl.multiple_of(start, wide)
        part = lax.dot_general(
            og[:, pl.ds(start, wide)], act[...], (((0,), (0,)), ((), ())),
            preferred_element_type=F32,
        )
        wsum[pl.ds(start, wide), :] = part
        wbf[pl.ds(start, wide), :] = part.astype(BF16)

    def own_rows(p, side):
        return pl.ds(pl.multiple_of((2 * p + side) * dr, dr), dr)

    def y_copy(p):
        return pltpu.make_async_remote_copy(
            src_ref=wbf.at[own_rows(p, 1 - par), :], dst_ref=recv1.at[p],
            send_sem=y_send.at[p], recv_sem=y_recv.at[p],
            device_id={"sp": partner}, device_id_type=MESH,
        )

    def partner_step(k, _):
        p = lax.rem(q + k, half)
        w_tile((2 * p + 1 - par) * dr)
        y_copy(p).start()
        return 0

    def own_step(k, _):
        w_tile((2 * lax.rem(q + k, half) + par) * dr)
        return 0

    if wide == dr:
        lax.fori_loop(1, half, partner_step, 0)
        w_tile((2 * q + 1 - par) * dr)
    else:
        def tile_step(j, _):
            w_tile(j * wide)
            return 0

        lax.fori_loop(0, depth // wide, tile_step, 0)

        def send_step(k, _):
            y_copy(lax.rem(q + k, half)).start()
            return 0

        lax.fori_loop(1, half, send_step, 0)

    def stat_block(b, sums):
        at = pl.ds(pl.multiple_of(b * BLOCK, BLOCK), BLOCK)
        plain = jnp.zeros((BLOCK, LANES), F32)
        cross = jnp.zeros((BLOCK, LANES), F32)
        new = []
        for ct in range(tiles):
            cen = centered[ct, at, :]
            ngrad = agrad[at, lanes(ct)] * slope[ct, at, :]
            scaled = ngrad * gain[:, lanes(ct)]
            agrad[at, lanes(ct)] = scaled
            plain = plain + scaled
            cross = cross + scaled * cen
            new.append(sums[ct] + jnp.sum((ngrad * cen).reshape(BLOCK // 8, 8, LANES), axis=0))
        psum[at, :] = plain
        csum[at, :] = cross
        return tuple(new)

    gains = lax.fori_loop(
        0, blocks, stat_block, tuple(jnp.zeros((8, LANES), F32) for _ in range(tiles))
    )
    stats[tp, 0:1, :] = jnp.sum(psum[...].T, axis=0, keepdims=True)
    stats[tp, 1:2, :] = jnp.sum(csum[...].T, axis=0, keepdims=True)

    def stat_copy(k, slot):
        return pltpu.make_async_remote_copy(
            src_ref=stats.at[slot], dst_ref=stats.at[slot],
            send_sem=stat_send.at[k], recv_sem=stat_recv.at[slot],
            device_id={"tp": lax.rem(tp + k, m)}, device_id_type=MESH,
        )

    @pl.loop(1, m)
    def _(k):
        stat_copy(k, tp).start()

    if wide == dr:
        lax.fori_loop(1, half + 1, own_step, 0)

    share = taploc.shape[2]

    def keep_tap(k, ct, sums):
        taploc[k // share, ct, k % share : k % share + 1, :] = jnp.sum(sums, axis=0, keepdims=True)

    for ct in range(tiles):
        keep_tap(kw, ct, gains[ct])
        for k in range(kw + 1, n * share):
            keep_tap(k, ct, jnp.zeros((8, LANES), F32))

    @pl.loop(1, m)
    def _(k):
        stat_copy(k, lax.rem(tp + m - k, m)).wait_recv()

    totals = stats[0]
    for k in range(1, m):
        totals = totals + stats[k]
    totals = totals / (chans * m)
    mpb[...] = jnp.broadcast_to(totals[0:1, :], (LANES, rows)).T
    mcb[...] = jnp.broadcast_to(totals[1:2, :], (LANES, rows)).T

    def cg_block(b, _):
        at = pl.ds(pl.multiple_of(b * BLOCK, BLOCK), BLOCK)
        for ct in range(tiles):
            cg[ct, at, :] = scaleb[at, :] * (
                agrad[at, lanes(ct)] - mpb[at, :] - centered[ct, at, :] * mcb[at, :]
            )
        return 0

    lax.fori_loop(0, blocks, cg_block, 0)
    back_copy = pltpu.make_async_remote_copy(
        src_ref=cg.at[:, pl.ds(0, halo), :], dst_ref=cg.at[:, pl.ds(rows, halo), :],
        send_sem=back_sem.at[0], recv_sem=back_sem.at[1],
        device_id={"sp": lax.rem(sp + n - 1, n)}, device_id_type=MESH,
    )

    @pl.when(sp > 0)
    def _():
        back_copy.start()

    def z_copy(k, p, slot):
        return pltpu.make_async_remote_copy(
            src_ref=send2.at[p], dst_ref=recv2.at[slot],
            send_sem=z_send.at[k], recv_sem=z_recv.at[slot],
            device_id={"sp": 2 * p + par}, device_id_type=MESH,
        )

    def relay(k, _):
        p = lax.rem(q + k, half)
        y_copy(p).wait_recv()
        send2[p] = (wsum[own_rows(p, par), :] + recv1[p].astype(F32)).astype(BF16)
        z_copy(k, p, q).start()
        return 0

    cut1 = 1 + (half - 1 + 2) // 3
    cut2 = cut1 + (half - cut1 + 1) // 2
    lax.fori_loop(1, cut1, relay, 0)

    span = 16
    for ct in range(tiles):
        def tap_block(b, sums, ct=ct):
            start = pl.multiple_of(b * span, span)
            grad = cg[ct, pl.ds(start, span), :]
            new = []
            for k in range(kw):
                prod = grad * source(gp, sh, k + lead, ct, start, span)
                new.append(sums[k] + jnp.sum(prod.reshape(span // 8, 8, LANES), axis=0))
            return tuple(new)

        sums = lax.fori_loop(
            0, rows // span, tap_block, tuple(jnp.zeros((8, LANES), F32) for _ in range(kw))
        )
        for k in range(kw):
            keep_tap(k, ct, sums[k])

    def tap_copy(k, slot):
        peer = lax.rem(sp + k, n)
        return pltpu.make_async_remote_copy(
            src_ref=taploc.at[peer], dst_ref=tapin.at[slot],
            send_sem=tap_send.at[k], recv_sem=tap_recv.at[slot],
            device_id={"sp": peer}, device_id_type=MESH,
        )

    def all_copy(k, slot):
        return pltpu.make_async_remote_copy(
            src_ref=tapsum.at[slot], dst_ref=tapsum.at[slot],
            send_sem=all_send.at[k], recv_sem=all_recv.at[slot],
            device_id={"sp": lax.rem(sp + k, n)}, device_id_type=MESH,
        )

    @pl.loop(1, n)
    def _(k):
        tap_copy(k, sp).start()

    y_copy(q).start()

    lax.fori_loop(cut1, cut2, relay, 0)

    for at in range(0, rows - 8, BLOCK):
        shifted(cg, sh2, at, min(BLOCK, rows - 8 - at))

    def back_block(b, _):
        start = pl.multiple_of(b * BLOCK, BLOCK)
        at = pl.ds(start, BLOCK)
        for ct in range(tiles):
            total = jnp.zeros((BLOCK, LANES), F32)
            for k in range(kw):
                total = total + taps[k : k + 1, lanes(ct)] * source(
                    cg, sh2, reach - k, ct, start, BLOCK
                )
            sig = jax.nn.sigmoid(gate[at, lanes(ct)].astype(F32))
            value_grad[at, lanes(ct)] = (total * sig).astype(BF16)
            gate_grad[at, lanes(ct)] = (
                total * val[at, lanes(ct)].astype(F32) * sig * (1.0 - sig)
            ).astype(BF16)
        return 0

    lax.fori_loop(0, blocks - 1, back_block, 0)

    @pl.when(sp < n - 1)
    def _():
        back_copy.wait_recv()

    @pl.when(sp == n - 1)
    def _():
        cg[:, rows : rows + halo, :] = jnp.zeros((tiles, halo, LANES), F32)

    shifted(cg, sh2, rows - 8, halo)
    back_block(blocks - 1, 0)

    lax.fori_loop(cut2, half, relay, 0)

    def tap_wait(k, total):
        slot = lax.rem(sp + n - k, n)
        tap_copy(k, slot).wait_recv()
        return total + tapin[slot]

    tapsum[sp] = lax.fori_loop(1, n, tap_wait, taploc[sp])

    @pl.loop(1, n)
    def _(k):
        all_copy(k, sp).start()

    y_copy(q).wait_recv()
    w_out[...] = wsum[own_rows(q, par), :] + recv1[q].astype(F32)

    def z_wait(k, _):
        p = lax.rem(q + half - k, half)
        z_copy(k, p, p).wait_recv()
        w_out[...] += recv2[p].astype(F32)
        return 0

    lax.fori_loop(1, half, z_wait, 0)

    @pl.loop(1, n)
    def _(k):
        all_copy(k, lax.rem(sp + n - k, n)).wait_recv()

    for ct in range(tiles):
        for k in range(kw):
            taps_out[k : k + 1, lanes(ct)] = tapsum[k // share, ct, k % share : k % share + 1, :]
        gain_out[:, lanes(ct)] = tapsum[kw // share, ct, kw % share : kw % share + 1, :]

    @pl.when(sp < n - 1)
    def _():
        halo_copy.wait_send()

    @pl.when(sp > 0)
    def _():
        back_copy.wait_send()

    @pl.loop(1, m)
    def _(k):
        stat_copy(k, tp).wait_send()

    @pl.loop(1, n)
    def _(k):
        tap_copy(k, sp).wait_send()
        all_copy(k, sp).wait_send()

    @pl.loop(0, half)
    def _(k):
        y_copy(k).wait_send()

    @pl.loop(1, half)
    def _(k):
        z_copy(k, lax.rem(q + k, half), q).wait_send()


def pair_body(
    n, m, kw,
    val_hbm, gate_hbm, taps_hbm, gain_hbm, mean_hbm, scale_hbm, og_hbm, ow_hbm,
    value_grad, gate_grad, taps_out, gain_out, w_out,
    val, gate, taps_in, gain, mean_row, scale_row, og, ow,
    taps, gp, cg, centered, slope, act, actt, agrad, psum, csum, meanb, scaleb, mpb, mcb,
    halo_out, halo_in, late_stats, head_stats, tapacc, taploc, tapout, tappair, tapz, wsum, ysend, yrecv, zsend, zrecv, xrecv,
    zfown, zfsend, zfin, zfysend, zfyrecv, whole,
    halo_sem, back_sem, stat_sem, pair_sem, tap_sem, y_recv, z_recv, x_recv, zf_recv, zfy_sem, hop,
    load_sem, sent,
):
    rows, chans = val.shape
    tiles = chans // LANES
    depth = og.shape[1]
    dr = depth // n
    half = n // 2
    reach = kw - 1
    halo = halo_out.shape[0]
    lead = halo - reach
    blocks = rows // BLOCK
    zf = chans // 4
    cut = (chans - zf) // 2
    sp = lax.axis_index("sp")
    tp = lax.axis_index("tp")
    par = lax.rem(sp, 2)
    q = lax.div(sp, 2)
    partner = sp + 1 - 2 * par
    low = q < 2
    outer = jnp.logical_or(q == 0, q == 3)
    sib = q + 1 - 2 * lax.rem(q, 2)

    barrier = pltpu.get_barrier_semaphore()

    up, down = q < half - 1, q > 0
    skew = jnp.where(par == 1, sp + 1, sp - 1)
    has_skew = jnp.logical_and(skew >= 0, skew < n)

    def greet(other):
        pl.semaphore_signal(barrier, inc=1, device_id={"sp": other}, device_id_type=MESH)

    greet(partner)

    @pl.when(up)
    def _():
        greet(sp + 2)

    @pl.when(down)
    def _():
        greet(sp - 2)

    @pl.when(has_skew)
    def _():
        greet(skew)

    @pl.loop(1, m)
    def _(k):
        pl.semaphore_signal(
            barrier, inc=1, device_id={"tp": lax.rem(tp + k, m)}, device_id_type=MESH
        )

    loads = [
        pltpu.make_async_copy(source, target, load_sem.at[k])
        for k, (source, target) in enumerate((
            (gate_hbm, gate), (val_hbm, val), (taps_hbm, taps_in), (mean_hbm, mean_row),
            (scale_hbm, scale_row), (gain_hbm, gain), (og_hbm, og), (ow_hbm, ow),
        ))
    ]
    for load in loads:
        load.start()

    def lanes(ct):
        return slice(ct * LANES, (ct + 1) * LANES)

    for load in loads[:6]:
        load.wait()
    tail = slice(rows - halo, rows)
    tail_sig = jax.nn.sigmoid(gate[tail, :].astype(F32))
    halo_out[...] = (val[tail, :].astype(F32) * tail_sig).astype(BF16)
    taps[...] = taps_in[...].astype(F32)

    def gate_block(b, _):
        at = pl.ds(pl.multiple_of(b * BLOCK, BLOCK), BLOCK)
        to = pl.ds(pl.multiple_of(b * BLOCK + halo, 16), BLOCK)
        for ct in range(tiles):
            sig = jax.nn.sigmoid(gate[at, lanes(ct)].astype(F32))
            gp[ct, to, :] = (val[at, lanes(ct)].astype(F32) * sig).astype(BF16).astype(F32)
        return 0

    lax.fori_loop(0, blocks, gate_block, 0)
    meanb[...] = jnp.broadcast_to(mean_row[...], (LANES, rows)).T
    scaleb[...] = jnp.broadcast_to(scale_row[...], (LANES, rows)).T

    def source(ref, shift, ct, start, count):
        return ref[ct, pl.ds(start + shift, count), :]

    def conv_rows(start, count):
        at = pl.ds(start, count)
        for ct in range(tiles):
            conv = jnp.zeros((count, LANES), F32)
            for k in range(kw):
                conv = conv + taps[k : k + 1, lanes(ct)] * source(gp, k + lead, ct, start, count)
            cen = (conv - meanb[at, :]) * scaleb[at, :]
            nor = cen * gain[:, lanes(ct)]
            sig = jax.nn.sigmoid(nor)
            centered[ct, at, :] = cen
            slope[ct, at, :] = sig * (1.0 + nor * (1.0 - sig))
            act[at, lanes(ct)] = (nor * sig).astype(BF16)

    def conv_block(b, _):
        conv_rows(pl.multiple_of(b * BLOCK, BLOCK), BLOCK)
        return 0

    lax.fori_loop(1, 2, conv_block, 0)

    near = up.astype(jnp.int32) + down.astype(jnp.int32) + has_skew.astype(jnp.int32)
    pl.semaphore_wait(barrier, m + near)

    halo_copy = pltpu.make_async_remote_copy(
        src_ref=halo_out, dst_ref=halo_in,
        send_sem=sent.at[0], recv_sem=halo_sem,
        device_id={"sp": lax.rem(sp + 1, n)}, device_id_type=MESH,
    )

    @pl.when(sp < n - 1)
    def _():
        halo_copy.start()

    def tell(r):
        @pl.when(up)
        def _():
            pl.semaphore_signal(
                hop.at[r, 0], inc=1, device_id={"sp": sp + 2}, device_id_type=MESH
            )

        @pl.when(down)
        def _():
            pl.semaphore_signal(
                hop.at[r, 1], inc=1, device_id={"sp": sp - 2}, device_id_type=MESH
            )

    def hear(r):
        @pl.when(down)
        def _():
            pl.semaphore_wait(hop.at[r, 0], 1)

        @pl.when(up)
        def _():
            pl.semaphore_wait(hop.at[r, 1], 1)

    tell(0)
    def turn(chunk):
        at = slice(chunk * LANES, (chunk + 1) * LANES)
        for ct in range(tiles):
            actt[lanes(ct), at] = act[at, lanes(ct)].T

    lax.fori_loop(2, blocks, conv_block, 0)
    conv_rows(halo, BLOCK - halo)
    for chunk in range(1, rows // LANES):
        turn(chunk)

    for load in loads[6:]:
        load.wait()
    slab = min(rows, 256)

    def grad_block(b, _):
        at = pl.ds(pl.multiple_of(b * slab, slab), slab)
        agrad[at, :] = jnp.dot(og[at, :], ow[...], preferred_element_type=F32)
        return 0

    lax.fori_loop(0, rows // slab, grad_block, 0, unroll=True)

    def stat_block(b, sums):
        at = pl.ds(pl.multiple_of(b * BLOCK, BLOCK), BLOCK)
        plain = jnp.zeros((BLOCK, LANES), F32)
        cross = jnp.zeros((BLOCK, LANES), F32)
        new = []
        for ct in range(tiles):
            cen = centered[ct, at, :]
            ngrad = agrad[at, lanes(ct)] * slope[ct, at, :]
            scaled = ngrad * gain[:, lanes(ct)]
            agrad[at, lanes(ct)] = scaled
            plain = plain + scaled
            cross = cross + scaled * cen
            new.append(sums[ct] + jnp.sum((ngrad * cen).reshape(BLOCK // 8, 8, LANES), axis=0))
        psum[at, :] = plain
        csum[at, :] = cross
        return tuple(new)

    first = LANES // BLOCK

    def pack(target, at):
        target[tp, 0:1, :] = jnp.sum(psum[at, :].T, axis=0, keepdims=True)
        target[tp, 1:2, :] = jnp.sum(csum[at, :].T, axis=0, keepdims=True)

    def stat_copy(k, target, c):
        return pltpu.make_async_remote_copy(
            src_ref=target.at[tp], dst_ref=target.at[tp],
            send_sem=sent.at[2 + c], recv_sem=stat_sem.at[c],
            device_id={"tp": lax.rem(tp + k, m)}, device_id_type=MESH,
        )

    def stat_all(target, c):
        others = target.at[pl.ds(0, m - 1)]
        return pltpu.make_async_remote_copy(
            src_ref=others, dst_ref=others,
            send_sem=sent.at[2 + c], recv_sem=stat_sem.at[c],
            device_id={"tp": lax.rem(tp + 1, m)}, device_id_type=MESH,
        )

    def stat_send(target, c):
        @pl.loop(1, m)
        def _(k):
            stat_copy(k, target, c).start()

    gains = lax.fori_loop(
        first, blocks, stat_block, tuple(jnp.zeros((8, LANES), F32) for _ in range(tiles))
    )
    late_rows, head_rows = slice(LANES, rows), slice(0, LANES)
    pack(late_stats, late_rows)
    stat_send(late_stats, 0)

    hear(0)
    tell(1)

    @pl.when(sp > 0)
    def _():
        halo_copy.wait_recv()
        for ct in range(tiles):
            gp[ct, 0:halo, :] = halo_in[:, lanes(ct)].astype(F32)

    @pl.when(sp == 0)
    def _():
        for ct in range(tiles):
            gp[ct, 0:halo, :] = jnp.zeros((halo, LANES), F32)

    conv_rows(0, halo)
    turn(0)
    below = q == 1
    above = q == 2

    def far(i):
        return jnp.where(low, half - 1 - i, i)

    order = [
        jnp.where(below, sib, far(0)),
        jnp.where(below, far(0), far(1)),
        jnp.where(below, far(1), sib),
        q,
    ]
    parts = (slice(0, cut), slice(cut, 2 * cut))
    last = slice(2 * cut, chans)

    def product(block):
        at = pl.ds(pl.multiple_of(block * dr, LANES), dr)
        return jnp.dot(actt[...], og[:, at], preferred_element_type=F32)

    def y_copy(p, s):
        return pltpu.make_async_remote_copy(
            src_ref=ysend.at[p, s], dst_ref=yrecv.at[p, s],
            send_sem=sent.at[6], recv_sem=y_recv.at[p, s],
            device_id={"sp": partner}, device_id_type=MESH,
        )

    def away(p):
        part = product(2 * p + 1 - par)
        for s in range(2):
            ysend[p, s] = part[parts[s], :].astype(BF16)
        zfown[p, 0] = part[last, :]

    def home(p):
        part = product(2 * p + par)
        for s in range(2):
            wsum[p, s] = part[parts[s], :]
        zfown[p, 1] = part[last, :]

    ahead = lax.rem(tp, 2) == 0

    def send(cond, halves):
        @pl.when(cond)
        def _():
            for i, s in halves:
                y_copy(order[i], s).start()

    def zf_copy(i, peer, slot):
        return pltpu.make_async_remote_copy(
            src_ref=zfsend.at[i], dst_ref=zfin.at[slot],
            send_sem=sent.at[8], recv_sem=zf_recv.at[slot],
            device_id={"sp": 2 * peer + par}, device_id_type=MESH,
        )

    def zf_far(i):
        zfsend[i] = zfown[far(i)].astype(BF16)
        zf_copy(i, far(i), jnp.where(outer, 1, 2)).start()

    def zf_sib():
        zfsend[2] = zfown[sib].astype(BF16)
        zf_copy(2, sib, 0).start()

    inner = jnp.logical_not(outer)
    away(order[0])
    send(ahead, ((0, 0), (0, 1)))
    gains = lax.fori_loop(0, first, stat_block, gains)
    pack(head_stats, head_rows)
    stat_send(head_stats, 1)
    away(order[1])
    send(ahead, ((1, 0), (1, 1)))
    hear(1)
    home(order[0])

    @pl.when(jnp.logical_not(below))
    def _():
        zf_far(0)

    home(order[1])

    @pl.when(below)
    def _():
        zf_far(0)

    @pl.when(jnp.logical_not(below))
    def _():
        zf_far(1)

    away(order[2])
    home(order[2])

    @pl.when(below)
    def _():
        zf_far(1)

    @pl.when(inner)
    def _():
        zf_sib()

    send(jnp.logical_not(ahead), [(i, s) for i in (0, 1) for s in range(2)])

    def cg_block(b, _):
        at = pl.ds(pl.multiple_of(b * BLOCK, BLOCK), BLOCK)
        for ct in range(tiles):
            cg[ct, at, :] = scaleb[at, :] * (
                agrad[at, lanes(ct)] - mpb[at, :] - centered[ct, at, :] * mcb[at, :]
            )
        return 0

    def cg_rows(target, c, at, begin, end):
        stat_all(target, c).wait_recv()
        totals = target[0]
        for k in range(1, m):
            totals = totals + target[k]
        totals = totals / (chans * m)
        count = target.shape[2]
        mpb[at, :] = jnp.broadcast_to(totals[0:1, :], (LANES, count)).T
        mcb[at, :] = jnp.broadcast_to(totals[1:2, :], (LANES, count)).T
        lax.fori_loop(begin, end, cg_block, 0)

    cg_rows(late_stats, 0, late_rows, first, blocks)

    span = 32

    def tap_rows(ct, begin, end, sums):
        def tap_block(b, sums):
            start = pl.multiple_of(b * span, span)
            grad = cg[ct, pl.ds(start, span), :]
            new = []
            for k in range(kw):
                prod = grad * source(gp, k + lead, ct, start, span)
                new.append(sums[k] + jnp.sum(prod.reshape(span // 8, 8, LANES), axis=0))
            return tuple(new)

        return lax.fori_loop(begin // span, end // span, tap_block, sums)

    for ct in range(tiles):
        sums = tap_rows(ct, LANES, rows, tuple(jnp.zeros((8, LANES), F32) for _ in range(kw)))
        for k in range(kw):
            tapacc[ct, k] = sums[k]

    def side_copy(i, slot, s):
        return pltpu.make_async_remote_copy(
            src_ref=zsend.at[i, s], dst_ref=zrecv.at[slot, s],
            send_sem=sent.at[7], recv_sem=z_recv.at[slot, s],
            device_id={"sp": 2 * sib + par}, device_id_type=MESH,
        )

    def cross_copy(i, s):
        return pltpu.make_async_remote_copy(
            src_ref=zsend.at[i, s], dst_ref=xrecv.at[s],
            send_sem=sent.at[7], recv_sem=x_recv.at[s],
            device_id={"sp": 2 * order[i] + par}, device_id_type=MESH,
        )

    def relay(i, s):
        p = order[i]
        crossing = (above, inner, below)[i]
        slot = (jnp.where(below, 2, 0), jnp.where(below, 0, 1), jnp.where(below, 1, 2))[i]
        y_copy(p, s).wait_recv()

        @pl.when(jnp.logical_not(crossing))
        def _():
            zsend[i, s] = (wsum[p, s] + yrecv[p, s].astype(F32)).astype(BF16)
            side_copy(i, slot, s).start()

        @pl.when(crossing)
        def _():
            own = wsum[p, s] + yrecv[p, s].astype(F32)
            side_copy(i, slot, s).wait_recv()
            zsend[i, s] = (own + zrecv[slot, s].astype(F32)).astype(BF16)
            cross_copy(i, s).start()

    @pl.when(jnp.logical_and(outer, ahead))
    def _():
        relay(0, 0)

    cg_rows(head_stats, 1, head_rows, 0, first)
    back_copy = pltpu.make_async_remote_copy(
        src_ref=cg.at[:, pl.ds(0, halo), :], dst_ref=cg.at[:, pl.ds(rows, halo), :],
        send_sem=sent.at[1], recv_sem=back_sem,
        device_id={"sp": lax.rem(sp + n - 1, n)}, device_id_type=MESH,
    )

    @pl.when(sp > 0)
    def _():
        back_copy.start()

    for ct in range(tiles):
        sums = tap_rows(ct, 0, LANES, tuple(tapacc[ct, k] for k in range(kw)))
        for k, total in enumerate((*sums, gains[ct])):
            taploc[ct, k : k + 1, :] = jnp.sum(total, axis=0, keepdims=True)

    tapout[...] = taploc[...].astype(BF16)
    pair_copy = pltpu.make_async_remote_copy(
        src_ref=tapout, dst_ref=tappair, send_sem=sent.at[4], recv_sem=pair_sem,
        device_id={"sp": partner}, device_id_type=MESH,
    )
    pair_copy.start()
    for s in range(2):
        y_copy(order[2], s).start()
    away(order[3])
    for s in range(2):
        y_copy(order[3], s).start()
    home(order[3])
    @pl.when(jnp.logical_and(outer, jnp.logical_not(ahead)))
    def _():
        relay(0, 0)

    @pl.when(outer)
    def _():
        relay(0, 1)

    @pl.when(below)
    def _():
        relay(0, 0)


    def back_block(b, _):
        start = pl.multiple_of(b * BLOCK, BLOCK)
        at = pl.ds(start, BLOCK)
        for ct in range(tiles):
            total = jnp.zeros((BLOCK, LANES), F32)
            for k in range(kw):
                total = total + taps[k : k + 1, lanes(ct)] * source(cg, reach - k, ct, start, BLOCK)
            sig = jax.nn.sigmoid(gate[at, lanes(ct)].astype(F32))
            value_grad[at, lanes(ct)] = (total * sig).astype(BF16)
            gate_grad[at, lanes(ct)] = (
                total * val[at, lanes(ct)].astype(F32) * sig * (1.0 - sig)
            ).astype(BF16)
        return 0

    lax.fori_loop(0, blocks // 2, back_block, 0)

    @pl.when(outer)
    def _():
        relay(1, 0)
        relay(1, 1)
        zf_sib()

    @pl.when(below)
    def _():
        relay(0, 1)

    pair_copy.wait_recv()
    tapz[q] = (tapout[...].astype(F32) + tappair[...].astype(F32)).astype(BF16)

    def tap_copy(p, source_ref):
        return pltpu.make_async_remote_copy(
            src_ref=source_ref, dst_ref=source_ref,
            send_sem=sent.at[5], recv_sem=tap_sem,
            device_id={"sp": 2 * p + par}, device_id_type=MESH,
        )

    for p in (far(0), far(1), sib):
        tap_copy(p, tapz.at[q]).start()

    tap_all = tap_copy(sib, tapz.at[pl.ds(0, half - 1)])

    lax.fori_loop(blocks // 2, blocks - 1, back_block, 0)

    @pl.when(above)
    def _():
        relay(0, 0)
        relay(0, 1)

    @pl.when(inner)
    def _():
        relay(1, 0)

    @pl.when(inner)
    def _():
        relay(1, 1)

    relay(2, 0)
    @pl.when(sp < n - 1)
    def _():
        back_copy.wait_recv()

    @pl.when(sp == n - 1)
    def _():
        cg[:, rows : rows + halo, :] = jnp.zeros((tiles, halo, LANES), F32)

    back_block(blocks - 1, 0)

    relay(2, 1)

    for slot in range(half - 1):
        zf_copy(0, sib, slot).wait_recv()
    for k in range(2):
        zfown[q, k] += (
            zfin[0, k].astype(F32) + zfin[1, k].astype(F32) + zfin[2, k].astype(F32)
        )
    zfysend[...] = zfown[q, 0].astype(BF16)
    zf_back = pltpu.make_async_remote_copy(
        src_ref=zfysend, dst_ref=zfyrecv, send_sem=sent.at[9], recv_sem=zfy_sem,
        device_id={"sp": partner}, device_id_type=MESH,
    )
    zf_back.start()

    for s in range(2):
        y_copy(q, s).wait_recv()
        wsum[q, s] += yrecv[q, s].astype(F32)
    tap_all.wait_recv()

    for ct in range(tiles):
        total = tapz[0, ct].astype(F32)
        for k in range(1, half):
            total = total + tapz[k, ct].astype(F32)
        taps_out[:, lanes(ct)] = total[0:kw]
        gain_out[:, lanes(ct)] = total[kw : kw + 1]

    for s in range(2):
        side_copy(0, 2, s).wait_recv()
        cross_copy(0, s).wait_recv()
        whole[parts[s], :] = wsum[q, s] + zrecv[2, s].astype(F32) + xrecv[s].astype(F32)
    zf_back.wait_recv()
    whole[last, :] = zfown[q, 1] + zfyrecv[...].astype(F32)
    w_out[...] = whole[...].T

    @pl.when(sp < n - 1)
    def _():
        halo_copy.wait_send()

    @pl.when(sp > 0)
    def _():
        back_copy.wait_send()

    stat_all(late_stats, 0).wait_send()
    stat_all(head_stats, 1).wait_send()
    pair_copy.wait_send()
    tap_all.wait_send()
    pltpu.make_async_remote_copy(
        src_ref=ysend, dst_ref=yrecv, send_sem=sent.at[6], recv_sem=y_recv.at[0, 0],
        device_id={"sp": partner}, device_id_type=MESH,
    ).wait_send()
    pltpu.make_async_remote_copy(
        src_ref=zsend, dst_ref=zrecv, send_sem=sent.at[7], recv_sem=z_recv.at[0, 0],
        device_id={"sp": partner}, device_id_type=MESH,
    ).wait_send()
    pltpu.make_async_remote_copy(
        src_ref=zfsend, dst_ref=zfin, send_sem=sent.at[8], recv_sem=zf_recv.at[0],
        device_id={"sp": partner}, device_id_type=MESH,
    ).wait_send()
    zf_back.wait_send()


def finish(count, *refs):
    sem = refs[-1]
    copies = [
        pltpu.make_async_copy(source, target, sem.at[k])
        for k, (source, target) in enumerate(zip(refs[:count], refs[count : 2 * count]))
    ]
    for copy in copies:
        copy.start()
    for copy in copies:
        copy.wait()


def pair_kernel(n, m, kw, *refs):
    pl.run_scoped(
        functools.partial(pair_body, n, m, kw, *refs),
        pltpu.SemaphoreType.DMA((8,)), pltpu.SemaphoreType.DMA((10,)),
    )


def outputs(rows, chans, kw, dr):
    return (
        pltpu.VMEM((rows, chans), BF16),
        pltpu.VMEM((rows, chans), BF16),
        pltpu.VMEM((kw, chans), F32),
        pltpu.VMEM((1, chans), F32),
        pltpu.VMEM((dr, chans), F32),
    )


def pair_call(n, m, rows, chans, kw, depth):
    dr = depth // n
    half = n // 2
    tiles = chans // LANES
    halo = rup(kw - 1, 16)
    taps_rows = rup(kw + 1, 16)
    zf = chans // 4
    cut = (chans - zf) // 2
    vm = pltpu.VMEM
    dma = pltpu.SemaphoreType.DMA
    wide = vm((rows, LANES), F32)
    block = vm((half, 2, cut, dr), BF16)
    part = vm((half - 1, 2, cut, dr), BF16)
    return pl.pallas_call(
        functools.partial(pair_kernel, n, m, kw),
        out_shape=outputs(rows, chans, kw, dr),
        in_specs=[pl.BlockSpec(memory_space=pltpu.HBM)] * 8,
        out_specs=(pl.BlockSpec(memory_space=pltpu.VMEM),) * 5,
        scratch_shapes=[
            vm((rows, chans), BF16), vm((rows, chans), BF16), vm((kw, chans), BF16),
            vm((1, chans), F32), vm((1, rows), F32), vm((1, rows), F32),
            vm((rows, depth), BF16), vm((depth, chans), BF16),
            vm((kw, chans), F32),
            vm((tiles, rows + halo, LANES), F32),
            vm((tiles, rows + halo, LANES), F32),
            vm((tiles, rows, LANES), F32),
            vm((tiles, rows, LANES), F32),
            vm((rows, chans), BF16),
            vm((chans, rows), BF16),
            vm((rows, chans), F32),
            wide, wide, wide, wide, wide, wide,
            vm((halo, chans), BF16), vm((halo, chans), BF16),
            vm((m, 2, rows - LANES), F32), vm((m, 2, LANES), F32), vm((tiles, kw, 8, LANES), F32),
            vm((tiles, taps_rows, LANES), F32), vm((tiles, taps_rows, LANES), BF16),
            vm((tiles, taps_rows, LANES), BF16),
            vm((half, tiles, taps_rows, LANES), BF16),
            vm((half, 2, cut, dr), F32),
            block, block, part, part, vm((2, cut, dr), BF16),
            vm((half, 2, zf, dr), F32), vm((half - 1, 2, zf, dr), BF16), vm((half - 1, 2, zf, dr), BF16),
            vm((zf, dr), BF16), vm((zf, dr), BF16), vm((chans, dr), F32),
            dma, dma, dma((2,)), dma, dma, dma((half, 2)), dma((half - 1, 2)), dma((2,)),
            dma((half - 1,)), dma,
            pltpu.SemaphoreType.REGULAR((half - 2, 2)),
        ],
        compiler_params=pltpu.CompilerParams(
            collective_id=0, has_side_effects=True, vmem_limit_bytes=VMEM_LIMIT,
        ),
    )


def wide_call(n, m, rows, chans, kw, depth):
    dr = depth // n
    half = n // 2
    tiles = chans // LANES
    halo = rup(kw - 1, 16)
    vm = pltpu.VMEM
    dma = pltpu.SemaphoreType.DMA
    whole = pl.BlockSpec(memory_space=pltpu.VMEM)
    far = pl.BlockSpec(memory_space=pltpu.HBM)
    return pl.pallas_call(
        functools.partial(kernel, n, m, kw),
        out_shape=outputs(rows, chans, kw, dr),
        in_specs=[whole] * 6 + [far] * 2,
        out_specs=(whole,) * 5,
        scratch_shapes=[
            vm((kw, chans), F32),
            vm((rows, depth), BF16),
            vm((depth, chans), BF16),
            vm((tiles, rows + halo, LANES), F32),
            vm((7, tiles, rows + halo, LANES), F32),
            vm((tiles, rows + halo, LANES), F32),
            vm((7, tiles, rows + halo, LANES), F32),
            vm((tiles, rows, LANES), F32),
            vm((tiles, rows, LANES), F32),
            vm((rows, chans), BF16),
            vm((rows, chans), F32),
            vm((rows, LANES), F32),
            vm((rows, LANES), F32),
            vm((rows, LANES), F32),
            vm((rows, LANES), F32),
            vm((rows, LANES), F32),
            vm((rows, LANES), F32),
            vm((halo, chans), BF16),
            vm((halo, chans), BF16),
            vm((m, 2, rows), F32),
            vm((n, tiles, rup(kw + 1, n) // n, LANES), F32),
            vm((n, tiles, rup(kw + 1, n) // n, LANES), F32),
            vm((n, tiles, rup(kw + 1, n) // n, LANES), F32),
            vm((depth, chans), F32),
            vm((depth, chans), BF16),
            vm((half, dr, chans), BF16),
            vm((half, dr, chans), BF16),
            vm((half, dr, chans), BF16),
            dma((2,)), dma((2,)), dma((2,)),
            dma((m,)), dma((m,)), dma((n,)), dma((n,)), dma((n,)), dma((n,)),
            dma((half,)), dma((half,)), dma((half,)), dma((half,)),
        ],
        compiler_params=pltpu.CompilerParams(
            collective_id=0, has_side_effects=True, vmem_limit_bytes=VMEM_LIMIT
        ),
    )


def per_device(
    n, m, glu_value, glu_gate, conv_taps, norm_gain, out_weight, norm_mean, norm_scale, out_grad
):
    rows, chans = glu_value.shape
    kw = conv_taps.shape[0]
    depth = out_grad.shape[1]
    paired = n == 8 and (depth // n) % LANES == 0 and chans % (2 * LANES) == 0
    call = (pair_call if paired else wide_call)(n, m, rows, chans, kw, depth)
    out = call(*[
        pltpu.with_memory_space_constraint(x, pltpu.HBM)
        for x in (
            glu_value, glu_gate, conv_taps, norm_gain[None, :],
            norm_mean[None, :], norm_scale[None, :], out_grad, out_weight,
        )
    ])
    whole = pl.BlockSpec(memory_space=pltpu.VMEM)
    out = pl.pallas_call(
        functools.partial(finish, len(out)),
        out_shape=tuple(jax.ShapeDtypeStruct(x.shape, x.dtype) for x in out),
        in_specs=[whole] * len(out),
        out_specs=(pl.BlockSpec(memory_space=pltpu.HBM),) * len(out),
        scratch_shapes=[pltpu.SemaphoreType.DMA((len(out),))],
        compiler_params=pltpu.CompilerParams(vmem_limit_bytes=2 * 1024 * 1024),
    )(*out)
    value_grad, gate_grad, taps_grad, gain_grad, weight_grad = out
    return value_grad, gate_grad, taps_grad, gain_grad[0], weight_grad


def solution(mesh):
    placed = (
        P("sp", "tp"), P("sp", "tp"), P(None, "tp"), P("tp"),
        P(None, "tp"), P("sp"), P("sp"), P("sp", None),
    )
    return jax.shard_map(
        functools.partial(per_device, mesh.shape["sp"], mesh.shape["tp"]),
        mesh=mesh,
        in_specs=placed,
        out_specs=(P("sp", "tp"), P("sp", "tp"), P(None, "tp"), P("tp"), P("sp", "tp")),
        check_vma=False,
    )
```
